512 devices in a mesh: sp: 32 (over z, x), tp: 16 (over y, core).
Axes of the slice: x: 4, y: 8, z: 8, core: 2. Of those that a mesh axis runs over, the one named last changes fastest.
Arguments:
- mixed: bfloat16 [4096, 2048], P('sp'), may hold values from -6 to 6
- cotangent: bfloat16 [4096, 2048], P('sp'), may hold values from -6 to 6
- routes: int32 [4096, 2], P('sp'), may hold values from 0 to 31, all different within a row; in each aligned block of 128 rows (0 to 127, 128 to 255, ...) at most 16 rows name the same one
- gates: float32 [4096, 2], P('sp'), may hold values from 0.1 to 1
- w_gate: bfloat16 [32, 2048, 1024], P('sp', None, 'tp'), may hold values from -0.125 to 0.125
- w_up: bfloat16 [32, 2048, 1024], P('sp', None, 'tp'), may hold values from -0.125 to 0.125
- w_down: bfloat16 [32, 1024, 2048], P('sp', 'tp'), may hold values from -0.1875 to 0.1875
- out_weight: bfloat16 [4096, 2048], P('tp'), may hold values from -0.09375 to 0.09375
- gate_pre: bfloat16 [4096, 4096], P('sp', 'tp'), may hold values from -8 to 8
- mixer_out: bfloat16 [4096, 4096], P('sp', 'tp'), may hold values from -6 to 6
- values: bfloat16 [4096, 4096], P('sp', 'tp'), may hold values from -6 to 6
- write_keys: bfloat16 [4096, 2048], P('sp', 'tp'), may hold values from -1.25 to 1.25
- read_keys: bfloat16 [4096, 2048], P('sp', 'tp'), may hold values from -1.25 to 1.25
- log_decay: float32 [64, 4096], P('tp', 'sp'), may hold values from -0.08 to 0
- entry_states: float32 [32, 64, 64, 128], P('sp', 'tp'), may hold values from -6 to 6
Outputs:
- d_w_gate: bfloat16 [32, 2048, 1024], P('sp', None, 'tp')
- d_w_up: bfloat16 [32, 2048, 1024], P('sp', None, 'tp')
- d_w_down: bfloat16 [32, 1024, 2048], P('sp', 'tp')
- d_out_weight: float32 [2048, 4096], P('sp', 'tp')
- d_input: bfloat16 [4096, 2048], P('sp', 'tp')
- d_values: bfloat16 [4096, 4096], P('sp', 'tp')
- d_write: float32 [4096, 2048], P('sp', 'tp')
- d_read: float32 [4096, 2048], P('sp', 'tp')
- d_gate: bfloat16 [4096, 4096], P('sp', 'tp')
The draws below stay inside these ranges and needn't reach their ends.
Inputs may be any that keep to these rules, and one draw needn't show every extreme that they name: `routes`: each row names 2 different experts; in the 128 rows of one device no expert is named more than 16 times, and in some blocks one is named exactly 16 times.
All inputs are finite; a program needn't handle non-finite values.
Results may differ from the reference program's by a relative error of at most 0.0062.
Values may be sent and summed in bfloat16 or wider, within the bound.
No kernel may reach another device: no remote copies, remote signals or barrier semaphores. Data moves between devices by JAX's collectives and lax.ppermute only.
A program may use at most 64 MiB of HBM per device.

```python
import math
import jax
import jax.numpy as jnp
import numpy as np
from jax import lax

D = 2048
FF_E = 1024
HEAD_DIM = 64
STATE = 128
HPG = 4
BLOCK = 128
TOPK = 2
TOK_DEV = 128
GROUPS = 16
HEADS = 64
D_INNER = 4096
EXPERTS = 32
TOKENS = 4096
CAP = 16
NBLK = 32
N_SP = 32
N_TP = 16


def draw_log_decay(key, part):
    key_set = jax.random.split(key, 3)
    chooser = jax.random.uniform(key_set[0], (HEADS, 1))
    fast_head = chooser < 0.5
    base_rate = jnp.where(fast_head, 1.0 / 40.0, 0.5 / TOKENS)
    shard_scale = jnp.exp(jax.random.uniform(key_set[1], (HEADS, TOKENS // TOK_DEV), minval=-0.7, maxval=0.7))
    shard_scale = jnp.repeat(shard_scale, TOK_DEV, axis=1)
    jitter = jax.random.uniform(key_set[2], (HEADS, TOKENS), minval=0.5, maxval=1.5)
    return -(base_rate * shard_scale * jitter)


def strengthened(values, own_key, source, target, shards_of, factor):
    owner, partner = [(jnp.arange(values.shape[dim]) // (values.shape[dim] // shards_of)).reshape([-1 if axis == dim else 1 for axis in range(values.ndim)]) for dim in (source, target)]
    chosen = jax.random.permutation(own_key, shards_of)[partner]
    strong = (owner == chosen) | (owner == (partner + shards_of // 2) % shards_of)
    return jnp.where(strong, factor * values, values)


def block_scale(key, shape, shards, smallest, high):
    loudness, own = 1.0, jax.random.fold_in(key, 6)
    for axis_at, parts in shards:
        steps = jnp.exp(jax.random.uniform(jax.random.fold_in(own, axis_at), (parts,), jnp.float32, smallest / len(shards), high / len(shards)))
        loudness = loudness * jnp.repeat(steps, shape[axis_at] // parts).reshape([-1 if axis == axis_at else 1 for axis in range(len(shape))])
    return loudness


def assign_block(stream_key, own, number, rows, count, top, limit, skew):
    sequence = jax.random.permutation(stream_key, count)
    packed, usual = load_shares(count, rows * top, limit, skew, True), load_shares(count, rows * top, limit, skew, False)
    places = jnp.arange(count)

    def named(tallies, turn):
        used = int((tallies > 0).sum())
        fixed = max(1, used // 4)
        passed = fixed + (places - fixed + turn * (used - fixed)) % max(1, count - fixed)
        return jnp.zeros((count,), jnp.int32).at[sequence[jnp.where(places < fixed, places, passed)]].set(jnp.asarray(tallies, jnp.int32))

    tallies = jnp.where(number % 4 == 0, named(packed, number // 4), named(usual, number - number // 4 - 1))
    mixed = jax.random.permutation(jax.random.fold_in(own, 3), count)
    source_of, receiver = mixed[0:count // 2 * 2:2], mixed[1:count // 2 * 2:2]
    slack = jnp.minimum(tallies[source_of] - 1, limit - tallies[receiver]) // 2
    slack = jnp.where((source_of == sequence[0]) | (receiver == sequence[0]) | (tallies[receiver] == 0), 0, jnp.maximum(slack, 0))
    passed = jax.random.randint(jax.random.fold_in(own, 4), (count // 2,), 0, 1 << 20) % (slack + 1)
    tallies = tallies.at[source_of].add(-passed).at[receiver].add(passed)
    members = jnp.searchsorted(jnp.cumsum(tallies), jnp.arange(rows * top), side="right").astype(jnp.int32)
    listing = members.reshape(top, rows).T
    listing = listing[jax.random.permutation(jax.random.fold_in(own, 1), rows)]
    turn = jax.random.randint(jax.random.fold_in(own, 2), (rows, 1), 0, top)
    return jnp.take_along_axis(listing, (jnp.arange(top)[None, :] + turn) % top, axis=1)


def load_shares(count, total, limit, slope, full):
    loads = [(1 << 20) // math.isqrt(grade ** slope) + 1 for grade in range(1, count + 1)]
    largest = limit if full else min(limit, max(-(-total // count), total * loads[0] // sum(loads)))
    least = 1 if total - largest >= count - 1 else 0
    counts, rest = [largest] + [least] * (count - 1), total - largest - least * (count - 1)
    while rest > 0:
        candidates = [i for i in range(1, count) if counts[i] < largest] or [i for i in range(1, count) if counts[i] < limit]
        whole, budget = sum([loads[i] for i in candidates]), rest
        for i in candidates:
            addition = min(limit - counts[i], max(1, budget * loads[i] // whole), rest)
            counts[i] = counts[i] + addition
            rest = rest - addition
    return np.array(counts)


def bell_draw(stream_key, shape, width, reach, shards=(), kind=jnp.bfloat16):
    entries = jax.random.normal(stream_key, shape, jnp.float32) * width
    if len(shards) > 0:
        entries = block_scale(stream_key, shape, shards, -0.22, 0.18) * entries
    return jnp.clip(entries, min=-reach, max=reach).astype(kind)


def noise_with(stream_key, shape, width, reach, shards, heavy, kind=jnp.bfloat16):
    drawn = width * jax.random.normal(stream_key, shape, jnp.float32)
    if shards:
        drawn = drawn * block_scale(stream_key, shape, shards, -0.22, 0.18)
    return jnp.clip(strengthened(drawn, jax.random.fold_in(stream_key, 3), *heavy), -reach, reach).astype(kind)


def setup_inputs(seed: int = 0) -> dict:
    arg_keys = jax.random.split(jax.random.key(seed), 16)
    mixed = bell_draw(arg_keys[0], (TOKENS, D), 1.0, 6.0, ((0, 32),))
    cotangent = noise_with(arg_keys[1], (TOKENS, D), 1.0, 6.0, ((0, 32),), (0, 1, 32, 2.75))
    routes_keys = jax.random.split(jax.random.fold_in(arg_keys[2], 1), TOKENS // TOK_DEV)
    routes_turns = jax.random.permutation(jax.random.fold_in(arg_keys[2], 3), TOKENS // TOK_DEV)
    routes = jax.vmap(lambda own, number: assign_block(jax.random.fold_in(arg_keys[2], 2), own, number, TOK_DEV, EXPERTS, TOPK, CAP, 2))(routes_keys, routes_turns).reshape((TOKENS, TOPK))
    gates = jnp.clip(0.1 + 0.9 * jax.random.uniform(arg_keys[3], (TOKENS, TOPK), jnp.float32) ** block_scale(arg_keys[3], (TOKENS, TOPK), ((0, 32),), -0.2, 0.2), 0.1, 1.0)
    w_gate = bell_draw(arg_keys[4], (EXPERTS, D, FF_E), D ** -0.5, 0.125, ((0, 32), (2, 16)))
    w_up = bell_draw(arg_keys[5], (EXPERTS, D, FF_E), D ** -0.5, 0.125, ((0, 32), (2, 16)))
    w_down = bell_draw(arg_keys[6], (EXPERTS, FF_E, D), FF_E ** -0.5, 0.1875, ((0, 32), (1, 16)))
    out_weight = bell_draw(arg_keys[7], (D_INNER, D), D_INNER ** -0.5, 0.09375, ((0, 16),))
    gate_pre = bell_draw(arg_keys[8], (TOKENS, D_INNER), 1.5, 8.0, ((0, 32), (1, 16)))
    mixer_out = bell_draw(arg_keys[9], (TOKENS, D_INNER), 1.0, 6.0, ((0, 32), (1, 16)))
    values = bell_draw(arg_keys[10], (TOKENS, D_INNER), 1.0, 6.0, ((0, 32), (1, 16)))
    write_keys = bell_draw(arg_keys[11], (TOKENS, GROUPS * STATE), 0.2, 1.25, ((0, 32), (1, 16)))
    read_keys = bell_draw(arg_keys[12], (TOKENS, GROUPS * STATE), 0.2, 1.25, ((0, 32), (1, 16)))
    log_decay = draw_log_decay(jax.random.fold_in(arg_keys[15], 71), 0)
    entry_states = bell_draw(arg_keys[14], (NBLK, HEADS, HEAD_DIM, STATE), 1.0, 6.0, ((0, 32), (1, 16)), jnp.float32)
    return dict(mixed=mixed, cotangent=cotangent, routes=routes, gates=gates, w_gate=w_gate, w_up=w_up, w_down=w_down, out_weight=out_weight, gate_pre=gate_pre, mixer_out=mixer_out, values=values, write_keys=write_keys, read_keys=read_keys, log_decay=log_decay, entry_states=entry_states)


precise = lax.Precision.HIGHEST

def silu_grad(pre_act):
    logistic = jax.nn.sigmoid(pre_act)
    return logistic * (1.0 + pre_act * (1.0 - logistic))

def expert_back(inputs):
    tok_rows, cot_rows, weight_g, weight_u, weight_d = inputs
    pre_gate = jnp.dot(tok_rows, weight_g, preferred_element_type=jnp.float32)
    pre_up = jnp.dot(tok_rows, weight_u, preferred_element_type=jnp.float32)
    active = jax.nn.silu(pre_gate)
    hidden = (active * pre_up).astype(jnp.bfloat16)
    grad_down = jnp.dot(hidden.T, cot_rows, preferred_element_type=jnp.float32)
    grad_hidden = jnp.dot(cot_rows, weight_d.T, preferred_element_type=jnp.float32)
    grad_gate = (grad_hidden * pre_up * silu_grad(pre_gate)).astype(jnp.bfloat16)
    grad_upval = (grad_hidden * active).astype(jnp.bfloat16)
    grad_wg = jnp.dot(tok_rows.T, grad_gate, preferred_element_type=jnp.float32)
    grad_wu = jnp.dot(tok_rows.T, grad_upval, preferred_element_type=jnp.float32)
    part_width = FF_E // N_TP
    gate_parts = grad_gate.astype(jnp.float32).reshape(-1, N_TP, part_width)
    up_parts = grad_upval.astype(jnp.float32).reshape(-1, N_TP, part_width)
    wg_parts = weight_g.astype(jnp.float32).reshape(D, N_TP, part_width)
    wu_parts = weight_u.astype(jnp.float32).reshape(D, N_TP, part_width)
    partial_value = jnp.einsum('rif,dif->ird', gate_parts, wg_parts) + jnp.einsum('rif,dif->ird', up_parts, wu_parts)
    rounded = lax.optimization_barrier(partial_value.astype(jnp.bfloat16))
    summed = lax.optimization_barrier(jnp.sum(rounded.astype(jnp.float32), axis=0))
    return (grad_wg.astype(jnp.bfloat16), grad_wu.astype(jnp.bfloat16), grad_down.astype(jnp.bfloat16), summed.astype(jnp.bfloat16))

def block_back(grad_state, inputs):
    inputs_x, grad_y, log_rate, write_rows, read_rows, start_state = inputs
    block_len = log_rate.shape[0]
    running = jnp.cumsum(log_rate, axis=0)
    causal_mask = (jnp.arange(block_len)[:, None] >= jnp.arange(block_len)[None, :])[:, :, None, None]
    spread = running[:, None] - running[None, :]
    decay_mat = jnp.where(causal_mask, jnp.exp(jnp.where(causal_mask, spread, 0.0)), 0.0)
    intersection = jnp.einsum('lgn,sgn->lsg', read_rows, write_rows, precision=precise)
    mixing = intersection[..., None] * decay_mat
    to_end = jnp.exp(running[-1][None] - running)
    from_start = jnp.exp(running)
    grad_x = jnp.einsum('lsgj,lgjp->sgjp', mixing, grad_y, precision=precise) + to_end[..., None] * jnp.einsum('sgn,gjpn->sgjp', write_rows, grad_state, precision=precise)
    weighted = jnp.einsum('lgjp,sgjp->lsgj', grad_y, inputs_x, precision=precise) * decay_mat
    grad_w = jnp.einsum('lsgj,lgn->sgn', weighted, read_rows, precision=precise) + jnp.einsum('sgj,sgjp,gjpn->sgn', to_end, inputs_x, grad_state, precision=precise)
    grad_r = jnp.einsum('lsgj,sgn->lgn', weighted, write_rows, precision=precise) + jnp.einsum('lgj,lgjp,gjpn->lgn', from_start, grad_y, start_state, precision=precise)
    earlier = jnp.exp(running[-1])[..., None, None] * grad_state + jnp.einsum('lgj,lgjp,lgn->gjpn', from_start, grad_y, read_rows, precision=precise)
    return (earlier, (grad_x, grad_w, grad_r))

def reference(mixed, cotangent, routes, gates, w_gate, w_up, w_down, out_weight, gate_pre, mixer_out, values, write_keys, read_keys, log_decay, entry_states):
    assigned = TOKENS * TOPK
    picks = routes.reshape(N_SP, TOK_DEV * TOPK)
    onehot = (picks[:, :, None] == jnp.arange(EXPERTS, dtype=jnp.int32)[None, None, :]).astype(jnp.int32)
    earlier_same = jnp.cumsum(onehot, axis=1) - onehot
    slot_of = lax.optimization_barrier(jnp.sum(earlier_same * onehot, axis=2))
    shard_ids = jnp.arange(N_SP, dtype=jnp.int32)[:, None]
    target = ((picks * N_SP + shard_ids) * CAP + slot_of).reshape(assigned).astype(jnp.int32)
    anchor = jnp.full((EXPERTS * N_SP * CAP,), assigned, jnp.int32).at[target].set(jnp.arange(assigned, dtype=jnp.int32))
    scaled = (gates[:, :, None] * cotangent[:, None, :].astype(jnp.float32)).astype(jnp.bfloat16).reshape(assigned, D)
    empty_row = jnp.zeros((1, D), jnp.bfloat16)
    cot_rows = jnp.concatenate([scaled, empty_row])[anchor].reshape(EXPERTS, N_SP * CAP, D)
    tok_rows = jnp.concatenate([mixed, empty_row])[anchor // TOPK].reshape(EXPERTS, N_SP * CAP, D)
    grad_wg, grad_wu, grad_down, row_grad = lax.map(expert_back, (tok_rows, cot_rows, w_gate, w_up, w_down))
    picked = row_grad.reshape(EXPERTS * N_SP * CAP, D)[target].reshape(TOKENS, TOPK, D).astype(jnp.float32)
    d_input = (cotangent.astype(jnp.float32) + lax.optimization_barrier(jnp.sum(picked, axis=1))).astype(jnp.bfloat16)
    back_proj = jnp.dot(d_input, out_weight.T, preferred_element_type=jnp.float32)
    pre_act = gate_pre.astype(jnp.float32)
    gate_act = jax.nn.silu(pre_act)
    saved_out = mixer_out.astype(jnp.float32)
    d_gate = (back_proj * saved_out * silu_grad(pre_act)).astype(jnp.bfloat16)
    gated = (saved_out * gate_act).astype(jnp.bfloat16)
    d_out_weight = jnp.dot(d_input.T, gated, preferred_element_type=jnp.float32)
    block_shape = (NBLK, BLOCK, GROUPS, HPG, HEAD_DIM)
    grad_y = (back_proj * gate_act).reshape(block_shape)
    inputs_x = values.astype(jnp.float32).reshape(block_shape)
    log_rate = log_decay.T.reshape(NBLK, BLOCK, GROUPS, HPG)
    write_rows = write_keys.astype(jnp.float32).reshape(NBLK, BLOCK, GROUPS, STATE)
    read_rows = read_keys.astype(jnp.float32).reshape(NBLK, BLOCK, GROUPS, STATE)
    start_states = entry_states.reshape(NBLK, GROUPS, HPG, HEAD_DIM, STATE)
    initial = jnp.zeros((GROUPS, HPG, HEAD_DIM, STATE), jnp.float32)
    final_state, outputs = lax.scan(block_back, initial, (inputs_x, grad_y, log_rate, write_rows, read_rows, start_states), reverse=True)
    grad_x, grad_w, grad_r = outputs
    d_values = grad_x.reshape(TOKENS, D_INNER).astype(jnp.bfloat16)
    d_write = grad_w.reshape(TOKENS, GROUPS * STATE)
    d_read = grad_r.reshape(TOKENS, GROUPS * STATE)
    return (grad_wg, grad_wu, grad_down, d_out_weight, d_input, d_values, d_write, d_read, d_gate)
```

```python
import jax
import jax.numpy as jnp
from jax import lax
from jax.sharding import Mesh
from jax.sharding import PartitionSpec as P

D = 2048
HEAD_DIM = 64
BLOCK = 128
TOPK = 2
TOK_DEV = 128
SP = ("sp_0", "sp_1")


precise = lax.Precision.HIGHEST


def sent_together(arrays, axis, split_dim, concat_dim, along):
    widths = [a.shape[along] for a in arrays]
    both = jnp.concatenate(arrays, axis=along)
    out = lax.all_to_all(both, axis, split_axis=split_dim, concat_axis=concat_dim, tiled=True)
    return tuple(jnp.split(out, [sum(widths[:k]) for k in range(1, len(widths))], axis=along))


def in_one_piece(arrays, axis, dim, along):
    widths = [a.shape[along] for a in arrays]
    both = jnp.concatenate(arrays, axis=along)
    out = lax.all_gather(both, axis, axis=dim, tiled=True)
    return tuple(jnp.split(out, [sum(widths[:k]) for k in range(1, len(widths))], axis=along))


def split_up(value, dim, count):
    before, after = (value.shape[:dim], value.shape[dim + 1 :])
    return jnp.moveaxis(value.reshape(*before, count, -1, *after), dim, 0)


def sent_and_summed(value, axis, dim):
    count = lax.axis_size(axis)
    parts = lax.all_to_all(split_up(value, dim, count), axis, 0, 0, tiled=True)
    return jnp.sum(parts.astype(jnp.float32), axis=0)


def three_parts(value):
    first = lax.reduce_precision(value, 8, 7)
    second = lax.reduce_precision(value - first, 8, 7)
    third = value - first - second
    return jnp.stack([first, second, third]).astype(jnp.bfloat16)


def later_states(shard_grad, logs):
    sp_count = lax.axis_size(SP)
    mine = lax.axis_index(SP)
    heads = shard_grad.shape[0]
    pieces = shard_grad.reshape(sp_count, -1, shard_grad.shape[-1])
    received = lax.all_to_all(pieces, SP, 0, 0, tiled=True)
    head = mine * heads // sp_count
    own = lax.dynamic_index_in_dim(logs, head, 1, keepdims=False)
    through = jnp.cumsum(own)
    before = through - own
    span = before[None, :] - through[:, None]
    later = jnp.arange(sp_count)[None, :] > jnp.arange(sp_count)[:, None]
    weights = jnp.where(later, jnp.exp(jnp.where(later, span, 0.0)), 0.0)
    flat = received.reshape(sp_count, -1)
    summed = jnp.dot(weights, flat, precision=precise).reshape(received.shape)
    back = lax.all_to_all(summed, SP, 0, 0, tiled=True)
    return back.reshape(shard_grad.shape)


def silu_grad(pre_act):
    logistic = jax.nn.sigmoid(pre_act)
    return logistic * (1.0 + pre_act * (1.0 - logistic))


def contract_rows(first_op, second_op):
    return lax.dot_general(
        first_op, second_op, (((0,), (0,)), ((), ())), preferred_element_type=jnp.float32
    )


def contract_cols(first_op, second_op):
    return lax.dot_general(
        first_op, second_op, (((1,), (1,)), ((), ())), preferred_element_type=jnp.float32
    )


def block_back(grad_state, inputs_x, grad_y, log_rate, write_rows, read_rows, start_state):
    block_len = log_rate.shape[0]
    running = jnp.cumsum(log_rate, axis=0)
    causal_mask = (jnp.arange(block_len)[:, None] >= jnp.arange(block_len)[None, :])[:, :, None]
    spread = running[:, None, :] - running[None, :, :]
    decay_mat = jnp.where(causal_mask, jnp.exp(jnp.where(causal_mask, spread, 0.0)), 0.0)
    intersection = jnp.dot(read_rows, write_rows.T, precision=precise)
    mixing = intersection[:, :, None] * decay_mat
    to_end = jnp.exp(running[-1][None, :] - running)
    from_start = jnp.exp(running)
    grad_x = jnp.einsum("lsj,ljp->sjp", mixing, grad_y, precision=precise) + to_end[
        :, :, None
    ] * jnp.einsum("sn,jpn->sjp", write_rows, grad_state, precision=precise)
    weighted = jnp.einsum("ljp,sjp->lsj", grad_y, inputs_x, precision=precise) * decay_mat
    grad_w = jnp.einsum("lsj,ln->sn", weighted, read_rows, precision=precise) + jnp.einsum(
        "sj,sjp,jpn->sn", to_end, inputs_x, grad_state, precision=precise
    )
    grad_r = jnp.einsum("lsj,sn->ln", weighted, write_rows, precision=precise) + jnp.einsum(
        "lj,ljp,jpn->ln", from_start, grad_y, start_state, precision=precise
    )
    earlier = jnp.exp(running[-1])[:, None, None] * grad_state + jnp.einsum(
        "lj,ljp,ln->jpn", from_start, grad_y, read_rows, precision=precise
    )
    return (earlier, grad_x, grad_w, grad_r)


def body(
    mixed,
    cotangent,
    routes,
    gates,
    w_gate,
    w_up,
    w_down,
    out_weight,
    gate_pre,
    mixer_out,
    values,
    write_keys,
    read_keys,
    log_decay,
    entry_states,
):
    sp_count = lax.axis_size(SP)
    tp_count = lax.axis_size("tp")
    capacity = 4 * TOK_DEV // sp_count
    assigned = TOK_DEV * TOPK
    picks = routes.reshape(assigned)
    onehot = (picks[:, None] == jnp.arange(sp_count, dtype=jnp.int32)[None, :]).astype(jnp.int32)
    earlier_same = jnp.cumsum(onehot, axis=0) - onehot
    slot_of = jnp.sum(earlier_same * onehot, axis=1)
    target = picks * capacity + slot_of
    anchor = (
        jnp.full((sp_count * capacity,), assigned, jnp.int32)
        .at[target]
        .set(jnp.arange(assigned, dtype=jnp.int32))
    )
    weight_g = w_gate[0]
    weight_u = w_up[0]
    weight_d = w_down[0]
    column_count = D // tp_count
    offset = lax.axis_index("tp") * column_count
    tok_slice = lax.dynamic_slice_in_dim(mixed, offset, column_count, 1)
    cot_slice = lax.dynamic_slice_in_dim(cotangent, offset, column_count, 1)
    columns = tok_slice.shape[1]
    scaled = (
        (gates[:, :, None] * cot_slice[:, None, :].astype(jnp.float32))
        .astype(jnp.bfloat16)
        .reshape(assigned, columns)
    )
    empty_row = jnp.zeros((1, columns), jnp.bfloat16)
    cot_buffer = jnp.concatenate([scaled, empty_row])[anchor].reshape(sp_count, capacity, columns)
    tok_buffer = jnp.concatenate([tok_slice, empty_row])[anchor // TOPK].reshape(
        sp_count, capacity, columns
    )
    tok_buffer, cot_buffer = (tok_buffer, cot_buffer)
    tok_part, cot_part = sent_together((tok_buffer, cot_buffer), SP, 0, 0, 1)
    tok_rows, cot_rows = in_one_piece((tok_part, cot_part), "tp", 2, 0)
    expert_tok_rows = tok_rows
    expert_cot_rows = cot_rows
    expert_tok_rows = expert_tok_rows.reshape(-1, D)
    expert_cot_rows = expert_cot_rows.reshape(-1, D)
    pre_gate = jnp.dot(expert_tok_rows, weight_g, preferred_element_type=jnp.float32)
    pre_up = jnp.dot(expert_tok_rows, weight_u, preferred_element_type=jnp.float32)
    active = jax.nn.silu(pre_gate)
    hidden = (active * pre_up).astype(jnp.bfloat16)
    grad_down = contract_rows(hidden, expert_cot_rows)
    grad_hidden = contract_cols(expert_cot_rows, weight_d)
    grad_gate = (grad_hidden * pre_up * silu_grad(pre_gate)).astype(jnp.bfloat16)
    grad_upval = (grad_hidden * active).astype(jnp.bfloat16)
    grad_wg = contract_rows(expert_tok_rows, grad_gate)
    grad_wu = contract_rows(expert_tok_rows, grad_upval)
    partial_value = contract_cols(grad_gate, weight_g) + contract_cols(grad_upval, weight_u)
    grad_wg, grad_wu, grad_down, partial_value = (grad_wg, grad_wu, grad_down, partial_value)
    row_total = partial_value.shape[0]
    pieces = partial_value.astype(jnp.bfloat16).reshape(row_total, tp_count, column_count)
    received = lax.all_to_all(pieces, "tp", split_axis=1, concat_axis=1, tiled=True)
    summed = (
        jnp.sum(received.astype(jnp.float32), axis=1)
        .astype(jnp.bfloat16)
        .reshape(sp_count, capacity, column_count)
    )
    head_count = out_weight.shape[0] // HEAD_DIM
    parts = three_parts(jnp.sum(log_decay, axis=1))
    extra = jnp.pad(parts, ((0, 5), (0, column_count - head_count)))
    extra = jnp.broadcast_to(extra[None], (sp_count, *extra.shape))
    both = lax.all_to_all(jnp.concatenate([summed, extra], axis=1), SP, 0, 0, tiled=True)
    returned = both[:, :capacity]
    logs = jnp.sum(both[:, capacity : capacity + 3, :head_count].astype(jnp.float32), axis=1)
    columns = returned.shape[-1]
    picked = returned.reshape(sp_count * capacity, columns)[target].reshape(TOK_DEV, TOPK, columns)
    d_input = (cot_slice.astype(jnp.float32) + jnp.sum(picked.astype(jnp.float32), axis=1)).astype(
        jnp.bfloat16
    )
    whole = lax.all_gather(d_input, "tp", axis=1, tiled=True)
    back_proj = contract_cols(whole, out_weight)
    pre_act = gate_pre.astype(jnp.float32)
    gate_act = jax.nn.silu(pre_act)
    saved_out = mixer_out.astype(jnp.float32)
    d_gate = (back_proj * saved_out * silu_grad(pre_act)).astype(jnp.bfloat16)
    gated = (saved_out * gate_act).astype(jnp.bfloat16)
    weight_part = contract_rows(whole, gated).astype(jnp.bfloat16)
    d_out_weight = sent_and_summed(weight_part, SP, 0)
    grad_y = (back_proj * gate_act).reshape(TOK_DEV, head_count, HEAD_DIM)
    inputs_x = values.astype(jnp.float32).reshape(TOK_DEV, head_count, HEAD_DIM)
    write_rows = write_keys.astype(jnp.float32)
    read_rows = read_keys.astype(jnp.float32)
    log_rate = log_decay.T
    total_run = jnp.cumsum(log_rate, axis=0)
    shard_grad = jnp.einsum(
        "lj,ljp,ln->jpn", jnp.exp(total_run), grad_y, read_rows, precision=precise
    )
    grad_state = later_states(shard_grad, logs)
    pieces_x = []
    pieces_w = []
    pieces_r = []
    for block_id in reversed(range(TOK_DEV // BLOCK)):
        grad_state, grad_x, grad_w, grad_r = block_back(
            grad_state, inputs_x, grad_y, log_rate, write_rows, read_rows, entry_states[block_id]
        )
        pieces_x.insert(0, grad_x)
        pieces_w.insert(0, grad_w)
        pieces_r.insert(0, grad_r)
    d_values = pieces_x[0].reshape(TOK_DEV, head_count * HEAD_DIM).astype(jnp.bfloat16)
    d_write = pieces_w[0]
    d_read = pieces_r[0]
    return (
        grad_wg.astype(jnp.bfloat16)[None],
        grad_wu.astype(jnp.bfloat16)[None],
        grad_down.astype(jnp.bfloat16)[None],
        d_out_weight,
        d_input,
        d_values,
        d_write,
        d_read,
        d_gate,
    )


def solution(mesh):
    finer = Mesh(mesh.devices.reshape(8, 4, mesh.shape["tp"]), ("sp_0", "sp_1", "tp"))
    return jax.shard_map(
        body,
        mesh=finer,
        in_specs=(
            P(SP, None),
            P(SP, None),
            P(SP, None),
            P(SP, None),
            P(SP, None, "tp"),
            P(SP, None, "tp"),
            P(SP, "tp", None),
            P("tp", None),
            P(SP, "tp"),
            P(SP, "tp"),
            P(SP, "tp"),
            P(SP, "tp"),
            P(SP, "tp"),
            P("tp", SP),
            P(SP, "tp", None, None),
        ),
        out_specs=(
            P(SP, None, "tp"),
            P(SP, None, "tp"),
            P(SP, "tp", None),
            P(SP, "tp"),
            P(SP, "tp"),
            P(SP, "tp"),
            P(SP, "tp"),
            P(SP, "tp"),
            P(SP, "tp"),
        ),
        check_vma=False,
    )
```

```python
import jax
import jax.numpy as jnp
from jax import lax
from jax.experimental import pallas as pl
from jax.experimental.pallas import tpu as pltpu
from jax.sharding import Mesh
from jax.sharding import PartitionSpec as P

D = 2048
TOK = 128
EXP = 32
CAP = 16
ROWS = EXP * CAP
QUART = 512
HALF = 1024
FF = 64
HEADS = 4
HD = 64
STATE = 128
SP = ("z", "x")
TP = ("y", "core")
BF = jnp.bfloat16
F32 = jnp.float32


def iota(shape, dim):
    return lax.broadcasted_iota(jnp.int32, shape, dim)


def mm(a, b, precision=None):
    return lax.dot_general(a, b, (((1,), (0,)), ((), ())), precision=precision, preferred_element_type=F32)


def mm_nt(a, b):
    return lax.dot_general(a, b, (((1,), (1,)), ((), ())), preferred_element_type=F32)


def columns(row):
    return jnp.broadcast_to(row, (8, row.shape[1])).T[:, 0:1]


def vmem():
    return pl.BlockSpec(memory_space=pltpu.VMEM)


def smem():
    return pl.BlockSpec(memory_space=pltpu.SMEM)


def call(kernel, name, outs, specs, args, flops=0):
    return pl.pallas_call(
        kernel,
        out_shape=outs,
        in_specs=specs,
        out_specs=jax.tree.map(lambda _: vmem(), outs),
        compiler_params=pltpu.CompilerParams(vmem_limit_bytes=48 * 1024 * 1024),
        cost_estimate=pl.CostEstimate(flops=flops, bytes_accessed=0, transcendentals=0),
        name=name,
    )(*args)


def prepare_kernel(where, routes, gates, mix, cot, buf, target):
    picks = routes[...]
    expert = iota((EXP, TOK), 0)
    hits = [expert == picks[k : k + 1] for k in range(2)]
    both = jnp.where(hits[0] | hits[1], 1.0, 0.0).astype(BF)
    before = jnp.where(iota((TOK, TOK), 0) < iota((TOK, TOK), 1), 1.0, 0.0).astype(BF)
    count = mm(both, before)
    row = iota((ROWS, TOK), 0)
    cots = cot[...].astype(F32)
    places, scaled, rows = [], [], []
    for k in range(2):
        slot = jnp.sum(jnp.where(hits[k], count, 0.0), axis=0, keepdims=True)
        place = picks[k : k + 1] * CAP + slot.astype(jnp.int32)
        rows.append(place)
        places.append(jnp.where(row == place, 1.0, 0.0).astype(BF))
        scaled.append((columns(gates[k : k + 1, :]) * cots).astype(BF))
    target[...] = jnp.concatenate(rows + [jnp.zeros((6, TOK), jnp.int32)], axis=0)
    toks = mm(places[0] + places[1], mix[...]).astype(BF)
    buf[:, 0:CAP, :] = toks.reshape(EXP, CAP, QUART)
    spread = mm(jnp.concatenate(places, axis=1), jnp.concatenate(scaled, axis=0)).astype(BF)
    buf[:, CAP : 2 * CAP, :] = spread.reshape(EXP, CAP, QUART)


def prepare(quarter, routes, gates, mixed, cotangent):
    whole = lambda i, q: (0, 0)
    part = lambda i, q: (0, q[0])
    return pl.pallas_call(
        prepare_kernel,
        out_shape=(
            jax.ShapeDtypeStruct((EXP, 2 * CAP, QUART), BF),
            jax.ShapeDtypeStruct((8, TOK), jnp.int32),
        ),
        grid_spec=pltpu.PrefetchScalarGridSpec(
            num_scalar_prefetch=1,
            grid=(1,),
            in_specs=[
                pl.BlockSpec((2, TOK), whole),
                pl.BlockSpec((2, TOK), whole),
                pl.BlockSpec((TOK, QUART), part),
                pl.BlockSpec((TOK, QUART), part),
            ],
            out_specs=(
                pl.BlockSpec((EXP, 2 * CAP, QUART), lambda i, q: (0, 0, 0)),
                pl.BlockSpec((8, TOK), whole),
            ),
        ),
        name="prepare",
    )(quarter, routes, gates, mixed, cotangent)


def row_blocks(chunk):
    toks = chunk[:, 0:CAP, :].reshape(ROWS, QUART)
    cots = chunk[:, CAP : 2 * CAP, :].reshape(ROWS, QUART)
    return toks, cots


def expert_kernel(where, c0, c1, c2, c3, own, other, out, g_gate, g_up, g_hid):
    quarter = where[0]
    core = where[1]
    pre = jnp.zeros((ROWS, 4 * FF), F32)
    grad_hidden = jnp.zeros((ROWS, 2 * FF), F32)
    for k, chunk in enumerate((c0, c1, c2, c3)):
        at = pl.ds(pl.multiple_of((quarter ^ k) * QUART, QUART), QUART)
        toks, cots = row_blocks(chunk)
        up_gate = jnp.concatenate([own[0, :, at], other[0, :, at], own[1, :, at], other[1, :, at]], axis=0)
        pre = pre + mm_nt(toks, up_gate)
        grad_hidden = grad_hidden + mm_nt(cots, jnp.concatenate([own[2, :, at], other[2, :, at]], axis=0))
    pre_gate = pre[:, : 2 * FF]
    pre_up = pre[:, 2 * FF :]
    logistic = 1.0 / (1.0 + jnp.exp(-pre_gate))
    active = pre_gate * logistic
    slope = logistic * (1.0 + pre_gate * (1.0 - logistic))
    gate = (grad_hidden * pre_up * slope).astype(BF)
    up = (grad_hidden * active).astype(BF)
    g_gate[...] = gate
    g_up[...] = up
    g_hid[...] = (active * pre_up).astype(BF)
    grads = jnp.concatenate([gate, up], axis=1)
    for k in range(8):
        at = pl.ds(pl.multiple_of((2 * k + core) * TOK, TOK), TOK)
        block = jnp.concatenate([own[0, :, at], other[0, :, at], own[1, :, at], other[1, :, at]], axis=0)
        part = mm(grads, block).astype(BF)
        out[:, :, k * TOK : (k + 1) * TOK] = part.reshape(EXP, CAP, TOK)


def weights_kernel(where, c0, c1, c2, c3, g_gate, g_up, g_hid, d_gate, d_up, d_down):
    quarter = where[0]
    gates = jnp.concatenate([g_gate[...].T[:FF], g_up[...].T[:FF]], axis=0)
    hidden = g_hid[...].T[:FF]
    for k, chunk in enumerate((c0, c1, c2, c3)):
        at = pl.ds(pl.multiple_of((quarter ^ k) * QUART, QUART), QUART)
        toks, cots = row_blocks(chunk)
        both = mm(gates, toks).astype(BF)
        d_gate[:, at] = both[:FF]
        d_up[:, at] = both[FF:]
        d_down[:, at] = mm(hidden, cots).astype(BF)


def combine_kernel(target, rows, out):
    lane = iota((TOK, ROWS), 1)
    places = target[...].T
    pick = jnp.where((lane == places[:, 0:1]) | (lane == places[:, 1:2]), 1.0, 0.0).astype(BF)
    total = mm(pick, rows[...].reshape(ROWS, HALF)).astype(BF)
    for k in range(8):
        out[k] = total[:, k * TOK : (k + 1) * TOK]


def project_kernel(whole, weight, gate_pre, mixer, logs, read, d_gate, gated, grad_y, run, buf):
    back = mm_nt(whole[...], weight[...])
    pre = gate_pre[...].astype(F32)
    saved = mixer[...].astype(F32)
    logistic = 1.0 / (1.0 + jnp.exp(-pre))
    active = pre * logistic
    d_gate[...] = (back * saved * (logistic * (1.0 + pre * (1.0 - logistic)))).astype(BF)
    gated[...] = (saved * active).astype(BF)
    grad = back * active
    grad_y[...] = grad.astype(BF)
    upto = jnp.where(iota((TOK, TOK), 0) <= iota((TOK, TOK), 1), 1.0, 0.0)
    rates = jnp.concatenate([logs[...], jnp.zeros((4, TOK), F32)], axis=0)
    running = mm(rates, upto, lax.Precision.HIGHEST)
    run[...] = running
    start = jnp.exp(running)
    turned = grad.T
    scale = jnp.concatenate([jnp.broadcast_to(start[j : j + 1], (HD, TOK)) for j in range(HEADS)], axis=0)
    state = mm((turned * scale).astype(BF), read[...])
    total = running[0:HEADS, TOK - 1 : TOK]
    first = total.astype(BF).astype(F32)
    second = (total - first).astype(BF).astype(F32)
    third = total - first - second
    line = iota((8, STATE), 0)
    notes = []
    for j in range(HEADS):
        note = jnp.where(line == 0, first[j : j + 1], jnp.where(line == 1, second[j : j + 1], third[j : j + 1]))
        note = jnp.where(line < 3, note, 0.0)
        notes.append(jnp.broadcast_to(note[None], (EXP // HEADS, 8, STATE)))
    sent = jnp.concatenate([state.reshape(EXP, 8, STATE), jnp.concatenate(notes, axis=0)], axis=1)
    buf[...] = sent.astype(BF)


def scan_kernel(received, out):
    state = jnp.zeros((8, STATE), F32)
    for k in reversed(range(EXP)):
        out[k] = state.astype(BF)
        if k > 0:
            piece = received[k].astype(F32)
            log = piece[8:9] + piece[9:10] + piece[10:11]
            state = jnp.exp(log) * state + piece[0:8]


def inner_kernel(grad_y, values, write, read, run, entry, dx, dw, dr):
    running = run[...]
    cols = running.T
    grads = grad_y[...]
    vals = values[...]
    cross = mm_nt(write[...], read[...])
    later = iota((TOK, TOK), 1) >= iota((TOK, TOK), 0)
    total = jnp.zeros((TOK, TOK), F32)
    parts = []
    starts = []
    for j in range(HEADS):
        spread = running[j : j + 1] - cols[:, j : j + 1]
        decay = jnp.where(later, jnp.exp(jnp.where(later, spread, 0.0)), 0.0)
        grad = grads[:, j * HD : (j + 1) * HD]
        parts.append(mm((cross * decay).astype(BF), grad))
        total = total + mm_nt(vals[:, j * HD : (j + 1) * HD], grad) * decay
        starts.append((grad.astype(F32) * jnp.exp(cols[:, j : j + 1])).astype(BF))
    dx[...] = jnp.concatenate(parts, axis=1)
    dw[...] = mm(total.astype(BF), read[...])
    entry_rows = entry[...].reshape(HEADS * HD, STATE).astype(BF)
    dr[...] = mm(total.T.astype(BF), write[...]) + mm(jnp.concatenate(starts, axis=1), entry_rows)


def outer_kernel(dx, dw, values, write, run, state, d_values, d_write):
    running = run[...]
    ends = jnp.exp(running[:, TOK - 1 : TOK] - running).T
    scale = jnp.concatenate([jnp.broadcast_to(ends[:, j : j + 1], (TOK, HD)) for j in range(HEADS)], axis=1)
    later = state[...].reshape(HEADS * HD, STATE)
    d_values[...] = (dx[...] + scale * mm_nt(write[...], later)).astype(BF)
    d_write[...] = dw[...] + mm((values[...].astype(F32) * scale).astype(BF), later)


def body(mixed, cotangent, routes, gates, w_gate, w_up, w_down, out_weight, gate_pre, mixer_out, values,
         write_keys, read_keys, log_decay, entry_states):
    shape = jax.ShapeDtypeStruct
    y = lax.axis_index("y")
    core = lax.axis_index("core")
    swap = [(0, 1), (1, 0)]
    ring = []
    for k in range(8):
        ring.append((2 * k, 2 * ((k + 1) % 8)))
        ring.append((2 * k + 1, 2 * ((k - 1) % 8) + 1))
    quarter = 2 * (y % 2) + core
    where = jnp.stack([quarter, core]).astype(jnp.int32)
    own = jnp.stack([w_gate[0].T, w_up[0].T, w_down[0]])
    other = lax.ppermute(own, "core", swap)
    buf, target = prepare(where, routes.T, gates.T, mixed, cotangent)
    c0 = lax.all_to_all(buf, SP, 0, 0, tiled=True)
    c2 = lax.ppermute(c0, TP, ring)
    c1 = lax.ppermute(c0, "core", swap)
    c3 = lax.ppermute(c2, "core", swap)
    chunks = (c0, c1, c2, c3)
    grad = shape((ROWS, 2 * FF), BF)
    parts, g_gate, g_up, g_hid = call(
        expert_kernel, "expert", (shape((EXP, CAP, HALF), BF), grad, grad, grad),
        [smem()] + [vmem()] * 6, (where, *chunks, own, other))
    back = lax.all_to_all(parts, SP, 0, 0, tiled=True)
    wide = shape((FF, D), BF)
    d_wg, d_wu, d_wd = call(
        weights_kernel, "weights", (wide, wide, wide),
        [smem()] + [vmem()] * 7, (where, *chunks, g_gate, g_up, g_hid), flops=10**9)
    summed = call(combine_kernel, "combine", shape((8, TOK, TOK), BF), [vmem()] * 2, (target, back))
    pieces = lax.all_to_all(summed, "y", 0, 0, tiled=True)
    offset = (2 * y + core) * TOK
    cot_slice = lax.dynamic_slice_in_dim(cotangent, offset, TOK, 1).astype(F32)
    d_input = (cot_slice + jnp.sum(pieces.astype(F32), axis=0)).astype(BF)
    whole = lax.all_gather(d_input, TP, axis=1, tiled=True)
    flat = shape((TOK, HEADS * HD), BF)
    d_gate, gated, grad_y, run, sent = call(
        project_kernel, "project",
        (flat, flat, flat, shape((8, TOK), F32), shape((EXP, 16, STATE), BF)),
        [vmem()] * 6, (whole, out_weight, gate_pre, mixer_out, log_decay, read_keys))
    received = lax.all_to_all(sent, SP, 0, 0, tiled=True)
    part = lax.dot_general(whole, gated, (((0,), (0,)), ((), ())), preferred_element_type=F32).astype(BF)
    shares = lax.all_to_all(part.reshape(EXP, D // EXP, HEADS * HD), SP, 0, 0, tiled=True)
    states = call(scan_kernel, "scan", shape((EXP, 8, STATE), BF), [vmem()], (received,))
    later = lax.all_to_all(states, SP, 0, 0, tiled=True)
    square = shape((TOK, STATE), F32)
    dx, dw, d_read = call(
        inner_kernel, "inner", (shape((TOK, HEADS * HD), F32), square, square),
        [vmem()] * 6, (grad_y, values, write_keys, read_keys, run, entry_states[0]), flops=10**9)
    d_values, d_write = call(
        outer_kernel, "outer", (flat, square), [vmem()] * 6,
        (dx, dw, values, write_keys, run, later))
    d_out_weight = jnp.sum(shares.astype(F32), axis=0)
    return (d_wg.T[None], d_wu.T[None], d_wd[None], d_out_weight, d_input, d_values, d_write, d_read, d_gate)


def solution(mesh):
    finer = Mesh(mesh.devices.reshape(8, 4, 8, 2), ("z", "x", "y", "core"))
    return jax.shard_map(
        body,
        mesh=finer,
        in_specs=(
            P(SP, None),
            P(SP, None),
            P(SP, None),
            P(SP, None),
            P(SP, None, TP),
            P(SP, None, TP),
            P(SP, TP, None),
            P(TP, None),
            P(SP, TP),
            P(SP, TP),
            P(SP, TP),
            P(SP, TP),
            P(SP, TP),
            P(TP, SP),
            P(SP, TP, None, None),
        ),
        out_specs=(
            P(SP, None, TP),
            P(SP, None, TP),
            P(SP, TP, None),
            P(SP, TP),
            P(SP, TP),
            P(SP, TP),
            P(SP, TP),
            P(SP, TP),
            P(SP, TP),
        ),
        check_vma=False,
    )
```

```python
import jax
import jax.numpy as jnp
from jax import lax
from jax.experimental import pallas as pl
from jax.experimental.pallas import tpu as pltpu
from jax.sharding import Mesh
from jax.sharding import PartitionSpec as P

D = 2048
TOK = 128
EXP = 32
CAP = 16
ROWS = EXP * CAP
WIDE = 256
FF = 64
HEADS = 4
HD = 64
STATE = 128
SP = ("z", "x")
TP = ("y", "core")
BF = jnp.bfloat16
F32 = jnp.float32


def iota(shape, dim):
    return lax.broadcasted_iota(jnp.int32, shape, dim)


def mm(a, b, precision=None):
    return lax.dot_general(a, b, (((1,), (0,)), ((), ())), precision=precision, preferred_element_type=F32)


def mm_nt(a, b):
    return lax.dot_general(a, b, (((1,), (1,)), ((), ())), preferred_element_type=F32)


def columns(row):
    return jnp.broadcast_to(row, (8, row.shape[1])).T[:, 0:1]


def vmem():
    return pl.BlockSpec(memory_space=pltpu.VMEM)


def smem():
    return pl.BlockSpec(memory_space=pltpu.SMEM)


def call(kernel, outs, specs, args, flops=0):
    return pl.pallas_call(
        kernel,
        out_shape=outs,
        in_specs=specs,
        out_specs=jax.tree.map(lambda _: vmem(), outs),
        compiler_params=pltpu.CompilerParams(vmem_limit_bytes=20 * 1024 * 1024),
        cost_estimate=pl.CostEstimate(flops=flops, bytes_accessed=0, transcendentals=0),
    )(*args)


def prepare_kernel(where, routes, gates, mix, cot, buf, target):
    picks = routes[...]
    expert = iota((EXP, TOK), 0)
    hits = [expert == picks[k : k + 1] for k in range(2)]
    both = jnp.where(hits[0] | hits[1], 1.0, 0.0).astype(BF)
    before = jnp.where(iota((TOK, TOK), 0) < iota((TOK, TOK), 1), 1.0, 0.0).astype(BF)
    count = mm(both, before)
    row = iota((ROWS, TOK), 0)
    cots = cot[...].astype(F32)
    places, scaled, rows = [], [], []
    for k in range(2):
        slot = jnp.sum(jnp.where(hits[k], count, 0.0), axis=0, keepdims=True)
        place = picks[k : k + 1] * CAP + slot.astype(jnp.int32)
        rows.append(place)
        places.append(jnp.where(row == place, 1.0, 0.0).astype(BF))
        scaled.append((columns(gates[k : k + 1, :]) * cots).astype(BF))
    target[...] = jnp.concatenate(rows + [jnp.zeros((6, TOK), jnp.int32)], axis=0)
    toks = mm(places[0] + places[1], mix[...]).astype(BF)
    buf[:, 0:CAP, :] = toks.reshape(EXP, CAP, WIDE)
    spread = mm(jnp.concatenate(places, axis=1), jnp.concatenate(scaled, axis=0)).astype(BF)
    buf[:, CAP : 2 * CAP, :] = spread.reshape(EXP, CAP, WIDE)


def prepare(quarter, routes, gates, mixed, cotangent):
    whole = lambda i, q: (0, 0)
    part = lambda i, q: (0, q[0])
    return pl.pallas_call(
        prepare_kernel,
        out_shape=(
            jax.ShapeDtypeStruct((EXP, 2 * CAP, WIDE), BF),
            jax.ShapeDtypeStruct((8, TOK), jnp.int32),
        ),
        grid_spec=pltpu.PrefetchScalarGridSpec(
            num_scalar_prefetch=1,
            grid=(1,),
            in_specs=[
                pl.BlockSpec((2, TOK), whole),
                pl.BlockSpec((2, TOK), whole),
                pl.BlockSpec((TOK, WIDE), part),
                pl.BlockSpec((TOK, WIDE), part),
            ],
            out_specs=(
                pl.BlockSpec((EXP, 2 * CAP, WIDE), lambda i, q: (0, 0, 0)),
                pl.BlockSpec((8, TOK), whole),
            ),
        ),
        name="prepare",
    )(quarter, routes, gates, mixed, cotangent)


def row_blocks(chunk):
    toks = chunk[:, 0:CAP, :].reshape(ROWS, WIDE)
    cots = chunk[:, CAP : 2 * CAP, :].reshape(ROWS, WIDE)
    return toks, cots


def gate_rows(own, other, at):
    return jnp.concatenate([own[0, :, at], other[0, :, at], own[1, :, at], other[1, :, at]], axis=0)


def expert_kernel(where, *refs):
    chunks = refs[:8]
    own, other, out, g_gate, g_up, g_hid = refs[8:]
    core = where[8]
    pre = jnp.zeros((ROWS, 4 * FF), F32)
    grad_hidden = jnp.zeros((ROWS, 2 * FF), F32)
    for k in range(8):
        at = pl.ds(pl.multiple_of(where[k] * WIDE, WIDE), WIDE)
        toks, cots = row_blocks(chunks[k])
        pre = pre + mm_nt(toks, gate_rows(own, other, at))
        grad_hidden = grad_hidden + mm_nt(cots, jnp.concatenate([own[2, :, at], other[2, :, at]], axis=0))
    pre_gate = pre[:, : 2 * FF]
    pre_up = pre[:, 2 * FF :]
    logistic = 1.0 / (1.0 + jnp.exp(-pre_gate))
    active = pre_gate * logistic
    slope = logistic * (1.0 + pre_gate * (1.0 - logistic))
    gate = (grad_hidden * pre_up * slope).astype(BF)
    up = (grad_hidden * active).astype(BF)
    g_gate[...] = gate
    g_up[...] = up
    g_hid[...] = (active * pre_up).astype(BF)
    grads = jnp.concatenate([gate, up], axis=1)
    for k in range(8):
        at = pl.ds(pl.multiple_of((2 * k + core) * TOK, TOK), TOK)
        out[k] = mm(grads, gate_rows(own, other, at)).astype(BF)


def weights_kernel(where, *refs):
    chunks = refs[:8]
    g_gate, g_up, g_hid, d_gate, d_up, d_down = refs[8:]
    gates = jnp.concatenate([g_gate[...].T[:FF], g_up[...].T[:FF]], axis=0)
    hidden = g_hid[...].T[:FF]
    for k in range(8):
        at = pl.ds(pl.multiple_of(where[k] * WIDE, WIDE), WIDE)
        toks, cots = row_blocks(chunks[k])
        both = mm(gates, toks).astype(BF)
        d_gate[:, at] = both[:FF]
        d_up[:, at] = both[FF:]
        d_down[:, at] = mm(hidden, cots).astype(BF)


def combine_kernel(where, target, rows, cot, out):
    lane = iota((TOK, ROWS), 1)
    places = target[...].T
    pick = jnp.where((lane == places[:, 0:1]) | (lane == places[:, 1:2]), 1.0, 0.0).astype(BF)
    out[...] = (cot[...].astype(F32) + mm(pick, rows[...].reshape(ROWS, TOK))).astype(BF)


def combine(slot, target, rows, cotangent):
    return pl.pallas_call(
        combine_kernel,
        out_shape=jax.ShapeDtypeStruct((TOK, TOK), BF),
        grid_spec=pltpu.PrefetchScalarGridSpec(
            num_scalar_prefetch=1,
            grid=(1,),
            in_specs=[
                pl.BlockSpec((8, TOK), lambda i, q: (0, 0)),
                pl.BlockSpec((EXP, CAP, TOK), lambda i, q: (0, 0, 0)),
                pl.BlockSpec((TOK, TOK), lambda i, q: (0, q[0])),
            ],
            out_specs=pl.BlockSpec((TOK, TOK), lambda i, q: (0, 0)),
        ),
        name="combine",
    )(slot, target, rows, cotangent)


def project_kernel(whole, weight, gate_pre, mixer, logs, read, d_gate, grad_y, run, buf):
    back = mm_nt(whole[...], weight[...])
    pre = gate_pre[...].astype(F32)
    saved = mixer[...].astype(F32)
    logistic = 1.0 / (1.0 + jnp.exp(-pre))
    active = pre * logistic
    d_gate[...] = (back * saved * (logistic * (1.0 + pre * (1.0 - logistic)))).astype(BF)
    gated = (saved * active).astype(BF)
    for k in range(8):
        turned = whole[:, k * WIDE : (k + 1) * WIDE].T
        buf[4 * k : 4 * k + 4, 0:FF, :] = mm(turned, gated).astype(BF).reshape(4, FF, WIDE)
    grad = back * active
    grad_y[...] = grad.astype(BF)
    upto = jnp.where(iota((TOK, TOK), 0) <= iota((TOK, TOK), 1), 1.0, 0.0)
    rates = jnp.concatenate([logs[...], jnp.zeros((4, TOK), F32)], axis=0)
    running = mm(rates, upto, lax.Precision.HIGHEST)
    run[...] = running
    start = jnp.exp(running)
    turned = grad.T
    scale = jnp.concatenate([jnp.broadcast_to(start[j : j + 1], (HD, TOK)) for j in range(HEADS)], axis=0)
    state = mm((turned * scale).astype(BF), read[...])
    total = running[0:HEADS, TOK - 1 : TOK]
    first = total.astype(BF).astype(F32)
    second = (total - first).astype(BF).astype(F32)
    third = total - first - second
    line = iota((8, STATE), 0)
    notes = []
    for j in range(HEADS):
        note = jnp.where(line == 0, first[j : j + 1], jnp.where(line == 1, second[j : j + 1], third[j : j + 1]))
        note = jnp.where(line < 3, note, 0.0)
        notes.append(jnp.broadcast_to(note[None], (EXP // HEADS, 8, STATE)))
    buf[:, FF:, 0:STATE] = state.reshape(EXP, 8, STATE).astype(BF)
    buf[:, FF:, STATE:] = jnp.concatenate(notes, axis=0).astype(BF)


def scan_kernel(received, out):
    state = jnp.zeros((8, STATE), F32)
    for k in reversed(range(EXP)):
        out[k] = state.astype(BF)
        if k > 0:
            piece = received[k, FF:, :].astype(F32)
            note = piece[:, STATE:]
            log = note[0:1] + note[1:2] + note[2:3]
            state = jnp.exp(log) * state + piece[:, :STATE]


def inner_kernel(grad_y, values, write, read, run, entry, dx, dw, dr):
    running = run[...]
    cols = running.T
    grads = grad_y[...]
    vals = values[...]
    cross = mm_nt(write[...], read[...])
    later = iota((TOK, TOK), 1) >= iota((TOK, TOK), 0)
    total = jnp.zeros((TOK, TOK), F32)
    parts = []
    starts = []
    for j in range(HEADS):
        spread = running[j : j + 1] - cols[:, j : j + 1]
        decay = jnp.where(later, jnp.exp(jnp.where(later, spread, 0.0)), 0.0)
        grad = grads[:, j * HD : (j + 1) * HD]
        parts.append(mm((cross * decay).astype(BF), grad))
        total = total + mm_nt(vals[:, j * HD : (j + 1) * HD], grad) * decay
        starts.append((grad.astype(F32) * jnp.exp(cols[:, j : j + 1])).astype(BF))
    dx[...] = jnp.concatenate(parts, axis=1)
    dw[...] = mm(total.astype(BF), read[...])
    entry_rows = entry[...].reshape(HEADS * HD, STATE).astype(BF)
    dr[...] = mm(total.T.astype(BF), write[...]) + mm(jnp.concatenate(starts, axis=1), entry_rows)


def outer_kernel(dx, dw, values, write, run, state, d_values, d_write):
    running = run[...]
    ends = jnp.exp(running[:, TOK - 1 : TOK] - running).T
    scale = jnp.concatenate([jnp.broadcast_to(ends[:, j : j + 1], (TOK, HD)) for j in range(HEADS)], axis=1)
    later = state[...].reshape(HEADS * HD, STATE)
    d_values[...] = (dx[...] + scale * mm_nt(write[...], later)).astype(BF)
    d_write[...] = dw[...] + mm((values[...].astype(F32) * scale).astype(BF), later)


def step(mixed, cotangent, routes, gates, w_gate, w_up, w_down, out_weight, gate_pre, mixer_out, values,
         write_keys, read_keys, log_decay, entry_states):
    shape = jax.ShapeDtypeStruct
    y = lax.axis_index("y")
    core = lax.axis_index("core")
    swap = [(0, 1), (1, 0)]
    ring = []
    for k in range(8):
        ring.append((2 * k, 2 * ((k + 1) % 8)))
        ring.append((2 * k + 1, 2 * ((k - 1) % 8) + 1))
    turn = 2 * core - 1
    near, far, beyond = (y + turn) % 4, (y - turn) % 4, (y + 2) % 4
    mine, theirs = core, 1 - core
    home = 2 * (y % 4)
    ids = [home + mine, home + theirs, 2 * near + mine, 2 * near + theirs, 2 * beyond + mine,
           2 * far + theirs, 2 * far + mine, 2 * beyond + theirs, core]
    where = jnp.stack(ids).astype(jnp.int32)
    slot = (2 * y + core).astype(jnp.int32).reshape(1)
    own = jnp.stack([w_gate[0].T, w_up[0].T, w_down[0]])
    other = lax.ppermute(own, "core", swap)
    buf, target = prepare(where, routes.T, gates.T, mixed, cotangent)
    c0 = lax.all_to_all(buf, SP, 0, 0, tiled=True)
    c2 = lax.ppermute(c0, TP, ring)
    c1 = lax.ppermute(c0, "core", swap)
    c3 = lax.ppermute(c1, TP, ring)
    c4 = lax.ppermute(c2, TP, ring)
    moved, other = lax.optimization_barrier((c2, other))
    c5 = lax.ppermute(moved, "core", swap)
    c6 = lax.ppermute(c3, "core", swap)
    c7 = lax.ppermute(c4, "core", swap)
    chunks = (c0, c1, c2, c3, c4, c5, c6, c7)
    grad = shape((ROWS, 2 * FF), BF)
    parts, g_gate, g_up, g_hid = call(
        expert_kernel, (shape((8, ROWS, TOK), BF), grad, grad, grad),
        [smem()] + [vmem()] * 10, (where, *chunks, own, other))
    pieces = lax.all_to_all(parts, "y", 0, 0, tiled=True)
    wide = shape((FF, D), BF)
    d_wg, d_wu, d_wd = call(
        weights_kernel, (wide, wide, wide),
        [smem()] + [vmem()] * 11, (where, *chunks, g_gate, g_up, g_hid), flops=10**9)
    pieces, d_wg, d_wu, d_wd = lax.optimization_barrier((pieces, d_wg, d_wu, d_wd))
    summed = jnp.sum(pieces.astype(F32), axis=0).astype(BF).reshape(EXP, CAP, TOK)
    back = lax.all_to_all(summed, SP, 0, 0, tiled=True)
    d_input = combine(slot, target, back, cotangent)
    whole = lax.all_gather(d_input, TP, axis=1, tiled=True)
    flat = shape((TOK, HEADS * HD), BF)
    d_gate, grad_y, run, sent = call(
        project_kernel,
        (flat, flat, shape((8, TOK), F32), shape((EXP, FF + 8, WIDE), BF)),
        [vmem()] * 6, (whole, out_weight, gate_pre, mixer_out, log_decay, read_keys))
    received = lax.all_to_all(sent, SP, 0, 0, tiled=True)
    square = shape((TOK, STATE), F32)
    dx, dw, d_read = call(
        inner_kernel, (shape((TOK, HEADS * HD), F32), square, square),
        [vmem()] * 6, (grad_y, values, write_keys, read_keys, run, entry_states[0]), flops=10**9)
    received, dx, dw, d_read = lax.optimization_barrier((received, dx, dw, d_read))
    states = call(scan_kernel, shape((EXP, 8, STATE), BF), [vmem()], (received,))
    later = lax.all_to_all(states, SP, 0, 0, tiled=True)
    d_out_weight = jnp.sum(received[:, :FF].astype(F32), axis=0)
    later, d_out_weight = lax.optimization_barrier((later, d_out_weight))
    d_values, d_write = call(
        outer_kernel, (flat, square), [vmem()] * 6,
        (dx, dw, values, write_keys, run, later))
    return (d_wg.T[None], d_wu.T[None], d_wd[None], d_out_weight, d_input, d_values, d_write, d_read, d_gate)


def solution(mesh):
    finer = Mesh(mesh.devices.reshape(8, 4, 8, 2), ("z", "x", "y", "core"))
    return jax.shard_map(
        step,
        mesh=finer,
        in_specs=(
            P(SP, None),
            P(SP, None),
            P(SP, None),
            P(SP, None),
            P(SP, None, TP),
            P(SP, None, TP),
            P(SP, TP, None),
            P(TP, None),
            P(SP, TP),
            P(SP, TP),
            P(SP, TP),
            P(SP, TP),
            P(SP, TP),
            P(TP, SP),
            P(SP, TP, None, None),
        ),
        out_specs=(
            P(SP, None, TP),
            P(SP, None, TP),
            P(SP, TP, None),
            P(SP, TP),
            P(SP, TP),
            P(SP, TP),
            P(SP, TP),
            P(SP, TP),
            P(SP, TP),
        ),
        check_vma=False,
    )
```

```python
import jax
import jax.numpy as jnp
from jax import lax
from jax.experimental import pallas as pl
from jax.experimental.pallas import tpu as pltpu
from jax.sharding import Mesh
from jax.sharding import PartitionSpec as P

D = 2048
TOK = 128
EXP = 32
CAP = 16
ROWS = EXP * CAP
WIDE = 256
FF = 64
HEADS = 4
HD = 64
STATE = 128
SP = ("z", "x")
TP = ("y", "core")
BF = jnp.bfloat16
F32 = jnp.float32


def iota(shape, dim):
    return lax.broadcasted_iota(jnp.int32, shape, dim)


def mm(a, b, precision=None):
    return lax.dot_general(a, b, (((1,), (0,)), ((), ())), precision=precision, preferred_element_type=F32)


def mm_nt(a, b):
    return lax.dot_general(a, b, (((1,), (1,)), ((), ())), preferred_element_type=F32)


def mm_nt_exact(a, b):
    return lax.dot_general(a, b, (((1,), (1,)), ((), ())), precision=lax.Precision.HIGHEST, preferred_element_type=F32)


def mm_exact(a, b):
    return mm(a, b, lax.Precision.HIGHEST)


def two_parts(value):
    high = value.astype(BF)
    return high, (value - high.astype(F32)).astype(BF)


def chunk_ids(slot):
    y, core = slot >> 1, slot & 1
    turn = 2 * core - 1
    near, far, beyond, home = (y + turn) & 3, (y - turn) & 3, (y + 2) & 3, y & 3
    mine, theirs = core, 1 - core
    return (2 * home + mine, 2 * home + theirs, 2 * near + mine, 2 * near + theirs, 2 * beyond + mine,
            2 * far + theirs, 2 * far + mine, 2 * beyond + theirs)


def columns(row):
    return jnp.broadcast_to(row, (8, row.shape[1])).T[:, 0:1]


def vmem():
    return pl.BlockSpec(memory_space=pltpu.VMEM)


def smem():
    return pl.BlockSpec(memory_space=pltpu.SMEM)


def call(kernel, outs, specs, args, flops=0):
    return pl.pallas_call(
        kernel,
        out_shape=outs,
        in_specs=specs,
        out_specs=jax.tree.map(lambda _: vmem(), outs),
        compiler_params=pltpu.CompilerParams(vmem_limit_bytes=20 * 1024 * 1024),
        cost_estimate=pl.CostEstimate(flops=flops, bytes_accessed=0, transcendentals=0),
    )(*args)


def prepare_kernel(where, routes, gates, mix, cot, buf, target):
    picks = routes[...]
    expert = iota((EXP, TOK), 0)
    hits = [expert == picks[k : k + 1] for k in range(2)]
    both = jnp.where(hits[0] | hits[1], 1.0, 0.0).astype(BF)
    before = jnp.where(iota((TOK, TOK), 0) < iota((TOK, TOK), 1), 1.0, 0.0).astype(BF)
    count = mm(both, before)
    row = iota((ROWS, TOK), 0)
    cots = cot[...].astype(F32)
    places, scaled, rows = [], [], []
    for k in range(2):
        slot = jnp.sum(jnp.where(hits[k], count, 0.0), axis=0, keepdims=True)
        place = picks[k : k + 1] * CAP + slot.astype(jnp.int32)
        rows.append(place)
        places.append(jnp.where(row == place, 1.0, 0.0).astype(BF))
        scaled.append((columns(gates[k : k + 1, :]) * cots).astype(BF))
    target[...] = jnp.concatenate(rows + [jnp.zeros((6, TOK), jnp.int32)], axis=0)
    toks = mm(places[0] + places[1], mix[...]).astype(BF)
    buf[:, 0:CAP, :] = toks.reshape(EXP, CAP, WIDE)
    spread = mm(jnp.concatenate(places, axis=1), jnp.concatenate(scaled, axis=0)).astype(BF)
    buf[:, CAP : 2 * CAP, :] = spread.reshape(EXP, CAP, WIDE)


def prepare(quarter, routes, gates, mixed, cotangent):
    whole = lambda i, q: (0, 0)
    part = lambda i, q: (0, lax.rem(q[0], 8))
    return pl.pallas_call(
        prepare_kernel,
        out_shape=(
            jax.ShapeDtypeStruct((EXP, 2 * CAP, WIDE), BF),
            jax.ShapeDtypeStruct((8, TOK), jnp.int32),
        ),
        grid_spec=pltpu.PrefetchScalarGridSpec(
            num_scalar_prefetch=1,
            grid=(1,),
            in_specs=[
                pl.BlockSpec((2, TOK), whole),
                pl.BlockSpec((2, TOK), whole),
                pl.BlockSpec((TOK, WIDE), part),
                pl.BlockSpec((TOK, WIDE), part),
            ],
            out_specs=(
                pl.BlockSpec((EXP, 2 * CAP, WIDE), lambda i, q: (0, 0, 0)),
                pl.BlockSpec((8, TOK), whole),
            ),
        ),
        name="prepare",
    )(quarter, routes, gates, mixed, cotangent)


def row_blocks(chunk):
    toks = chunk[:, 0:CAP, :].reshape(ROWS, WIDE)
    cots = chunk[:, CAP : 2 * CAP, :].reshape(ROWS, WIDE)
    return toks, cots


def gate_rows(own, other, at):
    return jnp.concatenate([own[0, :, at], other[0, :, at], own[1, :, at], other[1, :, at]], axis=0)


def expert_kernel(where, *refs):
    chunks = refs[:8]
    own, other, near, mid, far, last, home, g_gate, g_up, g_hid = refs[8:]
    ids = chunk_ids(where[0])
    pre = jnp.zeros((ROWS, 4 * FF), F32)
    grad_hidden = jnp.zeros((ROWS, 2 * FF), F32)
    for k in range(8):
        at = pl.ds(pl.multiple_of(ids[k] * WIDE, WIDE), WIDE)
        toks, cots = row_blocks(chunks[k])
        pre = pre + mm_nt(toks, gate_rows(own, other, at))
        grad_hidden = grad_hidden + mm_nt(cots, jnp.concatenate([own[2, :, at], other[2, :, at]], axis=0))
    pre_gate = pre[:, : 2 * FF]
    pre_up = pre[:, 2 * FF :]
    logistic = 1.0 / (1.0 + jnp.exp(-pre_gate))
    active = pre_gate * logistic
    slope = logistic * (1.0 + pre_gate * (1.0 - logistic))
    gate = (grad_hidden * pre_up * slope).astype(BF)
    up = (grad_hidden * active).astype(BF)
    g_gate[...] = gate
    g_up[...] = up
    g_hid[...] = (active * pre_up).astype(BF)
    grads = jnp.concatenate([gate, up], axis=1)
    y, core = where[0] >> 1, where[0] & 1
    step = 1 - 2 * core
    for k, out in ((4, last), (3, far), (2, mid), (1, near), (0, home)):
        chip = (y + step * k + 8) & 7
        start = chip * WIDE if k in (1, 2, 3) else chip * WIDE + core * TOK
        size = out.shape[1]
        at = pl.ds(pl.multiple_of(start, TOK), size)
        out[...] = mm(grads, gate_rows(own, other, at)).astype(BF)


def weights_kernel(where, *refs):
    chunks = refs[:8]
    g_gate, g_up, g_hid, d_gate, d_up, d_down = refs[8:]
    gates = jnp.concatenate([g_gate[...].T[:FF], g_up[...].T[:FF]], axis=0)
    hidden = g_hid[...].T[:FF]
    ids = chunk_ids(where[0])
    for k in range(8):
        at = pl.ds(pl.multiple_of(ids[k] * WIDE, WIDE), WIDE)
        toks, cots = row_blocks(chunks[k])
        both = mm(gates, toks).astype(BF)
        d_gate[:, at] = both[:FF]
        d_up[:, at] = both[FF:]
        d_down[:, at] = mm(hidden, cots).astype(BF)


def fold_kernel(where, near, mid, far, last, home, keep, give):
    total = near[...].astype(F32) + mid[...].astype(F32) + far[...].astype(F32)
    first = total[:, :TOK]
    second = total[:, TOK:]
    top = where[0] & 1 == 0
    keep[...] = jnp.where(top, first, second) + last[...].astype(F32) + home[...].astype(F32)
    give[...] = jnp.where(top, second, first).astype(BF)


def combine_kernel(where, target, rows, cotangent, out, cot, arrived):
    at = pl.ds(pl.multiple_of(where[0] * TOK, TOK), TOK)
    copy = pltpu.make_async_copy(cotangent.at[:, at], cot, arrived)
    copy.start()
    lane = iota((TOK, ROWS), 1)
    places = target[...].T
    pick = jnp.where((lane == places[:, 0:1]) | (lane == places[:, 1:2]), 1.0, 0.0).astype(BF)
    total = mm(pick, rows[...].reshape(ROWS, TOK))
    copy.wait()
    out[...] = (cot[...].astype(F32) + total).astype(BF)


def combine(slot, target, rows, cotangent):
    return pl.pallas_call(
        combine_kernel,
        out_shape=jax.ShapeDtypeStruct((TOK, TOK), BF),
        in_specs=[smem(), vmem(), vmem(), pl.BlockSpec(memory_space=pltpu.HBM)],
        out_specs=vmem(),
        scratch_shapes=[pltpu.VMEM((TOK, TOK), BF), pltpu.SemaphoreType.DMA],
        name="combine",
    )(slot, target, rows, cotangent)


def project_kernel(whole, weight, gate_pre, mixer, logs, read, d_gate, grad_y, run, buf, rest):
    back = mm_nt(whole[...], weight[...])
    pre = gate_pre[...].astype(F32)
    saved = mixer[...].astype(F32)
    logistic = 1.0 / (1.0 + jnp.exp(-pre))
    active = pre * logistic
    d_gate[...] = (back * saved * (logistic * (1.0 + pre * (1.0 - logistic)))).astype(BF)
    gated = (saved * active).astype(BF)
    for k in range(8):
        turned = whole[:, k * WIDE : (k + 1) * WIDE].T
        part = mm(turned, gated).astype(BF).reshape(4, FF, WIDE)
        buf[4 * k : 4 * k + 4, 0:EXP, :] = part[:, 0:EXP]
        rest[4 * k : 4 * k + 4] = part[:, EXP:]
    grad = back * active
    grad_y[...] = grad
    upto = jnp.where(iota((TOK, TOK), 0) <= iota((TOK, TOK), 1), 1.0, 0.0)
    rates = jnp.concatenate([logs[...], jnp.zeros((4, TOK), F32)], axis=0)
    running = mm(rates, upto, lax.Precision.HIGHEST)
    run[...] = running
    start = jnp.exp(running)
    turned = grad.T
    scale = jnp.concatenate([jnp.broadcast_to(start[j : j + 1], (HD, TOK)) for j in range(HEADS)], axis=0)
    high, low = two_parts(turned * scale)
    state = mm(high, read[...]) + mm(low, read[...])
    total = running[0:HEADS, TOK - 1 : TOK]
    first = total.astype(BF).astype(F32)
    second = (total - first).astype(BF).astype(F32)
    third = total - first - second
    line = iota((8, STATE), 0)
    notes = []
    for j in range(HEADS):
        note = jnp.where(line == 0, first[j : j + 1], jnp.where(line == 1, second[j : j + 1], third[j : j + 1]))
        note = jnp.where(line < 3, note, 0.0)
        notes.append(jnp.broadcast_to(note[None], (EXP // HEADS, 8, STATE)))
    buf[:, EXP:, 0:STATE] = state.reshape(EXP, 8, STATE).astype(BF)
    buf[:, EXP:, STATE:] = jnp.concatenate(notes, axis=0).astype(BF)


def scan_kernel(received, rest, out):
    out[:, 0:EXP, :] = rest[...]
    state = jnp.zeros((8, STATE), F32)
    for k in reversed(range(EXP)):
        high, low = two_parts(state)
        out[k, EXP:, 0:STATE] = high
        out[k, EXP:, STATE:] = low
        if k > 0:
            piece = received[k, EXP:, :].astype(F32)
            note = piece[:, STATE:]
            log = note[0:1] + note[1:2] + note[2:3]
            state = jnp.exp(log) * state + piece[:, :STATE]


def inner_kernel(grad_y, values, write, read, run, entry, dx, dw, dr):
    running = run[...]
    cols = running.T
    grads = grad_y[...]
    vals = values[...].astype(F32)
    cross = mm_nt(write[...], read[...])
    later = iota((TOK, TOK), 1) >= iota((TOK, TOK), 0)
    total = jnp.zeros((TOK, TOK), F32)
    parts = []
    starts = []
    for j in range(HEADS):
        spread = running[j : j + 1] - cols[:, j : j + 1]
        decay = jnp.where(later, jnp.exp(jnp.where(later, spread, 0.0)), 0.0)
        grad = grads[:, j * HD : (j + 1) * HD]
        parts.append(mm_exact(cross * decay, grad))
        total = total + mm_nt_exact(vals[:, j * HD : (j + 1) * HD], grad) * decay
        starts.append(grad * jnp.exp(cols[:, j : j + 1]))
    dx[...] = jnp.concatenate(parts, axis=1)
    dw[...] = mm_exact(total, read[...].astype(F32))
    entry_rows = entry[...].reshape(HEADS * HD, STATE)
    dr[...] = mm_exact(total.T, write[...].astype(F32)) + mm_exact(jnp.concatenate(starts, axis=1), entry_rows)


def outer_kernel(dx, dw, values, write, run, half, second, d_values, d_write, d_out):
    running = run[...]
    ends = jnp.exp(running[:, TOK - 1 : TOK] - running).T
    scale = jnp.concatenate([jnp.broadcast_to(ends[:, j : j + 1], (TOK, HD)) for j in range(HEADS)], axis=1)
    high = second[:, EXP:, 0:STATE].reshape(HEADS * HD, STATE)
    low = second[:, EXP:, STATE:].reshape(HEADS * HD, STATE)
    d_values[...] = (dx[...] + scale * (mm_nt(write[...], high) + mm_nt(write[...], low))).astype(BF)
    top, rest = two_parts(values[...].astype(F32) * scale)
    d_write[...] = dw[...] + mm(top, high) + mm(top, low) + mm(rest, high)
    total = second[0, 0:EXP, :].astype(F32)
    for k in range(1, EXP):
        total = total + second[k, 0:EXP, :].astype(F32)
    d_out[0:EXP, :] = half[...]
    d_out[EXP:, :] = total


def step(mixed, cotangent, routes, gates, w_gate, w_up, w_down, out_weight, gate_pre, mixer_out, values,
         write_keys, read_keys, log_decay, entry_states):
    shape = jax.ShapeDtypeStruct
    swap = [(0, 1), (1, 0)]
    rings = []
    for k in range(1, 5):
        up = [(2 * y, 2 * ((y + k) % 8)) for y in range(8)]
        rings.append(up + [(2 * y + 1, 2 * ((y - k) % 8) + 1) for y in range(8)])
    ring = rings[0]
    slot = lax.axis_index(TP).astype(jnp.int32).reshape(1)
    own = jnp.stack([w_gate[0].T, w_up[0].T, w_down[0]])
    other = lax.ppermute(own, "core", swap)
    buf, target = prepare(slot, routes.T, gates.T, mixed, cotangent)
    c0 = lax.all_to_all(buf, SP, 0, 0, tiled=True)
    c2 = lax.ppermute(c0, TP, ring)
    c1 = lax.ppermute(c0, "core", swap)
    c3 = lax.ppermute(c1, TP, ring)
    c4 = lax.ppermute(c2, TP, ring)
    moved, other = lax.optimization_barrier((c2, other))
    c5 = lax.ppermute(moved, "core", swap)
    c6 = lax.ppermute(c3, "core", swap)
    c7 = lax.ppermute(c4, "core", swap)
    chunks = (c0, c1, c2, c3, c4, c5, c6, c7)
    grad = shape((ROWS, 2 * FF), BF)
    full, thin = shape((ROWS, WIDE), BF), shape((ROWS, TOK), BF)
    *parts, home, g_gate, g_up, g_hid = call(
        expert_kernel, (full, full, full, thin, thin, grad, grad, grad),
        [smem()] + [vmem()] * 10, (slot, *chunks, own, other))
    pieces = []
    for k in range(4):
        pieces.append(lax.ppermute(parts[k], TP, rings[k]))
    wide = shape((FF, D), BF)
    d_wg, d_wu, d_wd = call(
        weights_kernel, (wide, wide, wide),
        [smem()] + [vmem()] * 11, (slot, *chunks, g_gate, g_up, g_hid), flops=10**9)
    pieces, d_wg, d_wu, d_wd = lax.optimization_barrier((pieces, d_wg, d_wu, d_wd))
    keep, give = call(
        fold_kernel, (shape((ROWS, TOK), F32), thin),
        [smem()] + [vmem()] * 5, (slot, *pieces, home))
    taken = lax.ppermute(give, "core", swap)
    summed = (keep + taken.astype(F32)).astype(BF).reshape(EXP, CAP, TOK)
    back = lax.all_to_all(summed, SP, 0, 0, tiled=True)
    d_input = combine(slot, target, back, cotangent)
    whole = lax.all_gather(d_input, TP, axis=1, tiled=True)
    flat = shape((TOK, HEADS * HD), BF)
    d_gate, grad_y, run, sent, rest = call(
        project_kernel,
        (flat, shape((TOK, HEADS * HD), F32), shape((8, TOK), F32), shape((EXP, EXP + 8, WIDE), BF),
         shape((EXP, EXP, WIDE), BF)),
        [vmem()] * 6, (whole, out_weight, gate_pre, mixer_out, log_decay, read_keys))
    received = lax.all_to_all(sent, SP, 0, 0, tiled=True)
    square = shape((TOK, STATE), F32)
    dx, dw, d_read = call(
        inner_kernel, (shape((TOK, HEADS * HD), F32), square, square),
        [vmem()] * 6, (grad_y, values, write_keys, read_keys, run, entry_states[0]), flops=10**9)
    received, dx, dw, d_read = lax.optimization_barrier((received, dx, dw, d_read))
    states = call(scan_kernel, shape((EXP, EXP + 8, WIDE), BF), [vmem()] * 2, (received, rest))
    second = lax.all_to_all(states, SP, 0, 0, tiled=True)
    half = jnp.sum(received[:, :EXP].astype(F32), axis=0)
    second, half = lax.optimization_barrier((second, half))
    d_values, d_write, d_out_weight = call(
        outer_kernel, (flat, square, shape((D // EXP, HEADS * HD), F32)), [vmem()] * 7,
        (dx, dw, values, write_keys, run, half, second))
    return (d_wg.T[None], d_wu.T[None], d_wd[None], d_out_weight, d_input, d_values, d_write, d_read, d_gate)


def solution(mesh):
    finer = Mesh(mesh.devices.reshape(8, 4, 8, 2), ("z", "x", "y", "core"))
    return jax.shard_map(
        step,
        mesh=finer,
        in_specs=(
            P(SP, None),
            P(SP, None),
            P(SP, None),
            P(SP, None),
            P(SP, None, TP),
            P(SP, None, TP),
            P(SP, TP, None),
            P(TP, None),
            P(SP, TP),
            P(SP, TP),
            P(SP, TP),
            P(SP, TP),
            P(SP, TP),
            P(TP, SP),
            P(SP, TP, None, None),
        ),
        out_specs=(
            P(SP, None, TP),
            P(SP, None, TP),
            P(SP, TP, None),
            P(SP, TP),
            P(SP, TP),
            P(SP, TP),
            P(SP, TP),
            P(SP, TP),
            P(SP, TP),
        ),
        check_vma=False,
    )
```

```python
import jax
import jax.numpy as jnp
from jax import lax
from jax.experimental import pallas as pl
from jax.experimental.pallas import tpu as pltpu
from jax.sharding import Mesh
from jax.sharding import PartitionSpec as P

D = 2048
TOK = 128
EXP = 32
CAP = 16
ROWS = EXP * CAP
WIDE = 256
FF = 64
HEADS = 4
HD = 64
STATE = 128
SP = ("z", "x")
TP = ("y", "core")
GRANT = 16 * 1024 * 1024
BF = jnp.bfloat16
F32 = jnp.float32


def iota(shape, dim):
    return lax.broadcasted_iota(jnp.int32, shape, dim)


def mm(a, b, precision=None):
    return lax.dot_general(a, b, (((1,), (0,)), ((), ())), precision=precision, preferred_element_type=F32)


def mm_nt(a, b):
    return lax.dot_general(a, b, (((1,), (1,)), ((), ())), preferred_element_type=F32)


def mm_parts(left, right, product):
    total = None
    for i, a in enumerate(left):
        for j, b in enumerate(right):
            if i + j < 2:
                part = product(a, b)
                total = part if total is None else total + part
    return total


def two_parts(value):
    high = value.astype(BF)
    return high, (value - high.astype(F32)).astype(BF)


def chunk_ids(slot):
    y, core = slot >> 1, slot & 1
    turn = 2 * core - 1
    near, far, beyond, home = (y + turn) & 3, (y - turn) & 3, (y + 2) & 3, y & 3
    mine, theirs = core, 1 - core
    return (2 * home + mine, 2 * home + theirs, 2 * near + mine, 2 * near + theirs, 2 * beyond + mine,
            2 * far + theirs, 2 * far + mine, 2 * beyond + theirs)


def columns(row):
    return jnp.broadcast_to(row, (8, row.shape[1])).T[:, 0:1]


def vmem():
    return pl.BlockSpec(memory_space=pltpu.VMEM)


def smem():
    return pl.BlockSpec(memory_space=pltpu.SMEM)


def call(kernel, outs, specs, args, flops=0):
    return pl.pallas_call(
        kernel,
        out_shape=outs,
        in_specs=specs,
        out_specs=jax.tree.map(lambda _: vmem(), outs),
        compiler_params=pltpu.CompilerParams(vmem_limit_bytes=GRANT),
        cost_estimate=pl.CostEstimate(flops=flops, bytes_accessed=0, transcendentals=0),
    )(*args)


def prepare_kernel(where, routes, gates, mixed, cotangent, buf, target, mix, cot, arrived):
    at = pl.ds(pl.multiple_of(lax.rem(where[0], 8) * WIDE, WIDE), WIDE)
    copies = [
        pltpu.make_async_copy(mixed.at[:, at], mix, arrived.at[0]),
        pltpu.make_async_copy(cotangent.at[:, at], cot, arrived.at[1]),
    ]
    for copy in copies:
        copy.start()
    picks = routes[...]
    expert = iota((EXP, TOK), 0)
    hits = [expert == picks[k : k + 1] for k in range(2)]
    both = jnp.where(hits[0] | hits[1], 1.0, 0.0).astype(BF)
    before = jnp.where(iota((TOK, TOK), 0) < iota((TOK, TOK), 1), 1.0, 0.0).astype(BF)
    count = mm(both, before)
    row = iota((ROWS, TOK), 0)
    places, rows = [], []
    for k in range(2):
        slot = jnp.sum(jnp.where(hits[k], count, 0.0), axis=0, keepdims=True)
        place = picks[k : k + 1] * CAP + slot.astype(jnp.int32)
        rows.append(place)
        places.append(jnp.where(row == place, 1.0, 0.0).astype(BF))
    target[...] = jnp.concatenate(rows + [jnp.zeros((6, TOK), jnp.int32)], axis=0)
    for copy in copies:
        copy.wait()
    cots = cot[...].astype(F32)
    scaled = [(columns(gates[k : k + 1, :]) * cots).astype(BF) for k in range(2)]
    toks = mm(places[0] + places[1], mix[...]).astype(BF)
    buf[:, 0:CAP, :] = toks.reshape(EXP, CAP, WIDE)
    spread = mm(jnp.concatenate(places, axis=1), jnp.concatenate(scaled, axis=0)).astype(BF)
    buf[:, CAP : 2 * CAP, :] = spread.reshape(EXP, CAP, WIDE)


def prepare(slot, routes, gates, mixed, cotangent):
    hbm = pl.BlockSpec(memory_space=pltpu.HBM)
    return pl.pallas_call(
        prepare_kernel,
        out_shape=(
            jax.ShapeDtypeStruct((EXP, 2 * CAP, WIDE), BF),
            jax.ShapeDtypeStruct((8, TOK), jnp.int32),
        ),
        in_specs=[smem(), vmem(), vmem(), hbm, hbm],
        out_specs=(vmem(), vmem()),
        scratch_shapes=[
            pltpu.VMEM((TOK, WIDE), BF),
            pltpu.VMEM((TOK, WIDE), BF),
            pltpu.SemaphoreType.DMA((2,)),
        ],
        compiler_params=pltpu.CompilerParams(vmem_limit_bytes=GRANT),
        name="prepare",
    )(slot, routes, gates, mixed, cotangent)


def row_blocks(chunk):
    toks = chunk[:, 0:CAP, :].reshape(ROWS, WIDE)
    cots = chunk[:, CAP : 2 * CAP, :].reshape(ROWS, WIDE)
    return toks, cots


def gate_rows(own, other, at):
    return jnp.concatenate([own[0, :, at], other[0, :, at], own[1, :, at], other[1, :, at]], axis=0)


def expert_kernel(where, *refs):
    chunks = refs[:8]
    own, other, near, mid, far, last, home, g_gate, g_up, g_hid = refs[8:]
    ids = chunk_ids(where[0])
    pre = jnp.zeros((ROWS, 4 * FF), F32)
    grad_hidden = jnp.zeros((ROWS, 2 * FF), F32)
    for k in range(8):
        at = pl.ds(pl.multiple_of(ids[k] * WIDE, WIDE), WIDE)
        toks, cots = row_blocks(chunks[k])
        pre = pre + mm_nt(toks, gate_rows(own, other, at))
        grad_hidden = grad_hidden + mm_nt(cots, jnp.concatenate([own[2, :, at], other[2, :, at]], axis=0))
    pre_gate = pre[:, : 2 * FF]
    pre_up = pre[:, 2 * FF :]
    logistic = 1.0 / (1.0 + jnp.exp(-pre_gate))
    active = pre_gate * logistic
    slope = logistic * (1.0 + pre_gate * (1.0 - logistic))
    gate = (grad_hidden * pre_up * slope).astype(BF)
    up = (grad_hidden * active).astype(BF)
    g_gate[...] = gate
    g_up[...] = up
    g_hid[...] = (active * pre_up).astype(BF)
    grads = jnp.concatenate([gate, up], axis=1)
    y, core = where[0] >> 1, where[0] & 1
    step = 1 - 2 * core
    for k, out in ((4, last), (3, far), (2, mid), (1, near), (0, home)):
        chip = (y + step * k + 8) & 7
        start = chip * WIDE if k in (1, 2, 3) else chip * WIDE + core * TOK
        size = out.shape[1]
        at = pl.ds(pl.multiple_of(start, TOK), size)
        out[...] = mm(grads, gate_rows(own, other, at)).astype(BF)


def weights_kernel(where, *refs):
    chunks = refs[:8]
    g_gate, g_up, g_hid, d_gate, d_up, d_down = refs[8:]
    gates = jnp.concatenate([g_gate[...].T[:FF], g_up[...].T[:FF]], axis=0)
    hidden = g_hid[...].T[:FF]
    ids = chunk_ids(where[0])
    for k in range(8):
        at = pl.ds(pl.multiple_of(ids[k] * WIDE, WIDE), WIDE)
        toks, cots = row_blocks(chunks[k])
        both = mm(gates, toks).astype(BF)
        d_gate[:, at] = both[:FF]
        d_up[:, at] = both[FF:]
        d_down[:, at] = mm(hidden, cots).astype(BF)


def fold_kernel(where, near, mid, far, last, home, keep, give):
    total = near[...].astype(F32) + mid[...].astype(F32) + far[...].astype(F32)
    first = total[:, :TOK]
    second = total[:, TOK:]
    top = where[0] & 1 == 0
    keep[...] = jnp.where(top, first, second) + last[...].astype(F32) + home[...].astype(F32)
    give[...] = jnp.where(top, second, first).astype(BF)


def combine_kernel(where, target, rows, cotangent, out, cot, arrived):
    at = pl.ds(pl.multiple_of(where[0] * TOK, TOK), TOK)
    copy = pltpu.make_async_copy(cotangent.at[:, at], cot, arrived)
    copy.start()
    lane = iota((TOK, ROWS), 1)
    places = target[...].T
    pick = jnp.where((lane == places[:, 0:1]) | (lane == places[:, 1:2]), 1.0, 0.0).astype(BF)
    total = mm(pick, rows[...].reshape(ROWS, TOK))
    copy.wait()
    out[...] = (cot[...].astype(F32) + total).astype(BF)


def combine(slot, target, rows, cotangent):
    return pl.pallas_call(
        combine_kernel,
        out_shape=jax.ShapeDtypeStruct((TOK, TOK), BF),
        in_specs=[smem(), vmem(), vmem(), pl.BlockSpec(memory_space=pltpu.HBM)],
        out_specs=vmem(),
        scratch_shapes=[pltpu.VMEM((TOK, TOK), BF), pltpu.SemaphoreType.DMA],
        compiler_params=pltpu.CompilerParams(vmem_limit_bytes=GRANT),
        name="combine",
    )(slot, target, rows, cotangent)


def project_kernel(whole, weight, gate_pre, mixer, logs, read, d_gate, grad_y, run, buf, rest):
    back = mm_nt(whole[...], weight[...])
    pre = gate_pre[...].astype(F32)
    saved = mixer[...].astype(F32)
    logistic = 1.0 / (1.0 + jnp.exp(-pre))
    active = pre * logistic
    d_gate[...] = (back * saved * (logistic * (1.0 + pre * (1.0 - logistic)))).astype(BF)
    gated = (saved * active).astype(BF)
    for k in range(8):
        turned = whole[:, k * WIDE : (k + 1) * WIDE].T
        part = mm(turned, gated).astype(BF).reshape(4, FF, WIDE)
        buf[4 * k : 4 * k + 4, 0:EXP, :] = part[:, 0:EXP]
        rest[4 * k : 4 * k + 4] = part[:, EXP:]
    grad = back * active
    grad_y[...] = grad
    upto = jnp.where(iota((TOK, TOK), 0) <= iota((TOK, TOK), 1), 1.0, 0.0)
    rates = jnp.concatenate([logs[...], jnp.zeros((4, TOK), F32)], axis=0)
    running = mm(rates, upto, lax.Precision.HIGHEST)
    run[...] = running
    start = jnp.exp(running)
    turned = grad.T
    scale = jnp.concatenate([jnp.broadcast_to(start[j : j + 1], (HD, TOK)) for j in range(HEADS)], axis=0)
    high, low = two_parts(turned * scale)
    state = mm(high, read[...]) + mm(low, read[...])
    total = running[0:HEADS, TOK - 1 : TOK]
    first = total.astype(BF).astype(F32)
    second = (total - first).astype(BF).astype(F32)
    third = total - first - second
    line = iota((8, STATE), 0)
    notes = []
    for j in range(HEADS):
        note = jnp.where(line == 0, first[j : j + 1], jnp.where(line == 1, second[j : j + 1], third[j : j + 1]))
        note = jnp.where(line < 3, note, 0.0)
        notes.append(jnp.broadcast_to(note[None], (EXP // HEADS, 8, STATE)))
    buf[:, EXP:, 0:STATE] = state.reshape(EXP, 8, STATE).astype(BF)
    buf[:, EXP:, STATE:] = jnp.concatenate(notes, axis=0).astype(BF)


def scan_kernel(received, rest, out):
    out[:, 0:EXP, :] = rest[...]
    state = jnp.zeros((8, STATE), F32)
    for k in reversed(range(EXP)):
        high, low = two_parts(state)
        out[k, EXP:, 0:STATE] = high
        out[k, EXP:, STATE:] = low
        if k > 0:
            piece = received[k, EXP:, :].astype(F32)
            note = piece[:, STATE:]
            log = note[0:1] + note[1:2] + note[2:3]
            state = jnp.exp(log) * state + piece[:, :STATE]


def inner_kernel(grad_y, values, write, read, run, entry, dx, dw, dr):
    running = run[...]
    cols = running.T
    grads = grad_y[...]
    vals = values[...]
    cross = mm_nt(write[...], read[...])
    later = iota((TOK, TOK), 1) >= iota((TOK, TOK), 0)
    total = jnp.zeros((TOK, TOK), F32)
    parts = []
    starts = []
    for j in range(HEADS):
        spread = running[j : j + 1] - cols[:, j : j + 1]
        decay = jnp.where(later, jnp.exp(jnp.where(later, spread, 0.0)), 0.0)
        grad = grads[:, j * HD : (j + 1) * HD]
        halves = two_parts(grad)
        parts.append(mm_parts(two_parts(cross * decay), halves, mm))
        total = total + mm_parts((vals[:, j * HD : (j + 1) * HD],), halves, mm_nt) * decay
        starts.append(grad * jnp.exp(cols[:, j : j + 1]))
    dx[...] = jnp.concatenate(parts, axis=1)
    dw[...] = mm_parts(two_parts(total), (read[...],), mm)
    entry_rows = two_parts(entry[...].reshape(HEADS * HD, STATE))
    first = mm_parts(two_parts(total.T), (write[...],), mm)
    dr[...] = first + mm_parts(two_parts(jnp.concatenate(starts, axis=1)), entry_rows, mm)


def outer_kernel(dx, dw, values, write, run, received, second, d_values, d_write, d_out):
    running = run[...]
    ends = jnp.exp(running[:, TOK - 1 : TOK] - running).T
    scale = jnp.concatenate([jnp.broadcast_to(ends[:, j : j + 1], (TOK, HD)) for j in range(HEADS)], axis=1)
    high = second[:, EXP:, 0:STATE].reshape(HEADS * HD, STATE)
    low = second[:, EXP:, STATE:].reshape(HEADS * HD, STATE)
    d_values[...] = (dx[...] + scale * (mm_nt(write[...], high) + mm_nt(write[...], low))).astype(BF)
    top, rest = two_parts(values[...].astype(F32) * scale)
    d_write[...] = dw[...] + mm(top, high) + mm(top, low) + mm(rest, high)
    for at, block in ((0, received), (EXP, second)):
        total = block[0, 0:EXP, :].astype(F32)
        for k in range(1, EXP):
            total = total + block[k, 0:EXP, :].astype(F32)
        d_out[at : at + EXP, :] = total


def step(mixed, cotangent, routes, gates, w_gate, w_up, w_down, out_weight, gate_pre, mixer_out, values,
         write_keys, read_keys, log_decay, entry_states):
    shape = jax.ShapeDtypeStruct
    swap = [(0, 1), (1, 0)]
    rings = []
    for k in range(1, 5):
        up = [(2 * y, 2 * ((y + k) % 8)) for y in range(8)]
        rings.append(up + [(2 * y + 1, 2 * ((y - k) % 8) + 1) for y in range(8)])
    ring = rings[0]
    slot = lax.axis_index(TP).astype(jnp.int32).reshape(1)
    own = jnp.stack([w_gate[0].T, w_up[0].T, w_down[0]])
    other = lax.ppermute(own, "core", swap)
    buf, target = prepare(slot, routes.T, gates.T, mixed, cotangent)
    c0 = lax.all_to_all(buf, SP, 0, 0, tiled=True)
    c2 = lax.ppermute(c0, TP, ring)
    c1 = lax.ppermute(c0, "core", swap)
    c3 = lax.ppermute(c1, TP, ring)
    c4 = lax.ppermute(c2, TP, ring)
    moved, other = lax.optimization_barrier((c2, other))
    c5 = lax.ppermute(moved, "core", swap)
    c6 = lax.ppermute(c3, "core", swap)
    c7 = lax.ppermute(c4, "core", swap)
    chunks = (c0, c1, c2, c3, c4, c5, c6, c7)
    grad = shape((ROWS, 2 * FF), BF)
    full, thin = shape((ROWS, WIDE), BF), shape((ROWS, TOK), BF)
    *parts, home, g_gate, g_up, g_hid = call(
        expert_kernel, (full, full, full, thin, thin, grad, grad, grad),
        [smem()] + [vmem()] * 10, (slot, *chunks, own, other))
    pieces = []
    for k in range(4):
        pieces.append(lax.ppermute(parts[k], TP, rings[k]))
    wide = shape((FF, D), BF)
    d_wg, d_wu, d_wd = call(
        weights_kernel, (wide, wide, wide),
        [smem()] + [vmem()] * 11, (slot, *chunks, g_gate, g_up, g_hid), flops=10**9)
    pieces, d_wg, d_wu, d_wd = lax.optimization_barrier((pieces, d_wg, d_wu, d_wd))
    keep, give = call(
        fold_kernel, (shape((ROWS, TOK), F32), thin),
        [smem()] + [vmem()] * 5, (slot, *pieces, home))
    taken = lax.ppermute(give, "core", swap)
    summed = (keep + taken.astype(F32)).astype(BF).reshape(EXP, CAP, TOK)
    back = lax.all_to_all(summed, SP, 0, 0, tiled=True)
    d_input = combine(slot, target, back, cotangent)
    whole = lax.all_gather(d_input, TP, axis=1, tiled=True)
    flat = shape((TOK, HEADS * HD), BF)
    d_gate, grad_y, run, sent, rest = call(
        project_kernel,
        (flat, shape((TOK, HEADS * HD), F32), shape((8, TOK), F32), shape((EXP, EXP + 8, WIDE), BF),
         shape((EXP, EXP, WIDE), BF)),
        [vmem()] * 6, (whole, out_weight, gate_pre, mixer_out, log_decay, read_keys))
    square = shape((TOK, STATE), F32)
    dx, dw, d_read = call(
        inner_kernel, (shape((TOK, HEADS * HD), F32), square, square),
        [vmem()] * 6, (grad_y, values, write_keys, read_keys, run, entry_states[0]), flops=10**9)
    sent, dx, dw, d_read = lax.optimization_barrier((sent, dx, dw, d_read))
    received = lax.all_to_all(sent, SP, 0, 0, tiled=True)
    states = call(scan_kernel, shape((EXP, EXP + 8, WIDE), BF), [vmem()] * 2, (received, rest))
    second = lax.all_to_all(states, SP, 0, 0, tiled=True)
    d_values, d_write, d_out_weight = call(
        outer_kernel, (flat, square, shape((D // EXP, HEADS * HD), F32)), [vmem()] * 7,
        (dx, dw, values, write_keys, run, received, second))
    return (d_wg.T[None], d_wu.T[None], d_wd[None], d_out_weight, d_input, d_values, d_write, d_read, d_gate)


def solution(mesh):
    finer = Mesh(mesh.devices.reshape(8, 4, 8, 2), ("z", "x", "y", "core"))
    return jax.shard_map(
        step,
        mesh=finer,
        in_specs=(
            P(SP, None),
            P(SP, None),
            P(SP, None),
            P(SP, None),
            P(SP, None, TP),
            P(SP, None, TP),
            P(SP, TP, None),
            P(TP, None),
            P(SP, TP),
            P(SP, TP),
            P(SP, TP),
            P(SP, TP),
            P(SP, TP),
            P(TP, SP),
            P(SP, TP, None, None),
        ),
        out_specs=(
            P(SP, None, TP),
            P(SP, None, TP),
            P(SP, TP, None),
            P(SP, TP),
            P(SP, TP),
            P(SP, TP),
            P(SP, TP),
            P(SP, TP),
            P(SP, TP),
        ),
        check_vma=False,
    )
```

```python
import jax
import jax.numpy as jnp
from jax import lax
from jax.experimental import pallas as pl
from jax.experimental.pallas import tpu as pltpu
from jax.sharding import Mesh
from jax.sharding import PartitionSpec as P

D = 2048
TOK = 128
EXP = 32
CAP = 16
ROWS = EXP * CAP
WIDE = 512
FF = 64
HEADS = 4
HD = 64
STATE = 128
SP = ("z", "x")
TP = ("y", "core")
GRANT = 16 * 1024 * 1024
BF = jnp.bfloat16
F32 = jnp.float32


def iota(shape, dim):
    return lax.broadcasted_iota(jnp.int32, shape, dim)


def mm(a, b, precision=None):
    return lax.dot_general(a, b, (((1,), (0,)), ((), ())), precision=precision, preferred_element_type=F32)


def mm_nt(a, b):
    return lax.dot_general(a, b, (((1,), (1,)), ((), ())), preferred_element_type=F32)


def mm_parts(left, right, product):
    total = None
    for i, a in enumerate(left):
        for j, b in enumerate(right):
            if i + j < 2:
                part = product(a, b)
                total = part if total is None else total + part
    return total


def two_parts(value):
    high = value.astype(BF)
    return high, (value - high.astype(F32)).astype(BF)


def quarter_of(slot):
    return slot & 3


def columns(row):
    return jnp.broadcast_to(row, (8, row.shape[1])).T[:, 0:1]


def vmem():
    return pl.BlockSpec(memory_space=pltpu.VMEM)


def smem():
    return pl.BlockSpec(memory_space=pltpu.SMEM)


def call(kernel, outs, specs, args, flops=0):
    return pl.pallas_call(
        kernel,
        out_shape=outs,
        in_specs=specs,
        out_specs=jax.tree.map(lambda _: vmem(), outs),
        compiler_params=pltpu.CompilerParams(vmem_limit_bytes=GRANT),
        cost_estimate=pl.CostEstimate(flops=flops, bytes_accessed=0, transcendentals=0),
    )(*args)


def prepare_kernel(where, routes, gates, mix, cot, buf, target):
    picks = routes[...]
    expert = iota((EXP, TOK), 0)
    hits = [expert == picks[k : k + 1] for k in range(2)]
    both = jnp.where(hits[0] | hits[1], 1.0, 0.0).astype(BF)
    before = jnp.where(iota((TOK, TOK), 0) < iota((TOK, TOK), 1), 1.0, 0.0).astype(BF)
    count = mm(both, before)
    row = iota((ROWS, TOK), 0)
    places, rows = [], []
    for k in range(2):
        slot = jnp.sum(jnp.where(hits[k], count, 0.0), axis=0, keepdims=True)
        place = picks[k : k + 1] * CAP + slot.astype(jnp.int32)
        rows.append(place)
        places.append(jnp.where(row == place, 1.0, 0.0).astype(BF))
    target[...] = jnp.concatenate(rows + [jnp.zeros((6, TOK), jnp.int32)], axis=0)
    cots = cot[...].astype(F32)
    scaled = [(columns(gates[k : k + 1, :]) * cots).astype(BF) for k in range(2)]
    toks = mm(places[0] + places[1], mix[...]).astype(BF)
    spread = mm(jnp.concatenate(places, axis=1), jnp.concatenate(scaled, axis=0)).astype(BF)
    for k in range(4):
        at = slice(k * TOK, (k + 1) * TOK)
        buf[:, 32 * k : 32 * k + CAP, :] = toks[:, at].reshape(EXP, CAP, TOK)
        buf[:, 32 * k + CAP : 32 * k + 32, :] = spread[:, at].reshape(EXP, CAP, TOK)


def prepare(slot, routes, gates, mixed, cotangent):
    whole = lambda i, q: (0, 0)
    part = lambda i, q: (0, quarter_of(q[0]))
    return pl.pallas_call(
        prepare_kernel,
        out_shape=(
            jax.ShapeDtypeStruct((EXP, 4 * EXP, TOK), BF),
            jax.ShapeDtypeStruct((8, TOK), jnp.int32),
        ),
        grid_spec=pltpu.PrefetchScalarGridSpec(
            num_scalar_prefetch=1,
            grid=(1,),
            in_specs=[
                pl.BlockSpec((2, TOK), whole),
                pl.BlockSpec((2, TOK), whole),
                pl.BlockSpec((TOK, WIDE), part),
                pl.BlockSpec((TOK, WIDE), part),
            ],
            out_specs=(
                pl.BlockSpec((EXP, 4 * EXP, TOK), lambda i, q: (0, 0, 0)),
                pl.BlockSpec((8, TOK), whole),
            ),
        ),
        compiler_params=pltpu.CompilerParams(vmem_limit_bytes=GRANT),
        name="prepare",
    )(slot, routes, gates, mixed, cotangent)


def row_blocks(chunk):
    toks, cots = [], []
    for k in range(4):
        toks.append(chunk[:, 32 * k : 32 * k + CAP, :].reshape(ROWS, TOK))
        cots.append(chunk[:, 32 * k + CAP : 32 * k + 32, :].reshape(ROWS, TOK))
    return jnp.concatenate(toks, axis=1), jnp.concatenate(cots, axis=1)


def gate_rows(own, other, at):
    return jnp.concatenate([own[0, :, at], other[0, :, at], own[1, :, at], other[1, :, at]], axis=0)


def expert_kernel(where, c0, c1, c2, c3, own, other, out, g_gate, g_up, g_hid):
    quarter, core = quarter_of(where[0]), where[0] & 1
    pre = jnp.zeros((ROWS, 4 * FF), F32)
    grad_hidden = jnp.zeros((ROWS, 2 * FF), F32)
    for k, chunk in enumerate((c0, c1, c2, c3)):
        at = pl.ds(pl.multiple_of((quarter ^ k) * WIDE, WIDE), WIDE)
        toks, cots = row_blocks(chunk)
        pre = pre + mm_nt(toks, gate_rows(own, other, at))
        grad_hidden = grad_hidden + mm_nt(cots, jnp.concatenate([own[2, :, at], other[2, :, at]], axis=0))
    pre_gate = pre[:, : 2 * FF]
    pre_up = pre[:, 2 * FF :]
    logistic = 1.0 / (1.0 + jnp.exp(-pre_gate))
    active = pre_gate * logistic
    slope = logistic * (1.0 + pre_gate * (1.0 - logistic))
    gate = (grad_hidden * pre_up * slope).astype(BF)
    up = (grad_hidden * active).astype(BF)
    g_gate[...] = gate
    g_up[...] = up
    g_hid[...] = (active * pre_up).astype(BF)
    grads = jnp.concatenate([gate, up], axis=1)
    for k in range(8):
        at = pl.ds(pl.multiple_of((2 * k + core) * TOK, TOK), TOK)
        part = mm(grads, gate_rows(own, other, at)).astype(BF)
        out[:, k * CAP : (k + 1) * CAP, :] = part.reshape(EXP, CAP, TOK)


def weights_kernel(where, c0, c1, c2, c3, g_gate, g_up, g_hid, d_gate, d_up, d_down):
    gates = jnp.concatenate([g_gate[...].T[:FF], g_up[...].T[:FF]], axis=0)
    hidden = g_hid[...].T[:FF]
    for k, chunk in enumerate((c0, c1, c2, c3)):
        at = pl.ds(pl.multiple_of((quarter_of(where[0]) ^ k) * WIDE, WIDE), WIDE)
        toks, cots = row_blocks(chunk)
        both = mm(gates, toks).astype(BF)
        d_gate[:, at] = both[:FF]
        d_up[:, at] = both[FF:]
        d_down[:, at] = mm(hidden, cots).astype(BF)


def combine_kernel(target, rows, out):
    lane = iota((TOK, ROWS), 1)
    places = target[...].T
    pick = jnp.where((lane == places[:, 0:1]) | (lane == places[:, 1:2]), 1.0, 0.0).astype(BF)
    for k in range(8):
        block = rows[:, k * CAP : (k + 1) * CAP, :].reshape(ROWS, TOK)
        out[k] = mm(pick, block).astype(BF)


def merge_kernel(where, pieces, cotangent, out, cot, arrived):
    at = pl.ds(pl.multiple_of(where[0] * TOK, TOK), TOK)
    copy = pltpu.make_async_copy(cotangent.at[:, at], cot, arrived)
    copy.start()
    total = pieces[0].astype(F32)
    for k in range(1, 8):
        total = total + pieces[k].astype(F32)
    copy.wait()
    out[...] = (cot[...].astype(F32) + total).astype(BF)


def merge(slot, pieces, cotangent):
    return pl.pallas_call(
        merge_kernel,
        out_shape=jax.ShapeDtypeStruct((TOK, TOK), BF),
        in_specs=[smem(), vmem(), pl.BlockSpec(memory_space=pltpu.HBM)],
        out_specs=vmem(),
        scratch_shapes=[pltpu.VMEM((TOK, TOK), BF), pltpu.SemaphoreType.DMA],
        compiler_params=pltpu.CompilerParams(vmem_limit_bytes=GRANT),
        name="merge",
    )(slot, pieces, cotangent)


def project_kernel(gathered, weight, gate_pre, mixer, logs, read, d_gate, grad_y, run, buf):
    whole = jnp.concatenate([gathered[k * TOK : (k + 1) * TOK, :] for k in range(16)], axis=1)
    back = mm_nt(whole, weight[...])
    pre = gate_pre[...].astype(F32)
    saved = mixer[...].astype(F32)
    logistic = 1.0 / (1.0 + jnp.exp(-pre))
    active = pre * logistic
    d_gate[...] = (back * saved * (logistic * (1.0 + pre * (1.0 - logistic)))).astype(BF)
    gated = (saved * active).astype(BF)
    for k in range(8):
        turned = whole[:, k * 256 : (k + 1) * 256].T
        part = mm(turned, gated).astype(BF)
        buf[4 * k : 4 * k + 4, 0:FF, :] = part[:, :TOK].reshape(4, FF, TOK)
        buf[4 * k : 4 * k + 4, FF : 2 * FF, :] = part[:, TOK:].reshape(4, FF, TOK)
    grad = back * active
    grad_y[...] = grad
    upto = jnp.where(iota((TOK, TOK), 0) <= iota((TOK, TOK), 1), 1.0, 0.0)
    rates = jnp.concatenate([logs[...], jnp.zeros((4, TOK), F32)], axis=0)
    running = mm(rates, upto, lax.Precision.HIGHEST)
    run[...] = running
    start = jnp.exp(running)
    turned = grad.T
    scale = jnp.concatenate([jnp.broadcast_to(start[j : j + 1], (HD, TOK)) for j in range(HEADS)], axis=0)
    high, low = two_parts(turned * scale)
    state = mm(high, read[...]) + mm(low, read[...])
    total = running[0:HEADS, TOK - 1 : TOK]
    first = total.astype(BF).astype(F32)
    second = (total - first).astype(BF).astype(F32)
    third = total - first - second
    line = iota((8, STATE), 0)
    notes = []
    for j in range(HEADS):
        note = jnp.where(line == 0, first[j : j + 1], jnp.where(line == 1, second[j : j + 1], third[j : j + 1]))
        note = jnp.where(line < 3, note, 0.0)
        notes.append(jnp.broadcast_to(note[None], (EXP // HEADS, 8, STATE)))
    sent = jnp.concatenate([state.reshape(EXP, 8, STATE), jnp.concatenate(notes, axis=0)], axis=1)
    buf[:, 2 * FF :, :] = sent.astype(BF)


def scan_kernel(received, out):
    state = jnp.zeros((8, STATE), F32)
    for k in reversed(range(EXP)):
        high, low = two_parts(state)
        out[k] = jnp.concatenate([high.astype(F32), low.astype(F32)], axis=0).astype(BF)
        if k > 0:
            piece = received[k, 2 * FF :, :].astype(F32)
            log = piece[8:9] + piece[9:10] + piece[10:11]
            state = jnp.exp(log) * state + piece[0:8]


def share_kernel(received, d_out):
    total = received[0, 0 : 2 * FF, :].astype(F32)
    for k in range(1, EXP):
        total = total + received[k, 0 : 2 * FF, :].astype(F32)
    d_out[:, :TOK] = total[:FF]
    d_out[:, TOK:] = total[FF:]


def inner_kernel(grad_y, values, write, read, run, entry, dx, dw, dr):
    running = run[...]
    cols = running.T
    grads = grad_y[...]
    vals = values[...]
    cross = mm_nt(write[...], read[...])
    later = iota((TOK, TOK), 1) >= iota((TOK, TOK), 0)
    total = jnp.zeros((TOK, TOK), F32)
    parts = []
    starts = []
    for j in range(HEADS):
        spread = running[j : j + 1] - cols[:, j : j + 1]
        decay = jnp.where(later, jnp.exp(jnp.where(later, spread, 0.0)), 0.0)
        grad = grads[:, j * HD : (j + 1) * HD]
        halves = two_parts(grad)
        parts.append(mm_parts(two_parts(cross * decay), halves, mm))
        total = total + mm_parts((vals[:, j * HD : (j + 1) * HD],), halves, mm_nt) * decay
        starts.append(grad * jnp.exp(cols[:, j : j + 1]))
    dx[...] = jnp.concatenate(parts, axis=1)
    dw[...] = mm_parts(two_parts(total), (read[...],), mm)
    entry_rows = two_parts(entry[...].reshape(HEADS * HD, STATE))
    first = mm_parts(two_parts(total.T), (write[...],), mm)
    dr[...] = first + mm_parts(two_parts(jnp.concatenate(starts, axis=1)), entry_rows, mm)


def outer_kernel(dx, dw, values, write, run, second, d_values, d_write):
    running = run[...]
    ends = jnp.exp(running[:, TOK - 1 : TOK] - running).T
    scale = jnp.concatenate([jnp.broadcast_to(ends[:, j : j + 1], (TOK, HD)) for j in range(HEADS)], axis=1)
    later = second[...].astype(F32)
    high = later[:, 0:8].reshape(HEADS * HD, STATE).astype(BF)
    low = later[:, 8:16].reshape(HEADS * HD, STATE).astype(BF)
    d_values[...] = (dx[...] + scale * (mm_nt(write[...], high) + mm_nt(write[...], low))).astype(BF)
    top, rest = two_parts(values[...].astype(F32) * scale)
    d_write[...] = dw[...] + mm(top, high) + mm(top, low) + mm(rest, high)


def step(mixed, cotangent, routes, gates, w_gate, w_up, w_down, out_weight, gate_pre, mixer_out, values,
         write_keys, read_keys, log_decay, entry_states):
    shape = jax.ShapeDtypeStruct
    swap = [(0, 1), (1, 0)]
    ring = []
    for k in range(8):
        ring.append((2 * k, 2 * ((k + 1) % 8)))
        ring.append((2 * k + 1, 2 * ((k - 1) % 8) + 1))
    slot = lax.axis_index(TP).astype(jnp.int32).reshape(1)
    own = jnp.stack([w_gate[0].T, w_up[0].T, w_down[0]])
    other = lax.ppermute(own, "core", swap)
    buf, target = prepare(slot, routes.T, gates.T, mixed, cotangent)
    c0 = lax.all_to_all(buf, SP, 0, 0, tiled=True)
    c2 = lax.ppermute(c0, TP, ring)
    c1 = lax.ppermute(c0, "core", swap)
    moved, other = lax.optimization_barrier((c2, other))
    c3 = lax.ppermute(moved, "core", swap)
    chunks = (c0, c1, c2, c3)
    grad = shape((ROWS, 2 * FF), BF)
    parts, g_gate, g_up, g_hid = call(
        expert_kernel, (shape((EXP, TOK, TOK), BF), grad, grad, grad),
        [smem()] + [vmem()] * 6, (slot, *chunks, own, other))
    back = lax.all_to_all(parts, SP, 0, 0, tiled=True)
    wide = shape((FF, D), BF)
    d_wg, d_wu, d_wd = call(
        weights_kernel, (wide, wide, wide),
        [smem()] + [vmem()] * 7, (slot, *chunks, g_gate, g_up, g_hid), flops=10**9)
    back, d_wg, d_wu, d_wd = lax.optimization_barrier((back, d_wg, d_wu, d_wd))
    summed = call(combine_kernel, shape((8, TOK, TOK), BF), [vmem()] * 2, (target, back))
    pieces = lax.all_to_all(summed, "y", 0, 0, tiled=True)
    d_input = merge(slot, pieces, cotangent)
    whole = lax.all_gather(d_input, TP, axis=0, tiled=True)
    flat = shape((TOK, HEADS * HD), BF)
    d_gate, grad_y, run, sent = call(
        project_kernel,
        (flat, shape((TOK, HEADS * HD), F32), shape((8, TOK), F32), shape((EXP, 2 * FF + 16, STATE), BF)),
        [vmem()] * 6, (whole, out_weight, gate_pre, mixer_out, log_decay, read_keys))
    square = shape((TOK, STATE), F32)
    dx, dw, d_read = call(
        inner_kernel, (shape((TOK, HEADS * HD), F32), square, square),
        [vmem()] * 6, (grad_y, values, write_keys, read_keys, run, entry_states[0]), flops=10**9)
    received = lax.all_to_all(sent, SP, 0, 0, tiled=True)
    received, dx, dw, d_read = lax.optimization_barrier((received, dx, dw, d_read))
    states = call(scan_kernel, shape((EXP, 16, STATE), BF), [vmem()], (received,))
    second = lax.all_to_all(states, SP, 0, 0, tiled=True)
    d_out_weight = call(share_kernel, shape((D // EXP, HEADS * HD), F32), [vmem()], (received,), flops=10**9)
    second, d_out_weight = lax.optimization_barrier((second, d_out_weight))
    d_values, d_write = call(
        outer_kernel, (flat, square), [vmem()] * 6,
        (dx, dw, values, write_keys, run, second))
    return (d_wg.T[None], d_wu.T[None], d_wd[None], d_out_weight, d_input, d_values, d_write, d_read, d_gate)


def solution(mesh):
    finer = Mesh(mesh.devices.reshape(8, 4, 8, 2), ("z", "x", "y", "core"))
    return jax.shard_map(
        step,
        mesh=finer,
        in_specs=(
            P(SP, None),
            P(SP, None),
            P(SP, None),
            P(SP, None),
            P(SP, None, TP),
            P(SP, None, TP),
            P(SP, TP, None),
            P(TP, None),
            P(SP, TP),
            P(SP, TP),
            P(SP, TP),
            P(SP, TP),
            P(SP, TP),
            P(TP, SP),
            P(SP, TP, None, None),
        ),
        out_specs=(
            P(SP, None, TP),
            P(SP, None, TP),
            P(SP, TP, None),
            P(SP, TP),
            P(SP, TP),
            P(SP, TP),
            P(SP, TP),
            P(SP, TP),
            P(SP, TP),
        ),
        check_vma=False,
    )
```

```python
import jax
import jax.numpy as jnp
from jax import lax
from jax.experimental import pallas as pl
from jax.experimental.pallas import tpu as pltpu
from jax.sharding import Mesh
from jax.sharding import PartitionSpec as P

D = 2048
TOK = 128
EXP = 32
CAP = 16
ROWS = EXP * CAP
WIDE = 256
FF = 64
HEADS = 4
HD = 64
STATE = 128
PLAN = ((1, True), (1, False), (3, True), (3, False), (4, True), (2, True), (2, False), (0, True))
SP = ("z", "x")
TP = ("y", "core")
GRANT = 16 * 1024 * 1024
BF = jnp.bfloat16
F32 = jnp.float32


def iota(shape, dim):
    return lax.broadcasted_iota(jnp.int32, shape, dim)


def mm(a, b, precision=None):
    return lax.dot_general(a, b, (((1,), (0,)), ((), ())), precision=precision, preferred_element_type=F32)


def mm_nt(a, b):
    return lax.dot_general(a, b, (((1,), (1,)), ((), ())), preferred_element_type=F32)


def mm_parts(left, right, product):
    total = None
    for i, a in enumerate(left):
        for j, b in enumerate(right):
            if i + j < 2:
                part = product(a, b)
                total = part if total is None else total + part
    return total


def two_parts(value):
    high = value.astype(BF)
    return high, (value - high.astype(F32)).astype(BF)


def chunk_ids(slot):
    y, core = slot >> 1, slot & 1
    turn = 2 * core - 1
    near, far, beyond, home = (y + turn) & 3, (y - turn) & 3, (y + 2) & 3, y & 3
    mine, theirs = core, 1 - core
    return (2 * home + mine, 2 * home + theirs, 2 * near + mine, 2 * near + theirs, 2 * beyond + mine,
            2 * far + theirs, 2 * far + mine, 2 * beyond + theirs)


def columns(row):
    return jnp.broadcast_to(row, (8, row.shape[1])).T[:, 0:1]


def vmem():
    return pl.BlockSpec(memory_space=pltpu.VMEM)


def smem():
    return pl.BlockSpec(memory_space=pltpu.SMEM)


def call(kernel, outs, specs, args, flops=0):
    return pl.pallas_call(
        kernel,
        out_shape=outs,
        in_specs=specs,
        out_specs=jax.tree.map(lambda _: vmem(), outs),
        compiler_params=pltpu.CompilerParams(vmem_limit_bytes=GRANT),
        cost_estimate=pl.CostEstimate(flops=flops, bytes_accessed=0, transcendentals=0),
    )(*args)


def prepare_kernel(where, routes, gates, mix, cot, buf, target):
    picks = routes[...]
    expert = iota((EXP, TOK), 0)
    hits = [expert == picks[k : k + 1] for k in range(2)]
    both = jnp.where(hits[0] | hits[1], 1.0, 0.0).astype(BF)
    before = jnp.where(iota((TOK, TOK), 0) < iota((TOK, TOK), 1), 1.0, 0.0).astype(BF)
    count = mm(both, before)
    row = iota((ROWS, TOK), 0)
    cots = cot[...].astype(F32)
    places, scaled, rows = [], [], []
    for k in range(2):
        slot = jnp.sum(jnp.where(hits[k], count, 0.0), axis=0, keepdims=True)
        place = picks[k : k + 1] * CAP + slot.astype(jnp.int32)
        rows.append(place)
        places.append(jnp.where(row == place, 1.0, 0.0).astype(BF))
        scaled.append((columns(gates[k : k + 1, :]) * cots).astype(BF))
    target[...] = jnp.concatenate(rows + [jnp.zeros((6, TOK), jnp.int32)], axis=0)
    toks = mm(places[0] + places[1], mix[...]).astype(BF)
    buf[:, 0:CAP, :] = toks.reshape(EXP, CAP, WIDE)
    spread = mm(jnp.concatenate(places, axis=1), jnp.concatenate(scaled, axis=0)).astype(BF)
    buf[:, CAP : 2 * CAP, :] = spread.reshape(EXP, CAP, WIDE)


def prepare(quarter, routes, gates, mixed, cotangent):
    whole = lambda i, q: (0, 0)
    part = lambda i, q: (0, lax.rem(q[0], 8))
    return pl.pallas_call(
        prepare_kernel,
        out_shape=(
            jax.ShapeDtypeStruct((EXP, 2 * CAP, WIDE), BF),
            jax.ShapeDtypeStruct((8, TOK), jnp.int32),
        ),
        grid_spec=pltpu.PrefetchScalarGridSpec(
            num_scalar_prefetch=1,
            grid=(1,),
            in_specs=[
                pl.BlockSpec((2, TOK), whole),
                pl.BlockSpec((2, TOK), whole),
                pl.BlockSpec((TOK, WIDE), part),
                pl.BlockSpec((TOK, WIDE), part),
            ],
            out_specs=(
                pl.BlockSpec((EXP, 2 * CAP, WIDE), lambda i, q: (0, 0, 0)),
                pl.BlockSpec((8, TOK), whole),
            ),
        ),
        name="prepare",
    )(quarter, routes, gates, mixed, cotangent)


def row_blocks(chunk):
    toks = chunk[:, 0:CAP, :].reshape(ROWS, WIDE)
    cots = chunk[:, CAP : 2 * CAP, :].reshape(ROWS, WIDE)
    return toks, cots


def gate_rows(own, other, at):
    return jnp.concatenate([own[0, :, at], other[0, :, at], own[1, :, at], other[1, :, at]], axis=0)


def expert_kernel(where, *refs):
    chunks = refs[:8]
    own, other = refs[8:10]
    outs = refs[10:18]
    g_gate, g_up, g_hid = refs[18:]
    ids = chunk_ids(where[0])
    pre = jnp.zeros((ROWS, 4 * FF), F32)
    grad_hidden = jnp.zeros((ROWS, 2 * FF), F32)
    for k in range(8):
        at = pl.ds(pl.multiple_of(ids[k] * WIDE, WIDE), WIDE)
        toks, cots = row_blocks(chunks[k])
        pre = pre + mm_nt(toks, gate_rows(own, other, at))
        grad_hidden = grad_hidden + mm_nt(cots, jnp.concatenate([own[2, :, at], other[2, :, at]], axis=0))
    pre_gate = pre[:, : 2 * FF]
    pre_up = pre[:, 2 * FF :]
    logistic = 1.0 / (1.0 + jnp.exp(-pre_gate))
    active = pre_gate * logistic
    slope = logistic * (1.0 + pre_gate * (1.0 - logistic))
    gate = (grad_hidden * pre_up * slope).astype(BF)
    up = (grad_hidden * active).astype(BF)
    g_gate[...] = gate
    g_up[...] = up
    g_hid[...] = (active * pre_up).astype(BF)
    grads = jnp.concatenate([gate, up], axis=1)
    y, core = where[0] >> 1, where[0] & 1
    step = 1 - 2 * core
    for out, (k, same) in zip(outs, PLAN):
        chip = (y + step * k + 8) & 7
        side = core if same else 1 - core
        at = pl.ds(pl.multiple_of((2 * chip + side) * TOK, TOK), TOK)
        out[...] = mm(grads, gate_rows(own, other, at)).astype(BF)


def weights_kernel(where, *refs):
    chunks = refs[:8]
    g_gate, g_up, g_hid, d_gate, d_up, d_down = refs[8:]
    gates = jnp.concatenate([g_gate[...].T[:FF], g_up[...].T[:FF]], axis=0)
    hidden = g_hid[...].T[:FF]
    ids = chunk_ids(where[0])
    for k in range(8):
        at = pl.ds(pl.multiple_of(ids[k] * WIDE, WIDE), WIDE)
        toks, cots = row_blocks(chunks[k])
        both = mm(gates, toks).astype(BF)
        d_gate[:, at] = both[:FF]
        d_up[:, at] = both[FF:]
        d_down[:, at] = mm(hidden, cots).astype(BF)


def fold_kernel(*refs):
    total = refs[0][...].astype(F32)
    for part in refs[1:8]:
        total = total + part[...].astype(F32)
    refs[8][...] = total.astype(BF).reshape(EXP, CAP, TOK)


def combine_kernel(where, target, rows, cotangent, out, cot, arrived):
    at = pl.ds(pl.multiple_of(where[0] * TOK, TOK), TOK)
    copy = pltpu.make_async_copy(cotangent.at[:, at], cot, arrived)
    copy.start()
    lane = iota((TOK, ROWS), 1)
    places = target[...].T
    pick = jnp.where((lane == places[:, 0:1]) | (lane == places[:, 1:2]), 1.0, 0.0).astype(BF)
    total = mm(pick, rows[...].reshape(ROWS, TOK))
    copy.wait()
    out[...] = (cot[...].astype(F32) + total).astype(BF)


def combine(slot, target, rows, cotangent):
    return pl.pallas_call(
        combine_kernel,
        out_shape=jax.ShapeDtypeStruct((TOK, TOK), BF),
        in_specs=[smem(), vmem(), vmem(), pl.BlockSpec(memory_space=pltpu.HBM)],
        out_specs=vmem(),
        scratch_shapes=[pltpu.VMEM((TOK, TOK), BF), pltpu.SemaphoreType.DMA],
        compiler_params=pltpu.CompilerParams(vmem_limit_bytes=GRANT),
        name="combine",
    )(slot, target, rows, cotangent)


def project_kernel(gathered, weight, gate_pre, mixer, logs, read, d_gate, grad_y, run, buf, rest):
    whole = jnp.concatenate([gathered[k * TOK : (k + 1) * TOK, :] for k in range(16)], axis=1)
    back = mm_nt(whole, weight[...])
    pre = gate_pre[...].astype(F32)
    saved = mixer[...].astype(F32)
    logistic = 1.0 / (1.0 + jnp.exp(-pre))
    active = pre * logistic
    d_gate[...] = (back * saved * (logistic * (1.0 + pre * (1.0 - logistic)))).astype(BF)
    gated = (saved * active).astype(BF)
    for k in range(8):
        turned = whole[:, k * WIDE : (k + 1) * WIDE].T
        part = mm(turned, gated).astype(BF).reshape(4, FF, WIDE)
        buf[4 * k : 4 * k + 4, 0:EXP, :] = part[:, 0:EXP]
        rest[4 * k : 4 * k + 4] = part[:, EXP:]
    grad = back * active
    grad_y[...] = grad
    upto = jnp.where(iota((TOK, TOK), 0) <= iota((TOK, TOK), 1), 1.0, 0.0)
    rates = jnp.concatenate([logs[...], jnp.zeros((4, TOK), F32)], axis=0)
    running = mm(rates, upto, lax.Precision.HIGHEST)
    run[...] = running
    start = jnp.exp(running)
    turned = grad.T
    scale = jnp.concatenate([jnp.broadcast_to(start[j : j + 1], (HD, TOK)) for j in range(HEADS)], axis=0)
    high, low = two_parts(turned * scale)
    state = mm(high, read[...]) + mm(low, read[...])
    total = running[0:HEADS, TOK - 1 : TOK]
    first = total.astype(BF).astype(F32)
    second = (total - first).astype(BF).astype(F32)
    third = total - first - second
    line = iota((8, STATE), 0)
    notes = []
    for j in range(HEADS):
        note = jnp.where(line == 0, first[j : j + 1], jnp.where(line == 1, second[j : j + 1], third[j : j + 1]))
        note = jnp.where(line < 3, note, 0.0)
        notes.append(jnp.broadcast_to(note[None], (EXP // HEADS, 8, STATE)))
    buf[:, EXP:, 0:STATE] = state.reshape(EXP, 8, STATE).astype(BF)
    buf[:, EXP:, STATE:] = jnp.concatenate(notes, axis=0).astype(BF)


def scan_kernel(received, rest, out):
    out[:, 0:EXP, :] = rest[...]
    state = jnp.zeros((8, STATE), F32)
    for k in reversed(range(EXP)):
        high, low = two_parts(state)
        out[k, EXP:, 0:STATE] = high
        out[k, EXP:, STATE:] = low
        if k > 0:
            piece = received[k, EXP:, :].astype(F32)
            note = piece[:, STATE:]
            log = note[0:1] + note[1:2] + note[2:3]
            state = jnp.exp(log) * state + piece[:, :STATE]


def inner_kernel(grad_y, values, write, read, run, entry, dx, dw, dr):
    running = run[...]
    cols = running.T
    grads = grad_y[...]
    vals = values[...]
    cross = mm_nt(write[...], read[...])
    later = iota((TOK, TOK), 1) >= iota((TOK, TOK), 0)
    total = jnp.zeros((TOK, TOK), F32)
    parts = []
    starts = []
    for j in range(HEADS):
        spread = running[j : j + 1] - cols[:, j : j + 1]
        decay = jnp.where(later, jnp.exp(jnp.where(later, spread, 0.0)), 0.0)
        grad = grads[:, j * HD : (j + 1) * HD]
        halves = two_parts(grad)
        parts.append(mm_parts(two_parts(cross * decay), halves, mm))
        total = total + mm_parts((vals[:, j * HD : (j + 1) * HD],), halves, mm_nt) * decay
        starts.append(grad * jnp.exp(cols[:, j : j + 1]))
    dx[...] = jnp.concatenate(parts, axis=1)
    dw[...] = mm_parts(two_parts(total), (read[...],), mm)
    entry_rows = two_parts(entry[...].reshape(HEADS * HD, STATE))
    first = mm_parts(two_parts(total.T), (write[...],), mm)
    dr[...] = first + mm_parts(two_parts(jnp.concatenate(starts, axis=1)), entry_rows, mm)


def outer_kernel(dx, dw, values, write, run, received, second, d_values, d_write, d_out):
    running = run[...]
    ends = jnp.exp(running[:, TOK - 1 : TOK] - running).T
    scale = jnp.concatenate([jnp.broadcast_to(ends[:, j : j + 1], (TOK, HD)) for j in range(HEADS)], axis=1)
    high = second[:, EXP:, 0:STATE].reshape(HEADS * HD, STATE)
    low = second[:, EXP:, STATE:].reshape(HEADS * HD, STATE)
    d_values[...] = (dx[...] + scale * (mm_nt(write[...], high) + mm_nt(write[...], low))).astype(BF)
    top, rest = two_parts(values[...].astype(F32) * scale)
    d_write[...] = dw[...] + mm(top, high) + mm(top, low) + mm(rest, high)
    for at, block in ((0, received), (EXP, second)):
        total = block[0, 0:EXP, :].astype(F32)
        for k in range(1, EXP):
            total = total + block[k, 0:EXP, :].astype(F32)
        d_out[at : at + EXP, :] = total


def step(mixed, cotangent, routes, gates, w_gate, w_up, w_down, out_weight, gate_pre, mixer_out, values,
         write_keys, read_keys, log_decay, entry_states):
    shape = jax.ShapeDtypeStruct
    swap = [(0, 1), (1, 0)]
    def route(k, same):
        pairs = []
        for y in range(8):
            pairs.append((2 * y, 2 * ((y + k) % 8) + (0 if same else 1)))
            pairs.append((2 * y + 1, 2 * ((y - k) % 8) + (1 if same else 0)))
        return pairs

    ring = route(1, True)
    slot = lax.axis_index(TP).astype(jnp.int32).reshape(1)
    own = jnp.stack([w_gate[0].T, w_up[0].T, w_down[0]])
    other = lax.ppermute(own, "core", swap)
    buf, target = prepare(slot, routes.T, gates.T, mixed, cotangent)
    c0 = lax.all_to_all(buf, SP, 0, 0, tiled=True)
    c2 = lax.ppermute(c0, TP, ring)
    c1 = lax.ppermute(c0, "core", swap)
    c3 = lax.ppermute(c1, TP, ring)
    c4 = lax.ppermute(c2, TP, ring)
    moved, other = lax.optimization_barrier((c2, other))
    c5 = lax.ppermute(moved, "core", swap)
    c6 = lax.ppermute(c3, "core", swap)
    c7 = lax.ppermute(c4, "core", swap)
    chunks = (c0, c1, c2, c3, c4, c5, c6, c7)
    grad = shape((ROWS, 2 * FF), BF)
    thin = shape((ROWS, TOK), BF)
    *parts, g_gate, g_up, g_hid = call(
        expert_kernel, (thin,) * 8 + (grad, grad, grad),
        [smem()] + [vmem()] * 10, (slot, *chunks, own, other))
    pieces = []
    for k, (far, same) in enumerate(PLAN[:7]):
        pieces.append(lax.ppermute(parts[k], TP, route(far, same)))
    wide = shape((FF, D), BF)
    d_wg, d_wu, d_wd = call(
        weights_kernel, (wide, wide, wide),
        [smem()] + [vmem()] * 11, (slot, *chunks, g_gate, g_up, g_hid), flops=10**9)
    pieces, d_wg, d_wu, d_wd = lax.optimization_barrier((pieces, d_wg, d_wu, d_wd))
    summed = call(fold_kernel, shape((EXP, CAP, TOK), BF), [vmem()] * 8, (*pieces, parts[7]))
    back = lax.all_to_all(summed, SP, 0, 0, tiled=True)
    d_input = combine(slot, target, back, cotangent)
    whole = lax.all_gather(d_input, TP, axis=0, tiled=True)
    flat = shape((TOK, HEADS * HD), BF)
    d_gate, grad_y, run, sent, rest = call(
        project_kernel,
        (flat, shape((TOK, HEADS * HD), F32), shape((8, TOK), F32), shape((EXP, EXP + 8, WIDE), BF),
         shape((EXP, EXP, WIDE), BF)),
        [vmem()] * 6, (whole, out_weight, gate_pre, mixer_out, log_decay, read_keys))
    square = shape((TOK, STATE), F32)
    dx, dw, d_read = call(
        inner_kernel, (shape((TOK, HEADS * HD), F32), square, square),
        [vmem()] * 6, (grad_y, values, write_keys, read_keys, run, entry_states[0]), flops=10**9)
    received = lax.all_to_all(sent, SP, 0, 0, tiled=True)
    received, dx, dw, d_read = lax.optimization_barrier((received, dx, dw, d_read))
    states = call(scan_kernel, shape((EXP, EXP + 8, WIDE), BF), [vmem()] * 2, (received, rest))
    second = lax.all_to_all(states, SP, 0, 0, tiled=True)
    d_values, d_write, d_out_weight = call(
        outer_kernel, (flat, square, shape((D // EXP, HEADS * HD), F32)), [vmem()] * 7,
        (dx, dw, values, write_keys, run, received, second))
    return (d_wg.T[None], d_wu.T[None], d_wd[None], d_out_weight, d_input, d_values, d_write, d_read, d_gate)


def solution(mesh):
    finer = Mesh(mesh.devices.reshape(8, 4, 8, 2), ("z", "x", "y", "core"))
    return jax.shard_map(
        step,
        mesh=finer,
        in_specs=(
            P(SP, None),
            P(SP, None),
            P(SP, None),
            P(SP, None),
            P(SP, None, TP),
            P(SP, None, TP),
            P(SP, TP, None),
            P(TP, None),
            P(SP, TP),
            P(SP, TP),
            P(SP, TP),
            P(SP, TP),
            P(SP, TP),
            P(TP, SP),
            P(SP, TP, None, None),
        ),
        out_specs=(
            P(SP, None, TP),
            P(SP, None, TP),
            P(SP, TP, None),
            P(SP, TP),
            P(SP, TP),
            P(SP, TP),
            P(SP, TP),
            P(SP, TP),
            P(SP, TP),
        ),
        check_vma=False,
    )
```

```python
import jax
import jax.numpy as jnp
from jax import lax
from jax.experimental import pallas as pl
from jax.experimental.pallas import tpu as pltpu
from jax.sharding import Mesh
from jax.sharding import PartitionSpec as P

D = 2048
TOK = 128
EXP = 32
CAP = 16
ROWS = EXP * CAP
WIDE = 256
FF = 64
HEADS = 4
HD = 64
STATE = 128
SP = ("z", "x")
TP = ("y", "core")
GRANT = 16 * 1024 * 1024
BF = jnp.bfloat16
F32 = jnp.float32


def iota(shape, dim):
    return lax.broadcasted_iota(jnp.int32, shape, dim)


def mm(a, b, precision=None):
    return lax.dot_general(a, b, (((1,), (0,)), ((), ())), precision=precision, preferred_element_type=F32)


def mm_nt(a, b):
    return lax.dot_general(a, b, (((1,), (1,)), ((), ())), preferred_element_type=F32)


def mm_parts(left, right, product):
    total = None
    for i, a in enumerate(left):
        for j, b in enumerate(right):
            if i + j < 2:
                part = product(a, b)
                total = part if total is None else total + part
    return total


def two_parts(value):
    high = value.astype(BF)
    return high, (value - high.astype(F32)).astype(BF)


def chunk_ids(slot):
    y, core = slot >> 1, slot & 1
    turn = 2 * core - 1
    near, far, beyond, home = (y + turn) & 3, (y - turn) & 3, (y + 2) & 3, y & 3
    mine, theirs = core, 1 - core
    return (2 * home + mine, 2 * home + theirs, 2 * near + mine, 2 * near + theirs, 2 * beyond + mine,
            2 * far + theirs, 2 * far + mine, 2 * beyond + theirs)


def columns(row):
    return jnp.broadcast_to(row, (8, row.shape[1])).T[:, 0:1]


def vmem():
    return pl.BlockSpec(memory_space=pltpu.VMEM)


def smem():
    return pl.BlockSpec(memory_space=pltpu.SMEM)


def call(kernel, outs, specs, args, flops=0, scratch=()):
    return pl.pallas_call(
        kernel,
        out_shape=outs,
        in_specs=specs,
        out_specs=jax.tree.map(lambda _: vmem(), outs),
        scratch_shapes=scratch,
        compiler_params=pltpu.CompilerParams(vmem_limit_bytes=GRANT),
        cost_estimate=pl.CostEstimate(flops=flops, bytes_accessed=0, transcendentals=0),
    )(*args)


def prepare_kernel(where, routes, gates, mix, cot, buf, target):
    picks = routes[...]
    expert = iota((EXP, TOK), 0)
    hits = [expert == picks[k : k + 1] for k in range(2)]
    both = jnp.where(hits[0] | hits[1], 1.0, 0.0).astype(BF)
    before = jnp.where(iota((TOK, TOK), 0) < iota((TOK, TOK), 1), 1.0, 0.0).astype(BF)
    count = mm(both, before)
    row = iota((ROWS, TOK), 0)
    cots = cot[...].astype(F32)
    places, scaled, rows = [], [], []
    for k in range(2):
        slot = jnp.sum(jnp.where(hits[k], count, 0.0), axis=0, keepdims=True)
        place = picks[k : k + 1] * CAP + slot.astype(jnp.int32)
        rows.append(place)
        places.append(jnp.where(row == place, 1.0, 0.0).astype(BF))
        scaled.append((columns(gates[k : k + 1, :]) * cots).astype(BF))
    target[...] = jnp.concatenate(rows + [jnp.zeros((6, TOK), jnp.int32)], axis=0)
    toks = mm(places[0] + places[1], mix[...]).astype(BF)
    buf[:, 0:CAP, :] = toks.reshape(EXP, CAP, WIDE)
    spread = mm(jnp.concatenate(places, axis=1), jnp.concatenate(scaled, axis=0)).astype(BF)
    buf[:, CAP : 2 * CAP, :] = spread.reshape(EXP, CAP, WIDE)


def prepare(quarter, routes, gates, mixed, cotangent):
    whole = lambda i, q: (0, 0)
    part = lambda i, q: (0, lax.rem(q[0], 8))
    return pl.pallas_call(
        prepare_kernel,
        out_shape=(
            jax.ShapeDtypeStruct((EXP, 2 * CAP, WIDE), BF),
            jax.ShapeDtypeStruct((8, TOK), jnp.int32),
        ),
        grid_spec=pltpu.PrefetchScalarGridSpec(
            num_scalar_prefetch=1,
            grid=(1,),
            in_specs=[
                pl.BlockSpec((2, TOK), whole),
                pl.BlockSpec((2, TOK), whole),
                pl.BlockSpec((TOK, WIDE), part),
                pl.BlockSpec((TOK, WIDE), part),
            ],
            out_specs=(
                pl.BlockSpec((EXP, 2 * CAP, WIDE), lambda i, q: (0, 0, 0)),
                pl.BlockSpec((8, TOK), whole),
            ),
        ),
        name="prepare",
    )(quarter, routes, gates, mixed, cotangent)


def row_blocks(chunk):
    toks = chunk[:, 0:CAP, :].reshape(ROWS, WIDE)
    cots = chunk[:, CAP : 2 * CAP, :].reshape(ROWS, WIDE)
    return toks, cots


def gate_rows(own, other, at):
    return jnp.concatenate([own[0, :, at], other[0, :, at], own[1, :, at], other[1, :, at]], axis=0)


def expert_kernel(where, *refs):
    chunks = refs[:8]
    own, other, near, mid, far, last, home, g_gate, g_up, g_hid = refs[8:]
    ids = chunk_ids(where[0])
    pre = jnp.zeros((ROWS, 4 * FF), F32)
    grad_hidden = jnp.zeros((ROWS, 2 * FF), F32)
    for k in range(8):
        at = pl.ds(pl.multiple_of(ids[k] * WIDE, WIDE), WIDE)
        toks, cots = row_blocks(chunks[k])
        pre = pre + mm_nt(toks, gate_rows(own, other, at))
        grad_hidden = grad_hidden + mm_nt(cots, jnp.concatenate([own[2, :, at], other[2, :, at]], axis=0))
    pre_gate = pre[:, : 2 * FF]
    pre_up = pre[:, 2 * FF :]
    logistic = 1.0 / (1.0 + jnp.exp(-pre_gate))
    active = pre_gate * logistic
    slope = logistic * (1.0 + pre_gate * (1.0 - logistic))
    gate = (grad_hidden * pre_up * slope).astype(BF)
    up = (grad_hidden * active).astype(BF)
    g_gate[...] = gate
    g_up[...] = up
    g_hid[...] = (active * pre_up).astype(BF)
    grads = jnp.concatenate([gate, up], axis=1)
    y, core = where[0] >> 1, where[0] & 1
    step = 1 - 2 * core
    for k, out in ((4, last), (3, far), (2, mid), (1, near), (0, home)):
        chip = (y + step * k + 8) & 7
        start = chip * WIDE if k in (1, 2, 3) else chip * WIDE + core * TOK
        size = out.shape[1]
        at = pl.ds(pl.multiple_of(start, TOK), size)
        out[...] = mm(grads, gate_rows(own, other, at)).astype(BF)


def weights_kernel(where, *refs):
    chunks = refs[:8]
    g_gate, g_up, g_hid, d_gate, d_up, d_down = refs[8:]
    gates = jnp.concatenate([g_gate[...].T[:FF], g_up[...].T[:FF]], axis=0)
    hidden = g_hid[...].T[:FF]
    ids = chunk_ids(where[0])
    for k in range(8):
        at = pl.ds(pl.multiple_of(ids[k] * WIDE, WIDE), WIDE)
        toks, cots = row_blocks(chunks[k])
        both = mm(gates, toks).astype(BF)
        d_gate[:, at] = both[:FF]
        d_up[:, at] = both[FF:]
        d_down[:, at] = mm(hidden, cots).astype(BF)


def fold_kernel(where, near, mid, far, last, home, keep, give):
    total = near[...].astype(F32) + mid[...].astype(F32) + far[...].astype(F32)
    first = total[:, :TOK]
    second = total[:, TOK:]
    top = where[0] & 1 == 0
    keep[...] = jnp.where(top, first, second) + last[...].astype(F32) + home[...].astype(F32)
    give[...] = jnp.where(top, second, first).astype(BF)


def combine_kernel(where, target, rows, cotangent, out, cot, arrived):
    at = pl.ds(pl.multiple_of(where[0] * TOK, TOK), TOK)
    copy = pltpu.make_async_copy(cotangent.at[:, at], cot, arrived)
    copy.start()
    lane = iota((TOK, ROWS), 1)
    places = target[...].T
    pick = jnp.where((lane == places[:, 0:1]) | (lane == places[:, 1:2]), 1.0, 0.0).astype(BF)
    total = mm(pick, rows[...].reshape(ROWS, TOK))
    copy.wait()
    out[...] = (cot[...].astype(F32) + total).astype(BF)


def combine(slot, target, rows, cotangent):
    return pl.pallas_call(
        combine_kernel,
        out_shape=jax.ShapeDtypeStruct((TOK, TOK), BF),
        in_specs=[smem(), vmem(), vmem(), pl.BlockSpec(memory_space=pltpu.HBM)],
        out_specs=vmem(),
        scratch_shapes=[pltpu.VMEM((TOK, TOK), BF), pltpu.SemaphoreType.DMA],
        compiler_params=pltpu.CompilerParams(vmem_limit_bytes=GRANT),
        name="combine",
    )(slot, target, rows, cotangent)


def project_kernel(spot, gathered, weight, gate_pre, mixer, logs, read, d_gate, grad_y, run, buf, *outs):
    quarters = outs[4]
    whole = jnp.concatenate([gathered[k * TOK : (k + 1) * TOK, :] for k in range(16)], axis=1)
    back = mm_nt(whole, weight[...])
    pre = gate_pre[...].astype(F32)
    saved = mixer[...].astype(F32)
    logistic = 1.0 / (1.0 + jnp.exp(-pre))
    active = pre * logistic
    d_gate[...] = (back * saved * (logistic * (1.0 + pre * (1.0 - logistic)))).astype(BF)
    gated = (saved * active).astype(BF)
    for k in range(8):
        turned = whole[:, k * WIDE : (k + 1) * WIDE].T
        part = mm(turned, gated).astype(BF)
        for r in range(4):
            half = part[:, (r & 1) * TOK : (r & 1) * TOK + TOK].reshape(4, FF, TOK)
            quarters[r, 4 * k : 4 * k + 4] = half[:, (r >> 1) * EXP : (r >> 1) * EXP + EXP]
    for k in range(4):
        outs[k][...] = quarters[(spot[0] + k) & 3]
    grad = back * active
    grad_y[...] = grad
    upto = jnp.where(iota((TOK, TOK), 0) <= iota((TOK, TOK), 1), 1.0, 0.0)
    rates = jnp.concatenate([logs[...], jnp.zeros((4, TOK), F32)], axis=0)
    running = mm(rates, upto, lax.Precision.HIGHEST)
    run[...] = running
    start = jnp.exp(running)
    turned = grad.T
    scale = jnp.concatenate([jnp.broadcast_to(start[j : j + 1], (HD, TOK)) for j in range(HEADS)], axis=0)
    high, low = two_parts(turned * scale)
    state = mm(high, read[...]) + mm(low, read[...])
    total = running[0:HEADS, TOK - 1 : TOK]
    first = total.astype(BF).astype(F32)
    second = (total - first).astype(BF).astype(F32)
    third = total - first - second
    line = iota((8, STATE), 0)
    notes = []
    for j in range(HEADS):
        note = jnp.where(line == 0, first[j : j + 1], jnp.where(line == 1, second[j : j + 1], third[j : j + 1]))
        note = jnp.where(line < 3, note, 0.0)
        notes.append(jnp.broadcast_to(note[None], (EXP // HEADS, 8, STATE)))
    sent = jnp.concatenate([state.reshape(EXP, 8, STATE), jnp.concatenate(notes, axis=0)], axis=1)
    buf[...] = sent.astype(BF)


def scan_kernel(received, p0, p1, p2, p3, out):
    total = p0[...].astype(F32) + p1[...].astype(F32) + p2[...].astype(F32) + p3[...].astype(F32)
    out[:, 0:EXP, :] = total.astype(BF)
    state = jnp.zeros((8, STATE), F32)
    for k in reversed(range(EXP)):
        high, low = two_parts(state)
        out[k, EXP:, :] = jnp.concatenate([high.astype(F32), low.astype(F32)], axis=0).astype(BF)
        if k > 0:
            piece = received[k].astype(F32)
            log = piece[8:9] + piece[9:10] + piece[10:11]
            state = jnp.exp(log) * state + piece[0:8]


def inner_kernel(grad_y, values, write, read, run, entry, dx, dw, dr):
    running = run[...]
    cols = running.T
    grads = grad_y[...]
    vals = values[...]
    cross = mm_nt(write[...], read[...])
    later = iota((TOK, TOK), 1) >= iota((TOK, TOK), 0)
    total = jnp.zeros((TOK, TOK), F32)
    parts = []
    starts = []
    for j in range(HEADS):
        spread = running[j : j + 1] - cols[:, j : j + 1]
        decay = jnp.where(later, jnp.exp(jnp.where(later, spread, 0.0)), 0.0)
        grad = grads[:, j * HD : (j + 1) * HD]
        halves = two_parts(grad)
        parts.append(mm_parts(two_parts(cross * decay), halves, mm))
        total = total + mm_parts((vals[:, j * HD : (j + 1) * HD],), halves, mm_nt) * decay
        starts.append(grad * jnp.exp(cols[:, j : j + 1]))
    dx[...] = jnp.concatenate(parts, axis=1)
    dw[...] = mm_parts(two_parts(total), (read[...],), mm)
    entry_rows = two_parts(entry[...].reshape(HEADS * HD, STATE))
    first = mm_parts(two_parts(total.T), (write[...],), mm)
    dr[...] = first + mm_parts(two_parts(jnp.concatenate(starts, axis=1)), entry_rows, mm)


def outer_kernel(dx, dw, values, write, run, second, d_values, d_write, d_out):
    running = run[...]
    ends = jnp.exp(running[:, TOK - 1 : TOK] - running).T
    scale = jnp.concatenate([jnp.broadcast_to(ends[:, j : j + 1], (TOK, HD)) for j in range(HEADS)], axis=1)
    later = second[:, EXP:, :].astype(F32)
    high = later[:, 0:8].reshape(HEADS * HD, STATE).astype(BF)
    low = later[:, 8:16].reshape(HEADS * HD, STATE).astype(BF)
    d_values[...] = (dx[...] + scale * (mm_nt(write[...], high) + mm_nt(write[...], low))).astype(BF)
    top, rest = two_parts(values[...].astype(F32) * scale)
    d_write[...] = dw[...] + mm(top, high) + mm(top, low) + mm(rest, high)
    for r in range(4):
        total = second[r, 0:EXP, :].astype(F32)
        for k in range(1, 8):
            total = total + second[4 * k + r, 0:EXP, :].astype(F32)
        d_out[(r >> 1) * EXP : (r >> 1) * EXP + EXP, (r & 1) * TOK : (r & 1) * TOK + TOK] = total


def step(mixed, cotangent, routes, gates, w_gate, w_up, w_down, out_weight, gate_pre, mixer_out, values,
         write_keys, read_keys, log_decay, entry_states):
    shape = jax.ShapeDtypeStruct
    swap = [(0, 1), (1, 0)]
    rings = []
    for k in range(1, 5):
        up = [(2 * y, 2 * ((y + k) % 8)) for y in range(8)]
        rings.append(up + [(2 * y + 1, 2 * ((y - k) % 8) + 1) for y in range(8)])
    ring = rings[0]
    slot = lax.axis_index(TP).astype(jnp.int32).reshape(1)
    own = jnp.stack([w_gate[0].T, w_up[0].T, w_down[0]])
    other = lax.ppermute(own, "core", swap)
    buf, target = prepare(slot, routes.T, gates.T, mixed, cotangent)
    c0 = lax.all_to_all(buf, SP, 0, 0, tiled=True)
    c2 = lax.ppermute(c0, TP, ring)
    c1 = lax.ppermute(c0, "core", swap)
    c3 = lax.ppermute(c1, TP, ring)
    c4 = lax.ppermute(c2, TP, ring)
    moved, other = lax.optimization_barrier((c2, other))
    c5 = lax.ppermute(moved, "core", swap)
    c6 = lax.ppermute(c3, "core", swap)
    c7 = lax.ppermute(c4, "core", swap)
    chunks = (c0, c1, c2, c3, c4, c5, c6, c7)
    grad = shape((ROWS, 2 * FF), BF)
    full, thin = shape((ROWS, WIDE), BF), shape((ROWS, TOK), BF)
    *parts, home, g_gate, g_up, g_hid = call(
        expert_kernel, (full, full, full, thin, thin, grad, grad, grad),
        [smem()] + [vmem()] * 10, (slot, *chunks, own, other))
    pieces = []
    for k in range(4):
        pieces.append(lax.ppermute(parts[k], TP, rings[k]))
    wide = shape((FF, D), BF)
    d_wg, d_wu, d_wd = call(
        weights_kernel, (wide, wide, wide),
        [smem()] + [vmem()] * 11, (slot, *chunks, g_gate, g_up, g_hid), flops=10**9)
    pieces, d_wg, d_wu, d_wd = lax.optimization_barrier((pieces, d_wg, d_wu, d_wd))
    keep, give = call(
        fold_kernel, (shape((ROWS, TOK), F32), thin),
        [smem()] + [vmem()] * 5, (slot, *pieces, home))
    taken = lax.ppermute(give, "core", swap)
    summed = (keep + taken.astype(F32)).astype(BF).reshape(EXP, CAP, TOK)
    back = lax.all_to_all(summed, SP, 0, 0, tiled=True)
    d_input = combine(slot, target, back, cotangent)
    whole = lax.all_gather(d_input, TP, axis=0, tiled=True)
    flat = shape((TOK, HEADS * HD), BF)
    quarter = shape((EXP, EXP, TOK), BF)
    spot = lax.axis_index("x").astype(jnp.int32).reshape(1)
    d_gate, grad_y, run, sent, *shares = call(
        project_kernel,
        (flat, shape((TOK, HEADS * HD), F32), shape((8, TOK), F32), shape((EXP, 16, STATE), BF),
         quarter, quarter, quarter, quarter),
        [smem()] + [vmem()] * 6, (spot, whole, out_weight, gate_pre, mixer_out, log_decay, read_keys),
        scratch=[pltpu.VMEM((4, EXP, EXP, TOK), BF)])
    received = lax.all_to_all(sent, SP, 0, 0, tiled=True)
    for k in range(1, 4):
        shares[k] = lax.ppermute(shares[k], "x", [(i, (i + k) % 4) for i in range(4)])
    square = shape((TOK, STATE), F32)
    dx, dw, d_read = call(
        inner_kernel, (shape((TOK, HEADS * HD), F32), square, square),
        [vmem()] * 6, (grad_y, values, write_keys, read_keys, run, entry_states[0]), flops=10**9)
    received, dx, dw, d_read = lax.optimization_barrier((received, dx, dw, d_read))
    states = call(scan_kernel, shape((EXP, 48, STATE), BF), [vmem()] * 5, (received, *shares))
    second = lax.all_to_all(states, SP, 0, 0, tiled=True)
    d_values, d_write, d_out_weight = call(
        outer_kernel, (flat, square, shape((D // EXP, HEADS * HD), F32)), [vmem()] * 6,
        (dx, dw, values, write_keys, run, second))
    return (d_wg.T[None], d_wu.T[None], d_wd[None], d_out_weight, d_input, d_values, d_write, d_read, d_gate)


def solution(mesh):
    finer = Mesh(mesh.devices.reshape(8, 4, 8, 2), ("z", "x", "y", "core"))
    return jax.shard_map(
        step,
        mesh=finer,
        in_specs=(
            P(SP, None),
            P(SP, None),
            P(SP, None),
            P(SP, None),
            P(SP, None, TP),
            P(SP, None, TP),
            P(SP, TP, None),
            P(TP, None),
            P(SP, TP),
            P(SP, TP),
            P(SP, TP),
            P(SP, TP),
            P(SP, TP),
            P(TP, SP),
            P(SP, TP, None, None),
        ),
        out_specs=(
            P(SP, None, TP),
            P(SP, None, TP),
            P(SP, TP, None),
            P(SP, TP),
            P(SP, TP),
            P(SP, TP),
            P(SP, TP),
            P(SP, TP),
            P(SP, TP),
        ),
        check_vma=False,
    )
```

```python
import jax
import jax.numpy as jnp
from jax import lax
from jax.experimental import pallas as pl
from jax.experimental.pallas import tpu as pltpu
from jax.sharding import Mesh
from jax.sharding import PartitionSpec as P

D = 2048
TOK = 128
EXP = 32
CAP = 16
ROWS = EXP * CAP
WIDE = 256
FF = 64
HEADS = 4
HD = 64
STATE = 128
SP = ("z", "x")
TP = ("y", "core")
GRANT = 16 * 1024 * 1024
BF = jnp.bfloat16
F32 = jnp.float32


def iota(shape, dim):
    return lax.broadcasted_iota(jnp.int32, shape, dim)


def mm(a, b, precision=None):
    return lax.dot_general(a, b, (((1,), (0,)), ((), ())), precision=precision, preferred_element_type=F32)


def mm_nt(a, b):
    return lax.dot_general(a, b, (((1,), (1,)), ((), ())), preferred_element_type=F32)


def mm_parts(left, right, product):
    total = None
    for i, a in enumerate(left):
        for j, b in enumerate(right):
            if i + j < 2:
                part = product(a, b)
                total = part if total is None else total + part
    return total


def two_parts(value):
    high = value.astype(BF)
    return high, (value - high.astype(F32)).astype(BF)


def chunk_ids(slot):
    y, core = slot >> 1, slot & 1
    turn = 2 * core - 1
    near, far, beyond, home = (y + turn) & 3, (y - turn) & 3, (y + 2) & 3, y & 3
    mine, theirs = core, 1 - core
    return (2 * home + mine, 2 * home + theirs, 2 * near + mine, 2 * near + theirs, 2 * beyond + mine,
            2 * far + theirs, 2 * far + mine, 2 * beyond + theirs)


def columns(row):
    return jnp.broadcast_to(row, (8, row.shape[1])).T[:, 0:1]


def vmem():
    return pl.BlockSpec(memory_space=pltpu.VMEM)


def smem():
    return pl.BlockSpec(memory_space=pltpu.SMEM)


def call(kernel, outs, specs, args, flops=0, scratch=()):
    return pl.pallas_call(
        kernel,
        out_shape=outs,
        in_specs=specs,
        out_specs=jax.tree.map(lambda _: vmem(), outs),
        scratch_shapes=scratch,
        compiler_params=pltpu.CompilerParams(vmem_limit_bytes=GRANT),
        cost_estimate=pl.CostEstimate(flops=flops, bytes_accessed=0, transcendentals=0),
    )(*args)


def prepare_kernel(where, routes, gates, mix, cot, buf, target):
    picks = routes[...]
    expert = iota((EXP, TOK), 0)
    hits = [expert == picks[k : k + 1] for k in range(2)]
    both = jnp.where(hits[0] | hits[1], 1.0, 0.0).astype(BF)
    before = jnp.where(iota((TOK, TOK), 0) < iota((TOK, TOK), 1), 1.0, 0.0).astype(BF)
    count = mm(both, before)
    row = iota((ROWS, TOK), 0)
    cots = cot[...].astype(F32)
    places, scaled, rows = [], [], []
    for k in range(2):
        slot = jnp.sum(jnp.where(hits[k], count, 0.0), axis=0, keepdims=True)
        place = picks[k : k + 1] * CAP + slot.astype(jnp.int32)
        rows.append(place)
        places.append(jnp.where(row == place, 1.0, 0.0).astype(BF))
        scaled.append((columns(gates[k : k + 1, :]) * cots).astype(BF))
    target[...] = jnp.concatenate(rows + [jnp.zeros((6, TOK), jnp.int32)], axis=0)
    toks = mm(places[0] + places[1], mix[...]).astype(BF)
    buf[:, 0:CAP, :] = toks.reshape(EXP, CAP, WIDE)
    spread = mm(jnp.concatenate(places, axis=1), jnp.concatenate(scaled, axis=0)).astype(BF)
    buf[:, CAP : 2 * CAP, :] = spread.reshape(EXP, CAP, WIDE)


def prepare(quarter, routes, gates, mixed, cotangent):
    whole = lambda i, q: (0, 0)
    part = lambda i, q: (0, lax.rem(q[0], 8))
    return pl.pallas_call(
        prepare_kernel,
        out_shape=(
            jax.ShapeDtypeStruct((EXP, 2 * CAP, WIDE), BF),
            jax.ShapeDtypeStruct((8, TOK), jnp.int32),
        ),
        grid_spec=pltpu.PrefetchScalarGridSpec(
            num_scalar_prefetch=1,
            grid=(1,),
            in_specs=[
                pl.BlockSpec((2, TOK), whole),
                pl.BlockSpec((2, TOK), whole),
                pl.BlockSpec((TOK, WIDE), part),
                pl.BlockSpec((TOK, WIDE), part),
            ],
            out_specs=(
                pl.BlockSpec((EXP, 2 * CAP, WIDE), lambda i, q: (0, 0, 0)),
                pl.BlockSpec((8, TOK), whole),
            ),
        ),
        name="prepare",
    )(quarter, routes, gates, mixed, cotangent)


def row_blocks(chunk):
    toks = chunk[:, 0:CAP, :].reshape(ROWS, WIDE)
    cots = chunk[:, CAP : 2 * CAP, :].reshape(ROWS, WIDE)
    return toks, cots


def gate_rows(own, other, at):
    return jnp.concatenate([own[0, :, at], other[0, :, at], own[1, :, at], other[1, :, at]], axis=0)


def chunk_products(chunk, position, own, other):
    at = pl.ds(pl.multiple_of(position * WIDE, WIDE), WIDE)
    toks, cots = row_blocks(chunk)
    down = jnp.concatenate([own[2, :, at], other[2, :, at]], axis=0)
    return mm_nt(toks, gate_rows(own, other, at)), mm_nt(cots, down)


def early_kernel(where, *refs):
    chunks = refs[:7]
    own, other, pre, grad_hidden = refs[7:]
    ids = chunk_ids(where[0])
    first, second = chunk_products(chunks[0], ids[0], own, other)
    for k in range(1, 7):
        more = chunk_products(chunks[k], ids[k], own, other)
        first, second = first + more[0], second + more[1]
    pre[...] = first
    grad_hidden[...] = second


def expert_kernel(where, chunk, early_pre, early_hidden, own, other, *outs):
    near, mid, far, last, home, g_gate, g_up, g_hid = outs
    more = chunk_products(chunk, chunk_ids(where[0])[7], own, other)
    pre = early_pre[...] + more[0]
    grad_hidden = early_hidden[...] + more[1]
    pre_gate = pre[:, : 2 * FF]
    pre_up = pre[:, 2 * FF :]
    logistic = 1.0 / (1.0 + jnp.exp(-pre_gate))
    active = pre_gate * logistic
    slope = logistic * (1.0 + pre_gate * (1.0 - logistic))
    gate = (grad_hidden * pre_up * slope).astype(BF)
    up = (grad_hidden * active).astype(BF)
    g_gate[...] = gate
    g_up[...] = up
    g_hid[...] = (active * pre_up).astype(BF)
    grads = jnp.concatenate([gate, up], axis=1)
    y, core = where[0] >> 1, where[0] & 1
    step = 1 - 2 * core
    for k, out in ((4, last), (3, far), (2, mid), (1, near), (0, home)):
        chip = (y + step * k + 8) & 7
        start = chip * WIDE if k in (1, 2, 3) else chip * WIDE + core * TOK
        size = out.shape[1]
        at = pl.ds(pl.multiple_of(start, TOK), size)
        out[...] = mm(grads, gate_rows(own, other, at)).astype(BF)


def weights_kernel(where, *refs):
    chunks = refs[:8]
    g_gate, g_up, g_hid, d_gate, d_up, d_down = refs[8:]
    gates = jnp.concatenate([g_gate[...].T[:FF], g_up[...].T[:FF]], axis=0)
    hidden = g_hid[...].T[:FF]
    ids = chunk_ids(where[0])
    for k in range(8):
        at = pl.ds(pl.multiple_of(ids[k] * WIDE, WIDE), WIDE)
        toks, cots = row_blocks(chunks[k])
        both = mm(gates, toks).astype(BF)
        d_gate[:, at] = both[:FF]
        d_up[:, at] = both[FF:]
        d_down[:, at] = mm(hidden, cots).astype(BF)


def fold_kernel(where, near, mid, far, last, home, keep, give):
    total = near[...].astype(F32) + mid[...].astype(F32) + far[...].astype(F32)
    first = total[:, :TOK]
    second = total[:, TOK:]
    top = where[0] & 1 == 0
    keep[...] = jnp.where(top, first, second) + last[...].astype(F32) + home[...].astype(F32)
    give[...] = jnp.where(top, second, first).astype(BF)


def join_kernel(keep, taken, out):
    out[...] = (keep[...] + taken[...].astype(F32)).astype(BF).reshape(EXP, CAP, TOK)


def combine_kernel(where, target, rows, cotangent, out, cot, arrived):
    at = pl.ds(pl.multiple_of(where[0] * TOK, TOK), TOK)
    copy = pltpu.make_async_copy(cotangent.at[:, at], cot, arrived)
    copy.start()
    lane = iota((TOK, ROWS), 1)
    places = target[...].T
    pick = jnp.where((lane == places[:, 0:1]) | (lane == places[:, 1:2]), 1.0, 0.0).astype(BF)
    total = mm(pick, rows[...].reshape(ROWS, TOK))
    copy.wait()
    out[...] = (cot[...].astype(F32) + total).astype(BF)


def combine(slot, target, rows, cotangent):
    return pl.pallas_call(
        combine_kernel,
        out_shape=jax.ShapeDtypeStruct((TOK, TOK), BF),
        in_specs=[smem(), vmem(), vmem(), pl.BlockSpec(memory_space=pltpu.HBM)],
        out_specs=vmem(),
        scratch_shapes=[pltpu.VMEM((TOK, TOK), BF), pltpu.SemaphoreType.DMA],
        compiler_params=pltpu.CompilerParams(vmem_limit_bytes=GRANT),
        name="combine",
    )(slot, target, rows, cotangent)


def project_kernel(spot, gathered, weight, gate_pre, mixer, logs, read, d_gate, grad_y, run, buf, *outs):
    quarters = outs[4]
    whole = jnp.concatenate([gathered[k * TOK : (k + 1) * TOK, :] for k in range(16)], axis=1)
    back = mm_nt(whole, weight[...])
    pre = gate_pre[...].astype(F32)
    saved = mixer[...].astype(F32)
    logistic = 1.0 / (1.0 + jnp.exp(-pre))
    active = pre * logistic
    d_gate[...] = (back * saved * (logistic * (1.0 + pre * (1.0 - logistic)))).astype(BF)
    gated = (saved * active).astype(BF)
    for k in range(8):
        turned = whole[:, k * WIDE : (k + 1) * WIDE].T
        part = mm(turned, gated).astype(BF)
        for r in range(4):
            half = part[:, (r & 1) * TOK : (r & 1) * TOK + TOK].reshape(4, FF, TOK)
            quarters[r, 4 * k : 4 * k + 4] = half[:, (r >> 1) * EXP : (r >> 1) * EXP + EXP]
    for k in range(4):
        outs[k][...] = quarters[(spot[0] + k) & 3]
    grad = back * active
    grad_y[...] = grad
    upto = jnp.where(iota((TOK, TOK), 0) <= iota((TOK, TOK), 1), 1.0, 0.0)
    rates = jnp.concatenate([logs[...], jnp.zeros((4, TOK), F32)], axis=0)
    running = mm(rates, upto, lax.Precision.HIGHEST)
    run[...] = running
    start = jnp.exp(running)
    turned = grad.T
    scale = jnp.concatenate([jnp.broadcast_to(start[j : j + 1], (HD, TOK)) for j in range(HEADS)], axis=0)
    high, low = two_parts(turned * scale)
    state = mm(high, read[...]) + mm(low, read[...])
    total = running[0:HEADS, TOK - 1 : TOK]
    first = total.astype(BF).astype(F32)
    second = (total - first).astype(BF).astype(F32)
    third = total - first - second
    line = iota((8, STATE), 0)
    notes = []
    for j in range(HEADS):
        note = jnp.where(line == 0, first[j : j + 1], jnp.where(line == 1, second[j : j + 1], third[j : j + 1]))
        note = jnp.where(line < 3, note, 0.0)
        notes.append(jnp.broadcast_to(note[None], (EXP // HEADS, 8, STATE)))
    sent = jnp.concatenate([state.reshape(EXP, 8, STATE), jnp.concatenate(notes, axis=0)], axis=1)
    buf[...] = sent.astype(BF)


def scan_kernel(received, p0, p1, p2, p3, out):
    total = p0[...].astype(F32) + p1[...].astype(F32) + p2[...].astype(F32) + p3[...].astype(F32)
    out[:, 0:EXP, :] = total.astype(BF)
    state = jnp.zeros((8, STATE), F32)
    for k in reversed(range(EXP)):
        high, low = two_parts(state)
        out[k, EXP:, :] = jnp.concatenate([high.astype(F32), low.astype(F32)], axis=0).astype(BF)
        if k > 0:
            piece = received[k].astype(F32)
            log = piece[8:9] + piece[9:10] + piece[10:11]
            state = jnp.exp(log) * state + piece[0:8]


def inner_kernel(grad_y, values, write, read, run, entry, dx, dw, dr):
    running = run[...]
    cols = running.T
    grads = grad_y[...]
    vals = values[...]
    cross = mm_nt(write[...], read[...])
    later = iota((TOK, TOK), 1) >= iota((TOK, TOK), 0)
    total = jnp.zeros((TOK, TOK), F32)
    parts = []
    starts = []
    for j in range(HEADS):
        spread = running[j : j + 1] - cols[:, j : j + 1]
        decay = jnp.where(later, jnp.exp(jnp.where(later, spread, 0.0)), 0.0)
        grad = grads[:, j * HD : (j + 1) * HD]
        halves = two_parts(grad)
        parts.append(mm_parts(two_parts(cross * decay), halves, mm))
        total = total + mm_parts((vals[:, j * HD : (j + 1) * HD],), halves, mm_nt) * decay
        starts.append(grad * jnp.exp(cols[:, j : j + 1]))
    dx[...] = jnp.concatenate(parts, axis=1)
    dw[...] = mm_parts(two_parts(total), (read[...],), mm)
    entry_rows = two_parts(entry[...].reshape(HEADS * HD, STATE))
    first = mm_parts(two_parts(total.T), (write[...],), mm)
    dr[...] = first + mm_parts(two_parts(jnp.concatenate(starts, axis=1)), entry_rows, mm)


def outer_kernel(dx, dw, values, write, run, second, d_values, d_write, d_out):
    running = run[...]
    ends = jnp.exp(running[:, TOK - 1 : TOK] - running).T
    scale = jnp.concatenate([jnp.broadcast_to(ends[:, j : j + 1], (TOK, HD)) for j in range(HEADS)], axis=1)
    later = second[:, EXP:, :].astype(F32)
    high = later[:, 0:8].reshape(HEADS * HD, STATE).astype(BF)
    low = later[:, 8:16].reshape(HEADS * HD, STATE).astype(BF)
    d_values[...] = (dx[...] + scale * (mm_nt(write[...], high) + mm_nt(write[...], low))).astype(BF)
    top, rest = two_parts(values[...].astype(F32) * scale)
    d_write[...] = dw[...] + mm(top, high) + mm(top, low) + mm(rest, high)
    for r in range(4):
        total = second[r, 0:EXP, :].astype(F32)
        for k in range(1, 8):
            total = total + second[4 * k + r, 0:EXP, :].astype(F32)
        d_out[(r >> 1) * EXP : (r >> 1) * EXP + EXP, (r & 1) * TOK : (r & 1) * TOK + TOK] = total


def step(mixed, cotangent, routes, gates, w_gate, w_up, w_down, out_weight, gate_pre, mixer_out, values,
         write_keys, read_keys, log_decay, entry_states):
    shape = jax.ShapeDtypeStruct
    swap = [(0, 1), (1, 0)]
    rings = []
    for k in range(1, 5):
        up = [(2 * y, 2 * ((y + k) % 8)) for y in range(8)]
        rings.append(up + [(2 * y + 1, 2 * ((y - k) % 8) + 1) for y in range(8)])
    ring = rings[0]
    slot = lax.axis_index(TP).astype(jnp.int32).reshape(1)
    own = jnp.stack([w_gate[0].T, w_up[0].T, w_down[0]])
    other = lax.ppermute(own, "core", swap)
    buf, target = prepare(slot, routes.T, gates.T, mixed, cotangent)
    c0 = lax.all_to_all(buf, SP, 0, 0, tiled=True)
    c2 = lax.ppermute(c0, TP, ring)
    c1 = lax.ppermute(c0, "core", swap)
    c3 = lax.ppermute(c1, TP, ring)
    c4 = lax.ppermute(c2, TP, ring)
    moved, other = lax.optimization_barrier((c2, other))
    c5 = lax.ppermute(moved, "core", swap)
    c6 = lax.ppermute(c3, "core", swap)
    c7 = lax.ppermute(c4, "core", swap)
    chunks = (c0, c1, c2, c3, c4, c5, c6, c7)
    grad = shape((ROWS, 2 * FF), BF)
    full, thin = shape((ROWS, WIDE), BF), shape((ROWS, TOK), BF)
    early = call(
        early_kernel, (shape((ROWS, 4 * FF), F32), shape((ROWS, 2 * FF), F32)),
        [smem()] + [vmem()] * 9, (slot, *chunks[:7], own, other), flops=10**8)
    *parts, home, g_gate, g_up, g_hid = call(
        expert_kernel, (full, full, full, thin, thin, grad, grad, grad),
        [smem()] + [vmem()] * 5, (slot, c7, *early, own, other))
    pieces = []
    for k in range(4):
        pieces.append(lax.ppermute(parts[k], TP, rings[k]))
    wide = shape((FF, D), BF)
    d_wg, d_wu, d_wd = call(
        weights_kernel, (wide, wide, wide),
        [smem()] + [vmem()] * 11, (slot, *chunks, g_gate, g_up, g_hid), flops=10**9)
    pieces, d_wg, d_wu, d_wd = lax.optimization_barrier((pieces, d_wg, d_wu, d_wd))
    keep, give = call(
        fold_kernel, (shape((ROWS, TOK), F32), thin),
        [smem()] + [vmem()] * 5, (slot, *pieces, home))
    taken = lax.ppermute(give, "core", swap)
    summed = call(join_kernel, shape((EXP, CAP, TOK), BF), [vmem()] * 2, (keep, taken))
    back = lax.all_to_all(summed, SP, 0, 0, tiled=True)
    d_input = combine(slot, target, back, cotangent)
    whole = lax.all_gather(d_input, TP, axis=0, tiled=True)
    flat = shape((TOK, HEADS * HD), BF)
    quarter = shape((EXP, EXP, TOK), BF)
    spot = lax.axis_index("x").astype(jnp.int32).reshape(1)
    d_gate, grad_y, run, sent, *shares = call(
        project_kernel,
        (flat, shape((TOK, HEADS * HD), F32), shape((8, TOK), F32), shape((EXP, 16, STATE), BF),
         quarter, quarter, quarter, quarter),
        [smem()] + [vmem()] * 6, (spot, whole, out_weight, gate_pre, mixer_out, log_decay, read_keys),
        scratch=[pltpu.VMEM((4, EXP, EXP, TOK), BF)])
    received = lax.all_to_all(sent, SP, 0, 0, tiled=True)
    for k in range(1, 4):
        shares[k] = lax.ppermute(shares[k], "x", [(i, (i + k) % 4) for i in range(4)])
    square = shape((TOK, STATE), F32)
    dx, dw, d_read = call(
        inner_kernel, (shape((TOK, HEADS * HD), F32), square, square),
        [vmem()] * 6, (grad_y, values, write_keys, read_keys, run, entry_states[0]), flops=10**9)
    received, dx, dw, d_read = lax.optimization_barrier((received, dx, dw, d_read))
    states = call(scan_kernel, shape((EXP, 48, STATE), BF), [vmem()] * 5, (received, *shares))
    second = lax.all_to_all(states, SP, 0, 0, tiled=True)
    d_values, d_write, d_out_weight = call(
        outer_kernel, (flat, square, shape((D // EXP, HEADS * HD), F32)), [vmem()] * 6,
        (dx, dw, values, write_keys, run, second))
    return (d_wg.T[None], d_wu.T[None], d_wd[None], d_out_weight, d_input, d_values, d_write, d_read, d_gate)


def solution(mesh):
    finer = Mesh(mesh.devices.reshape(8, 4, 8, 2), ("z", "x", "y", "core"))
    return jax.shard_map(
        step,
        mesh=finer,
        in_specs=(
            P(SP, None),
            P(SP, None),
            P(SP, None),
            P(SP, None),
            P(SP, None, TP),
            P(SP, None, TP),
            P(SP, TP, None),
            P(TP, None),
            P(SP, TP),
            P(SP, TP),
            P(SP, TP),
            P(SP, TP),
            P(SP, TP),
            P(TP, SP),
            P(SP, TP, None, None),
        ),
        out_specs=(
            P(SP, None, TP),
            P(SP, None, TP),
            P(SP, TP, None),
            P(SP, TP),
            P(SP, TP),
            P(SP, TP),
            P(SP, TP),
            P(SP, TP),
            P(SP, TP),
        ),
        check_vma=False,
    )
```

```python
import jax
import jax.numpy as jnp
from jax import lax
from jax.experimental import pallas as pl
from jax.experimental.pallas import tpu as pltpu
from jax.sharding import Mesh
from jax.sharding import PartitionSpec as P

D = 2048
TOK = 128
EXP = 32
CAP = 16
ROWS = EXP * CAP
WIDE = 256
FF = 64
HEADS = 4
HD = 64
STATE = 128
PLAN = ((3, True), (3, False), (2, True), (2, False), (1, True), (1, False), (4, True), (0, True))
SP = ("z", "x")
TP = ("y", "core")
GRANT = 16 * 1024 * 1024
BF = jnp.bfloat16
F32 = jnp.float32


def iota(shape, dim):
    return lax.broadcasted_iota(jnp.int32, shape, dim)


def mm(a, b, precision=None):
    return lax.dot_general(a, b, (((1,), (0,)), ((), ())), precision=precision, preferred_element_type=F32)


def mm_nt(a, b):
    return lax.dot_general(a, b, (((1,), (1,)), ((), ())), preferred_element_type=F32)


def mm_parts(left, right, product):
    total = None
    for i, a in enumerate(left):
        for j, b in enumerate(right):
            if i + j < 2:
                part = product(a, b)
                total = part if total is None else total + part
    return total


def two_parts(value):
    high = value.astype(BF)
    return high, (value - high.astype(F32)).astype(BF)


def chunk_ids(slot):
    y, core = slot >> 1, slot & 1
    turn = 2 * core - 1
    near, far, beyond, home = (y + turn) & 3, (y - turn) & 3, (y + 2) & 3, y & 3
    mine, theirs = core, 1 - core
    return (2 * home + mine, 2 * home + theirs, 2 * near + mine, 2 * near + theirs, 2 * beyond + mine,
            2 * far + theirs, 2 * far + mine, 2 * beyond + theirs)


def columns(row):
    return jnp.broadcast_to(row, (8, row.shape[1])).T[:, 0:1]


def vmem():
    return pl.BlockSpec(memory_space=pltpu.VMEM)


def smem():
    return pl.BlockSpec(memory_space=pltpu.SMEM)


def call(kernel, outs, specs, args, flops=0, scratch=()):
    return pl.pallas_call(
        kernel,
        out_shape=outs,
        in_specs=specs,
        out_specs=jax.tree.map(lambda _: vmem(), outs),
        scratch_shapes=scratch,
        compiler_params=pltpu.CompilerParams(vmem_limit_bytes=GRANT),
        cost_estimate=pl.CostEstimate(flops=flops, bytes_accessed=0, transcendentals=0),
    )(*args)


def prepare_kernel(where, routes, gates, mix, cot, buf, target):
    picks = routes[...]
    expert = iota((EXP, TOK), 0)
    hits = [expert == picks[k : k + 1] for k in range(2)]
    both = jnp.where(hits[0] | hits[1], 1.0, 0.0).astype(BF)
    before = jnp.where(iota((TOK, TOK), 0) < iota((TOK, TOK), 1), 1.0, 0.0).astype(BF)
    count = mm(both, before)
    row = iota((ROWS, TOK), 0)
    cots = cot[...].astype(F32)
    places, scaled, rows = [], [], []
    for k in range(2):
        slot = jnp.sum(jnp.where(hits[k], count, 0.0), axis=0, keepdims=True)
        place = picks[k : k + 1] * CAP + slot.astype(jnp.int32)
        rows.append(place)
        places.append(jnp.where(row == place, 1.0, 0.0).astype(BF))
        scaled.append((columns(gates[k : k + 1, :]) * cots).astype(BF))
    target[...] = jnp.concatenate(rows + [jnp.zeros((6, TOK), jnp.int32)], axis=0)
    toks = mm(places[0] + places[1], mix[...]).astype(BF)
    buf[:, 0:CAP, :] = toks.reshape(EXP, CAP, WIDE)
    spread = mm(jnp.concatenate(places, axis=1), jnp.concatenate(scaled, axis=0)).astype(BF)
    buf[:, CAP : 2 * CAP, :] = spread.reshape(EXP, CAP, WIDE)


def prepare(quarter, routes, gates, mixed, cotangent):
    whole = lambda i, q: (0, 0)
    part = lambda i, q: (0, lax.rem(q[0], 8))
    return pl.pallas_call(
        prepare_kernel,
        out_shape=(
            jax.ShapeDtypeStruct((EXP, 2 * CAP, WIDE), BF),
            jax.ShapeDtypeStruct((8, TOK), jnp.int32),
        ),
        grid_spec=pltpu.PrefetchScalarGridSpec(
            num_scalar_prefetch=1,
            grid=(1,),
            in_specs=[
                pl.BlockSpec((2, TOK), whole),
                pl.BlockSpec((2, TOK), whole),
                pl.BlockSpec((TOK, WIDE), part),
                pl.BlockSpec((TOK, WIDE), part),
            ],
            out_specs=(
                pl.BlockSpec((EXP, 2 * CAP, WIDE), lambda i, q: (0, 0, 0)),
                pl.BlockSpec((8, TOK), whole),
            ),
        ),
        name="prepare",
    )(quarter, routes, gates, mixed, cotangent)


def row_blocks(chunk):
    toks = chunk[:, 0:CAP, :].reshape(ROWS, WIDE)
    cots = chunk[:, CAP : 2 * CAP, :].reshape(ROWS, WIDE)
    return toks, cots


def gate_rows(own, other, at):
    return jnp.concatenate([own[0, :, at], other[0, :, at], own[1, :, at], other[1, :, at]], axis=0)


def chunk_products(chunk, position, own, other):
    at = pl.ds(pl.multiple_of(position * WIDE, WIDE), WIDE)
    toks, cots = row_blocks(chunk)
    down = jnp.concatenate([own[2, :, at], other[2, :, at]], axis=0)
    return mm_nt(toks, gate_rows(own, other, at)), mm_nt(cots, down)


def early_kernel(where, *refs):
    chunks = refs[:7]
    own, other, pre, grad_hidden = refs[7:]
    ids = chunk_ids(where[0])
    first, second = chunk_products(chunks[0], ids[0], own, other)
    for k in range(1, 7):
        more = chunk_products(chunks[k], ids[k], own, other)
        first, second = first + more[0], second + more[1]
    pre[...] = first
    grad_hidden[...] = second


def expert_kernel(where, chunk, early_pre, early_hidden, own, other, *outs):
    g_gate, g_up, g_hid = outs[8:]
    more = chunk_products(chunk, chunk_ids(where[0])[7], own, other)
    pre = early_pre[...] + more[0]
    grad_hidden = early_hidden[...] + more[1]
    pre_gate = pre[:, : 2 * FF]
    pre_up = pre[:, 2 * FF :]
    logistic = 1.0 / (1.0 + jnp.exp(-pre_gate))
    active = pre_gate * logistic
    slope = logistic * (1.0 + pre_gate * (1.0 - logistic))
    gate = (grad_hidden * pre_up * slope).astype(BF)
    up = (grad_hidden * active).astype(BF)
    g_gate[...] = gate
    g_up[...] = up
    g_hid[...] = (active * pre_up).astype(BF)
    grads = jnp.concatenate([gate, up], axis=1)
    y, core = where[0] >> 1, where[0] & 1
    step = 1 - 2 * core
    for out, (k, same) in zip(outs[:8], PLAN):
        chip = (y + step * k + 8) & 7
        side = core if same else 1 - core
        at = pl.ds(pl.multiple_of((2 * chip + side) * TOK, TOK), TOK)
        out[...] = mm(grads, gate_rows(own, other, at)).astype(BF)


def weights_kernel(where, *refs):
    chunks = refs[:8]
    g_gate, g_up, g_hid, d_gate, d_up, d_down = refs[8:]
    gates = jnp.concatenate([g_gate[...].T[:FF], g_up[...].T[:FF]], axis=0)
    hidden = g_hid[...].T[:FF]
    ids = chunk_ids(where[0])
    for k in range(8):
        at = pl.ds(pl.multiple_of(ids[k] * WIDE, WIDE), WIDE)
        toks, cots = row_blocks(chunks[k])
        both = mm(gates, toks).astype(BF)
        d_gate[:, at] = both[:FF]
        d_up[:, at] = both[FF:]
        d_down[:, at] = mm(hidden, cots).astype(BF)


def fold_kernel(*refs):
    total = refs[0][...].astype(F32)
    for part in refs[1:8]:
        total = total + part[...].astype(F32)
    refs[8][...] = total.astype(BF).reshape(EXP, CAP, TOK)


def combine_kernel(where, target, rows, cotangent, out, cot, arrived):
    at = pl.ds(pl.multiple_of(where[0] * TOK, TOK), TOK)
    copy = pltpu.make_async_copy(cotangent.at[:, at], cot, arrived)
    copy.start()
    lane = iota((TOK, ROWS), 1)
    places = target[...].T
    pick = jnp.where((lane == places[:, 0:1]) | (lane == places[:, 1:2]), 1.0, 0.0).astype(BF)
    total = mm(pick, rows[...].reshape(ROWS, TOK))
    copy.wait()
    out[...] = (cot[...].astype(F32) + total).astype(BF)


def combine(slot, target, rows, cotangent):
    return pl.pallas_call(
        combine_kernel,
        out_shape=jax.ShapeDtypeStruct((TOK, TOK), BF),
        in_specs=[smem(), vmem(), vmem(), pl.BlockSpec(memory_space=pltpu.HBM)],
        out_specs=vmem(),
        scratch_shapes=[pltpu.VMEM((TOK, TOK), BF), pltpu.SemaphoreType.DMA],
        compiler_params=pltpu.CompilerParams(vmem_limit_bytes=GRANT),
        name="combine",
    )(slot, target, rows, cotangent)


def project_kernel(spot, gathered, weight, gate_pre, mixer, logs, read, d_gate, grad_y, run, buf, *outs):
    quarters = outs[4]
    whole = jnp.concatenate([gathered[k * TOK : (k + 1) * TOK, :] for k in range(16)], axis=1)
    back = mm_nt(whole, weight[...])
    pre = gate_pre[...].astype(F32)
    saved = mixer[...].astype(F32)
    logistic = 1.0 / (1.0 + jnp.exp(-pre))
    active = pre * logistic
    d_gate[...] = (back * saved * (logistic * (1.0 + pre * (1.0 - logistic)))).astype(BF)
    gated = (saved * active).astype(BF)
    for k in range(8):
        turned = whole[:, k * WIDE : (k + 1) * WIDE].T
        part = mm(turned, gated).astype(BF)
        for r in range(4):
            half = part[:, (r & 1) * TOK : (r & 1) * TOK + TOK].reshape(4, FF, TOK)
            quarters[r, 4 * k : 4 * k + 4] = half[:, (r >> 1) * EXP : (r >> 1) * EXP + EXP]
    for k in range(4):
        outs[k][...] = quarters[(spot[0] + k) & 3]
    grad = back * active
    grad_y[...] = grad
    upto = jnp.where(iota((TOK, TOK), 0) <= iota((TOK, TOK), 1), 1.0, 0.0)
    rates = jnp.concatenate([logs[...], jnp.zeros((4, TOK), F32)], axis=0)
    running = mm(rates, upto, lax.Precision.HIGHEST)
    run[...] = running
    start = jnp.exp(running)
    turned = grad.T
    scale = jnp.concatenate([jnp.broadcast_to(start[j : j + 1], (HD, TOK)) for j in range(HEADS)], axis=0)
    high, low = two_parts(turned * scale)
    state = mm(high, read[...]) + mm(low, read[...])
    total = running[0:HEADS, TOK - 1 : TOK]
    first = total.astype(BF).astype(F32)
    second = (total - first).astype(BF).astype(F32)
    third = total - first - second
    line = iota((8, STATE), 0)
    notes = []
    for j in range(HEADS):
        note = jnp.where(line == 0, first[j : j + 1], jnp.where(line == 1, second[j : j + 1], third[j : j + 1]))
        note = jnp.where(line < 3, note, 0.0)
        notes.append(jnp.broadcast_to(note[None], (EXP // HEADS, 8, STATE)))
    sent = jnp.concatenate([state.reshape(EXP, 8, STATE), jnp.concatenate(notes, axis=0)], axis=1)
    buf[...] = sent.astype(BF)


def scan_kernel(received, p0, p1, p2, p3, out):
    total = p0[...].astype(F32) + p1[...].astype(F32) + p2[...].astype(F32) + p3[...].astype(F32)
    out[:, 0:EXP, :] = total.astype(BF)
    state = jnp.zeros((8, STATE), F32)
    for k in reversed(range(EXP)):
        high, low = two_parts(state)
        out[k, EXP:, :] = jnp.concatenate([high.astype(F32), low.astype(F32)], axis=0).astype(BF)
        if k > 0:
            piece = received[k].astype(F32)
            log = piece[8:9] + piece[9:10] + piece[10:11]
            state = jnp.exp(log) * state + piece[0:8]


def inner_kernel(grad_y, values, write, read, run, entry, dx, dw, dr):
    running = run[...]
    cols = running.T
    grads = grad_y[...]
    vals = values[...]
    cross = mm_nt(write[...], read[...])
    later = iota((TOK, TOK), 1) >= iota((TOK, TOK), 0)
    total = jnp.zeros((TOK, TOK), F32)
    parts = []
    starts = []
    for j in range(HEADS):
        spread = running[j : j + 1] - cols[:, j : j + 1]
        decay = jnp.where(later, jnp.exp(jnp.where(later, spread, 0.0)), 0.0)
        grad = grads[:, j * HD : (j + 1) * HD]
        halves = two_parts(grad)
        parts.append(mm_parts(two_parts(cross * decay), halves, mm))
        total = total + mm_parts((vals[:, j * HD : (j + 1) * HD],), halves, mm_nt) * decay
        starts.append(grad * jnp.exp(cols[:, j : j + 1]))
    dx[...] = jnp.concatenate(parts, axis=1)
    dw[...] = mm_parts(two_parts(total), (read[...],), mm)
    entry_rows = two_parts(entry[...].reshape(HEADS * HD, STATE))
    first = mm_parts(two_parts(total.T), (write[...],), mm)
    dr[...] = first + mm_parts(two_parts(jnp.concatenate(starts, axis=1)), entry_rows, mm)


def outer_kernel(dx, dw, values, write, run, second, d_values, d_write, d_out):
    running = run[...]
    ends = jnp.exp(running[:, TOK - 1 : TOK] - running).T
    scale = jnp.concatenate([jnp.broadcast_to(ends[:, j : j + 1], (TOK, HD)) for j in range(HEADS)], axis=1)
    later = second[:, EXP:, :].astype(F32)
    high = later[:, 0:8].reshape(HEADS * HD, STATE).astype(BF)
    low = later[:, 8:16].reshape(HEADS * HD, STATE).astype(BF)
    d_values[...] = (dx[...] + scale * (mm_nt(write[...], high) + mm_nt(write[...], low))).astype(BF)
    top, rest = two_parts(values[...].astype(F32) * scale)
    d_write[...] = dw[...] + mm(top, high) + mm(top, low) + mm(rest, high)
    for r in range(4):
        total = second[r, 0:EXP, :].astype(F32)
        for k in range(1, 8):
            total = total + second[4 * k + r, 0:EXP, :].astype(F32)
        d_out[(r >> 1) * EXP : (r >> 1) * EXP + EXP, (r & 1) * TOK : (r & 1) * TOK + TOK] = total


def step(mixed, cotangent, routes, gates, w_gate, w_up, w_down, out_weight, gate_pre, mixer_out, values,
         write_keys, read_keys, log_decay, entry_states):
    shape = jax.ShapeDtypeStruct
    swap = [(0, 1), (1, 0)]
    def route(k, same):
        pairs = []
        for y in range(8):
            pairs.append((2 * y, 2 * ((y + k) % 8) + (0 if same else 1)))
            pairs.append((2 * y + 1, 2 * ((y - k) % 8) + (1 if same else 0)))
        return pairs

    ring = route(1, True)
    slot = lax.axis_index(TP).astype(jnp.int32).reshape(1)
    own = jnp.stack([w_gate[0].T, w_up[0].T, w_down[0]])
    other = lax.ppermute(own, "core", swap)
    buf, target = prepare(slot, routes.T, gates.T, mixed, cotangent)
    c0 = lax.all_to_all(buf, SP, 0, 0, tiled=True)
    c2 = lax.ppermute(c0, TP, ring)
    c1 = lax.ppermute(c0, "core", swap)
    c3 = lax.ppermute(c1, TP, ring)
    c4 = lax.ppermute(c2, TP, ring)
    moved, other = lax.optimization_barrier((c2, other))
    c5 = lax.ppermute(moved, "core", swap)
    c6 = lax.ppermute(c3, "core", swap)
    c7 = lax.ppermute(c4, "core", swap)
    chunks = (c0, c1, c2, c3, c4, c5, c6, c7)
    grad = shape((ROWS, 2 * FF), BF)
    thin = shape((ROWS, TOK), BF)
    early = call(
        early_kernel, (shape((ROWS, 4 * FF), F32), shape((ROWS, 2 * FF), F32)),
        [smem()] + [vmem()] * 9, (slot, *chunks[:7], own, other), flops=10**8)
    *parts, g_gate, g_up, g_hid = call(
        expert_kernel, (thin,) * 8 + (grad, grad, grad),
        [smem()] + [vmem()] * 5, (slot, c7, *early, own, other))
    pieces = []
    for k, (far, same) in enumerate(PLAN[:7]):
        pieces.append(lax.ppermute(parts[k], TP, route(far, same)))
    wide = shape((FF, D), BF)
    d_wg, d_wu, d_wd = call(
        weights_kernel, (wide, wide, wide),
        [smem()] + [vmem()] * 11, (slot, *chunks, g_gate, g_up, g_hid), flops=10**9)
    pieces, d_wg, d_wu, d_wd = lax.optimization_barrier((pieces, d_wg, d_wu, d_wd))
    summed = call(fold_kernel, shape((EXP, CAP, TOK), BF), [vmem()] * 8, (*pieces, parts[7]))
    back = lax.all_to_all(summed, SP, 0, 0, tiled=True)
    d_input = combine(slot, target, back, cotangent)
    whole = lax.all_gather(d_input, TP, axis=0, tiled=True)
    flat = shape((TOK, HEADS * HD), BF)
    quarter = shape((EXP, EXP, TOK), BF)
    spot = lax.axis_index("x").astype(jnp.int32).reshape(1)
    d_gate, grad_y, run, sent, *shares = call(
        project_kernel,
        (flat, shape((TOK, HEADS * HD), F32), shape((8, TOK), F32), shape((EXP, 16, STATE), BF),
         quarter, quarter, quarter, quarter),
        [smem()] + [vmem()] * 6, (spot, whole, out_weight, gate_pre, mixer_out, log_decay, read_keys),
        scratch=[pltpu.VMEM((4, EXP, EXP, TOK), BF)])
    received = lax.all_to_all(sent, SP, 0, 0, tiled=True)
    for k in range(1, 4):
        shares[k] = lax.ppermute(shares[k], "x", [(i, (i + k) % 4) for i in range(4)])
    square = shape((TOK, STATE), F32)
    dx, dw, d_read = call(
        inner_kernel, (shape((TOK, HEADS * HD), F32), square, square),
        [vmem()] * 6, (grad_y, values, write_keys, read_keys, run, entry_states[0]), flops=10**9)
    received, dx, dw, d_read = lax.optimization_barrier((received, dx, dw, d_read))
    states = call(scan_kernel, shape((EXP, 48, STATE), BF), [vmem()] * 5, (received, *shares))
    second = lax.all_to_all(states, SP, 0, 0, tiled=True)
    d_values, d_write, d_out_weight = call(
        outer_kernel, (flat, square, shape((D // EXP, HEADS * HD), F32)), [vmem()] * 6,
        (dx, dw, values, write_keys, run, second))
    return (d_wg.T[None], d_wu.T[None], d_wd[None], d_out_weight, d_input, d_values, d_write, d_read, d_gate)


def solution(mesh):
    finer = Mesh(mesh.devices.reshape(8, 4, 8, 2), ("z", "x", "y", "core"))
    return jax.shard_map(
        step,
        mesh=finer,
        in_specs=(
            P(SP, None),
            P(SP, None),
            P(SP, None),
            P(SP, None),
            P(SP, None, TP),
            P(SP, None, TP),
            P(SP, TP, None),
            P(TP, None),
            P(SP, TP),
            P(SP, TP),
            P(SP, TP),
            P(SP, TP),
            P(SP, TP),
            P(TP, SP),
            P(SP, TP, None, None),
        ),
        out_specs=(
            P(SP, None, TP),
            P(SP, None, TP),
            P(SP, TP, None),
            P(SP, TP),
            P(SP, TP),
            P(SP, TP),
            P(SP, TP),
            P(SP, TP),
            P(SP, TP),
        ),
        check_vma=False,
    )
```

```python
import jax
import jax.numpy as jnp
from jax import lax
from jax.experimental import pallas as pl
from jax.experimental.pallas import tpu as pltpu
from jax.sharding import Mesh
from jax.sharding import PartitionSpec as P

D = 2048
TOK = 128
EXP = 32
CAP = 16
ROWS = EXP * CAP
WIDE = 256
FF = 64
HEADS = 4
HD = 64
STATE = 128
SP = ("z", "x")
TP = ("y", "core")
GRANT = 16 * 1024 * 1024
BF = jnp.bfloat16
F32 = jnp.float32


def iota(shape, dim):
    return lax.broadcasted_iota(jnp.int32, shape, dim)


def mm(a, b, precision=None):
    return lax.dot_general(a, b, (((1,), (0,)), ((), ())), precision=precision, preferred_element_type=F32)


def mm_nt(a, b):
    return lax.dot_general(a, b, (((1,), (1,)), ((), ())), preferred_element_type=F32)


def mm_parts(left, right, product):
    total = None
    for i, a in enumerate(left):
        for j, b in enumerate(right):
            if i + j < 2:
                part = product(a, b)
                total = part if total is None else total + part
    return total


def two_parts(value):
    high = value.astype(BF)
    return high, (value - high.astype(F32)).astype(BF)


def chunk_ids(slot):
    y, core = slot >> 1, slot & 1
    turn = 2 * core - 1
    near, far, beyond, home = (y + turn) & 3, (y - turn) & 3, (y + 2) & 3, y & 3
    mine, theirs = core, 1 - core
    return (2 * home + mine, 2 * home + theirs, 2 * near + mine, 2 * near + theirs, 2 * beyond + mine,
            2 * far + theirs, 2 * far + mine, 2 * beyond + theirs)


def columns(row):
    return jnp.broadcast_to(row, (8, row.shape[1])).T[:, 0:1]


def vmem():
    return pl.BlockSpec(memory_space=pltpu.VMEM)


def smem():
    return pl.BlockSpec(memory_space=pltpu.SMEM)


def call(kernel, outs, specs, args, flops=0, scratch=()):
    return pl.pallas_call(
        kernel,
        out_shape=outs,
        in_specs=specs,
        out_specs=jax.tree.map(lambda _: vmem(), outs),
        scratch_shapes=scratch,
        compiler_params=pltpu.CompilerParams(vmem_limit_bytes=GRANT),
        cost_estimate=pl.CostEstimate(flops=flops, bytes_accessed=0, transcendentals=0),
    )(*args)


def prepare_kernel(where, routes, gates, mix, cot, buf, target):
    picks = routes[...]
    expert = iota((EXP, TOK), 0)
    hits = [expert == picks[k : k + 1] for k in range(2)]
    both = jnp.where(hits[0] | hits[1], 1.0, 0.0).astype(BF)
    before = jnp.where(iota((TOK, TOK), 0) < iota((TOK, TOK), 1), 1.0, 0.0).astype(BF)
    count = mm(both, before)
    row = iota((ROWS, TOK), 0)
    cots = cot[...].astype(F32)
    places, scaled, rows = [], [], []
    for k in range(2):
        slot = jnp.sum(jnp.where(hits[k], count, 0.0), axis=0, keepdims=True)
        place = picks[k : k + 1] * CAP + slot.astype(jnp.int32)
        rows.append(place)
        places.append(jnp.where(row == place, 1.0, 0.0).astype(BF))
        scaled.append((columns(gates[k : k + 1, :]) * cots).astype(BF))
    target[...] = jnp.concatenate(rows + [jnp.zeros((6, TOK), jnp.int32)], axis=0)
    toks = mm(places[0] + places[1], mix[...]).astype(BF)
    buf[:, 0:CAP, :] = toks.reshape(EXP, CAP, WIDE)
    spread = mm(jnp.concatenate(places, axis=1), jnp.concatenate(scaled, axis=0)).astype(BF)
    buf[:, CAP : 2 * CAP, :] = spread.reshape(EXP, CAP, WIDE)


def prepare(quarter, routes, gates, mixed, cotangent):
    whole = lambda i, q: (0, 0)
    part = lambda i, q: (0, lax.rem(q[0], 8))
    return pl.pallas_call(
        prepare_kernel,
        out_shape=(
            jax.ShapeDtypeStruct((EXP, 2 * CAP, WIDE), BF),
            jax.ShapeDtypeStruct((8, TOK), jnp.int32),
        ),
        grid_spec=pltpu.PrefetchScalarGridSpec(
            num_scalar_prefetch=1,
            grid=(1,),
            in_specs=[
                pl.BlockSpec((2, TOK), whole),
                pl.BlockSpec((2, TOK), whole),
                pl.BlockSpec((TOK, WIDE), part),
                pl.BlockSpec((TOK, WIDE), part),
            ],
            out_specs=(
                pl.BlockSpec((EXP, 2 * CAP, WIDE), lambda i, q: (0, 0, 0)),
                pl.BlockSpec((8, TOK), whole),
            ),
        ),
        name="prepare",
    )(quarter, routes, gates, mixed, cotangent)


def row_blocks(chunk):
    toks = chunk[:, 0:CAP, :].reshape(ROWS, WIDE)
    cots = chunk[:, CAP : 2 * CAP, :].reshape(ROWS, WIDE)
    return toks, cots


def gate_rows(own, other, at):
    return jnp.concatenate([own[0, :, at], other[0, :, at], own[1, :, at], other[1, :, at]], axis=0)


def chunk_products(chunk, position, own, other):
    at = pl.ds(pl.multiple_of(position * WIDE, WIDE), WIDE)
    toks, cots = row_blocks(chunk)
    down = jnp.concatenate([own[2, :, at], other[2, :, at]], axis=0)
    return mm_nt(toks, gate_rows(own, other, at)), mm_nt(cots, down)


def early_kernel(where, *refs):
    chunks = refs[:7]
    own, other, pre, grad_hidden = refs[7:]
    ids = chunk_ids(where[0])
    first, second = chunk_products(chunks[0], ids[0], own, other)
    for k in range(1, 7):
        more = chunk_products(chunks[k], ids[k], own, other)
        first, second = first + more[0], second + more[1]
    pre[...] = first
    grad_hidden[...] = second


def expert_kernel(where, chunk, early_pre, early_hidden, own, other, *outs):
    near, mid, far, last, home, g_gate, g_up, g_hid = outs
    more = chunk_products(chunk, chunk_ids(where[0])[7], own, other)
    pre = early_pre[...] + more[0]
    grad_hidden = early_hidden[...] + more[1]
    pre_gate = pre[:, : 2 * FF]
    pre_up = pre[:, 2 * FF :]
    logistic = 1.0 / (1.0 + jnp.exp(-pre_gate))
    active = pre_gate * logistic
    slope = logistic * (1.0 + pre_gate * (1.0 - logistic))
    gate = (grad_hidden * pre_up * slope).astype(BF)
    up = (grad_hidden * active).astype(BF)
    g_gate[...] = gate
    g_up[...] = up
    g_hid[...] = (active * pre_up).astype(BF)
    grads = jnp.concatenate([gate, up], axis=1)
    y, core = where[0] >> 1, where[0] & 1
    step = 1 - 2 * core
    for k, out in ((4, last), (3, far), (2, mid), (1, near), (0, home)):
        chip = (y + step * k + 8) & 7
        start = chip * WIDE if k in (1, 2, 3) else chip * WIDE + core * TOK
        size = out.shape[1]
        at = pl.ds(pl.multiple_of(start, TOK), size)
        out[...] = mm(grads, gate_rows(own, other, at)).astype(BF)


def weights_kernel(where, *refs):
    chunks = refs[:8]
    g_gate, g_up, g_hid, d_gate, d_up, d_down = refs[8:]
    gates = jnp.concatenate([g_gate[...].T[:FF], g_up[...].T[:FF]], axis=0)
    hidden = g_hid[...].T[:FF]
    ids = chunk_ids(where[0])
    for k in range(8):
        at = pl.ds(pl.multiple_of(ids[k] * WIDE, WIDE), WIDE)
        toks, cots = row_blocks(chunks[k])
        both = mm(gates, toks).astype(BF)
        d_gate[:, at] = both[:FF]
        d_up[:, at] = both[FF:]
        d_down[:, at] = mm(hidden, cots).astype(BF)


def fold_kernel(where, near, mid, far, last, home, out):
    total = near[...].astype(F32) + mid[...].astype(F32) + far[...].astype(F32)
    extra = last[...].astype(F32) + home[...].astype(F32)
    for side in range(2):
        own = jnp.where((where[0] & 1) == side, extra, 0.0)
        part = total[:, side * TOK : (side + 1) * TOK] + own
        out[:, side * CAP : (side + 1) * CAP, :] = part.astype(BF).reshape(EXP, CAP, TOK)


def combine_kernel(where, target, rows, cotangent, out, cot, arrived):
    at = pl.ds(pl.multiple_of(where[0] * TOK, TOK), TOK)
    copy = pltpu.make_async_copy(cotangent.at[:, at], cot, arrived)
    copy.start()
    lane = iota((TOK, ROWS), 1)
    places = target[...].T
    pick = jnp.where((lane == places[:, 0:1]) | (lane == places[:, 1:2]), 1.0, 0.0).astype(BF)
    total = mm(pick, rows[:, 0:CAP, :].reshape(ROWS, TOK)) + mm(pick, rows[:, CAP:, :].reshape(ROWS, TOK))
    copy.wait()
    out[...] = (cot[...].astype(F32) + total).astype(BF)


def combine(slot, target, rows, cotangent):
    return pl.pallas_call(
        combine_kernel,
        out_shape=jax.ShapeDtypeStruct((TOK, TOK), BF),
        in_specs=[smem(), vmem(), vmem(), pl.BlockSpec(memory_space=pltpu.HBM)],
        out_specs=vmem(),
        scratch_shapes=[pltpu.VMEM((TOK, TOK), BF), pltpu.SemaphoreType.DMA],
        compiler_params=pltpu.CompilerParams(vmem_limit_bytes=GRANT),
        name="combine",
    )(slot, target, rows, cotangent)


def project_kernel(spot, gathered, weight, gate_pre, mixer, logs, read, d_gate, grad_y, run, buf, *outs):
    quarters = outs[4]
    whole = jnp.concatenate([gathered[k * TOK : (k + 1) * TOK, :] for k in range(16)], axis=1)
    back = mm_nt(whole, weight[...])
    pre = gate_pre[...].astype(F32)
    saved = mixer[...].astype(F32)
    logistic = 1.0 / (1.0 + jnp.exp(-pre))
    active = pre * logistic
    d_gate[...] = (back * saved * (logistic * (1.0 + pre * (1.0 - logistic)))).astype(BF)
    gated = (saved * active).astype(BF)
    for k in range(8):
        turned = whole[:, k * WIDE : (k + 1) * WIDE].T
        part = mm(turned, gated).astype(BF)
        for r in range(4):
            half = part[:, (r & 1) * TOK : (r & 1) * TOK + TOK].reshape(4, FF, TOK)
            quarters[r, 4 * k : 4 * k + 4] = half[:, (r >> 1) * EXP : (r >> 1) * EXP + EXP]
    for k in range(4):
        outs[k][...] = quarters[(spot[0] + k) & 3]
    grad = back * active
    grad_y[...] = grad
    upto = jnp.where(iota((TOK, TOK), 0) <= iota((TOK, TOK), 1), 1.0, 0.0)
    rates = jnp.concatenate([logs[...], jnp.zeros((4, TOK), F32)], axis=0)
    running = mm(rates, upto, lax.Precision.HIGHEST)
    run[...] = running
    start = jnp.exp(running)
    turned = grad.T
    scale = jnp.concatenate([jnp.broadcast_to(start[j : j + 1], (HD, TOK)) for j in range(HEADS)], axis=0)
    high, low = two_parts(turned * scale)
    state = mm(high, read[...]) + mm(low, read[...])
    total = running[0:HEADS, TOK - 1 : TOK]
    first = total.astype(BF).astype(F32)
    second = (total - first).astype(BF).astype(F32)
    third = total - first - second
    line = iota((8, STATE), 0)
    notes = []
    for j in range(HEADS):
        note = jnp.where(line == 0, first[j : j + 1], jnp.where(line == 1, second[j : j + 1], third[j : j + 1]))
        note = jnp.where(line < 3, note, 0.0)
        notes.append(jnp.broadcast_to(note[None], (EXP // HEADS, 8, STATE)))
    sent = jnp.concatenate([state.reshape(EXP, 8, STATE), jnp.concatenate(notes, axis=0)], axis=1)
    buf[...] = sent.astype(BF)


def scan_kernel(received, p0, p1, p2, p3, out):
    total = p0[...].astype(F32) + p1[...].astype(F32) + p2[...].astype(F32) + p3[...].astype(F32)
    out[:, 0:EXP, :] = total.astype(BF)
    state = jnp.zeros((8, STATE), F32)
    for k in reversed(range(EXP)):
        high, low = two_parts(state)
        out[k, EXP:, :] = jnp.concatenate([high.astype(F32), low.astype(F32)], axis=0).astype(BF)
        if k > 0:
            piece = received[k].astype(F32)
            log = piece[8:9] + piece[9:10] + piece[10:11]
            state = jnp.exp(log) * state + piece[0:8]


def inner_kernel(grad_y, values, write, read, run, entry, dx, dw, dr):
    running = run[...]
    cols = running.T
    grads = grad_y[...]
    vals = values[...]
    cross = mm_nt(write[...], read[...])
    later = iota((TOK, TOK), 1) >= iota((TOK, TOK), 0)
    total = jnp.zeros((TOK, TOK), F32)
    parts = []
    starts = []
    for j in range(HEADS):
        spread = running[j : j + 1] - cols[:, j : j + 1]
        decay = jnp.where(later, jnp.exp(jnp.where(later, spread, 0.0)), 0.0)
        grad = grads[:, j * HD : (j + 1) * HD]
        halves = two_parts(grad)
        parts.append(mm_parts(two_parts(cross * decay), halves, mm))
        total = total + mm_parts((vals[:, j * HD : (j + 1) * HD],), halves, mm_nt) * decay
        starts.append(grad * jnp.exp(cols[:, j : j + 1]))
    dx[...] = jnp.concatenate(parts, axis=1)
    dw[...] = mm_parts(two_parts(total), (read[...],), mm)
    entry_rows = two_parts(entry[...].reshape(HEADS * HD, STATE))
    first = mm_parts(two_parts(total.T), (write[...],), mm)
    dr[...] = first + mm_parts(two_parts(jnp.concatenate(starts, axis=1)), entry_rows, mm)


def outer_kernel(dx, dw, values, write, run, second, d_values, d_write, d_out):
    running = run[...]
    ends = jnp.exp(running[:, TOK - 1 : TOK] - running).T
    scale = jnp.concatenate([jnp.broadcast_to(ends[:, j : j + 1], (TOK, HD)) for j in range(HEADS)], axis=1)
    later = second[:, EXP:, :].astype(F32)
    high = later[:, 0:8].reshape(HEADS * HD, STATE).astype(BF)
    low = later[:, 8:16].reshape(HEADS * HD, STATE).astype(BF)
    d_values[...] = (dx[...] + scale * (mm_nt(write[...], high) + mm_nt(write[...], low))).astype(BF)
    top, rest = two_parts(values[...].astype(F32) * scale)
    d_write[...] = dw[...] + mm(top, high) + mm(top, low) + mm(rest, high)
    for r in range(4):
        total = second[r, 0:EXP, :].astype(F32)
        for k in range(1, 8):
            total = total + second[4 * k + r, 0:EXP, :].astype(F32)
        d_out[(r >> 1) * EXP : (r >> 1) * EXP + EXP, (r & 1) * TOK : (r & 1) * TOK + TOK] = total


def step(mixed, cotangent, routes, gates, w_gate, w_up, w_down, out_weight, gate_pre, mixer_out, values,
         write_keys, read_keys, log_decay, entry_states):
    shape = jax.ShapeDtypeStruct
    swap = [(0, 1), (1, 0)]
    rings = []
    for k in range(1, 5):
        up = [(2 * y, 2 * ((y + k) % 8)) for y in range(8)]
        rings.append(up + [(2 * y + 1, 2 * ((y - k) % 8) + 1) for y in range(8)])
    ring = rings[0]
    slot = lax.axis_index(TP).astype(jnp.int32).reshape(1)
    own = jnp.stack([w_gate[0].T, w_up[0].T, w_down[0]])
    other = lax.ppermute(own, "core", swap)
    buf, target = prepare(slot, routes.T, gates.T, mixed, cotangent)
    c0 = lax.all_to_all(buf, SP, 0, 0, tiled=True)
    c2 = lax.ppermute(c0, TP, ring)
    c1 = lax.ppermute(c0, "core", swap)
    c3 = lax.ppermute(c1, TP, ring)
    c4 = lax.ppermute(c2, TP, ring)
    moved, other = lax.optimization_barrier((c2, other))
    c5 = lax.ppermute(moved, "core", swap)
    c6 = lax.ppermute(c3, "core", swap)
    c7 = lax.ppermute(c4, "core", swap)
    chunks = (c0, c1, c2, c3, c4, c5, c6, c7)
    grad = shape((ROWS, 2 * FF), BF)
    full, thin = shape((ROWS, WIDE), BF), shape((ROWS, TOK), BF)
    early = call(
        early_kernel, (shape((ROWS, 4 * FF), F32), shape((ROWS, 2 * FF), F32)),
        [smem()] + [vmem()] * 9, (slot, *chunks[:7], own, other), flops=10**8)
    *parts, home, g_gate, g_up, g_hid = call(
        expert_kernel, (full, full, full, thin, thin, grad, grad, grad),
        [smem()] + [vmem()] * 5, (slot, c7, *early, own, other))
    pieces = []
    for k in range(4):
        pieces.append(lax.ppermute(parts[k], TP, rings[k]))
    wide = shape((FF, D), BF)
    d_wg, d_wu, d_wd = call(
        weights_kernel, (wide, wide, wide),
        [smem()] + [vmem()] * 11, (slot, *chunks, g_gate, g_up, g_hid), flops=10**9)
    pieces, d_wg, d_wu, d_wd = lax.optimization_barrier((pieces, d_wg, d_wu, d_wd))
    summed = call(
        fold_kernel, shape((EXP, 2 * CAP, TOK), BF),
        [smem()] + [vmem()] * 5, (slot, *pieces, home))
    back = lax.all_to_all(summed.reshape(2 * EXP, CAP, TOK), SP + ("core",), 0, 0, tiled=True)
    back = back.reshape(EXP, 2 * CAP, TOK)
    d_input = combine(slot, target, back, cotangent)
    whole = lax.all_gather(d_input, TP, axis=0, tiled=True)
    flat = shape((TOK, HEADS * HD), BF)
    quarter = shape((EXP, EXP, TOK), BF)
    spot = lax.axis_index("x").astype(jnp.int32).reshape(1)
    d_gate, grad_y, run, sent, *shares = call(
        project_kernel,
        (flat, shape((TOK, HEADS * HD), F32), shape((8, TOK), F32), shape((EXP, 16, STATE), BF),
         quarter, quarter, quarter, quarter),
        [smem()] + [vmem()] * 6, (spot, whole, out_weight, gate_pre, mixer_out, log_decay, read_keys),
        scratch=[pltpu.VMEM((4, EXP, EXP, TOK), BF)])
    received = lax.all_to_all(sent, SP, 0, 0, tiled=True)
    for k in range(1, 4):
        shares[k] = lax.ppermute(shares[k], "x", [(i, (i + k) % 4) for i in range(4)])
    square = shape((TOK, STATE), F32)
    dx, dw, d_read = call(
        inner_kernel, (shape((TOK, HEADS * HD), F32), square, square),
        [vmem()] * 6, (grad_y, values, write_keys, read_keys, run, entry_states[0]), flops=10**9)
    received, dx, dw, d_read = lax.optimization_barrier((received, dx, dw, d_read))
    states = call(scan_kernel, shape((EXP, 48, STATE), BF), [vmem()] * 5, (received, *shares))
    second = lax.all_to_all(states, SP, 0, 0, tiled=True)
    d_values, d_write, d_out_weight = call(
        outer_kernel, (flat, square, shape((D // EXP, HEADS * HD), F32)), [vmem()] * 6,
        (dx, dw, values, write_keys, run, second))
    return (d_wg.T[None], d_wu.T[None], d_wd[None], d_out_weight, d_input, d_values, d_write, d_read, d_gate)


def solution(mesh):
    finer = Mesh(mesh.devices.reshape(8, 4, 8, 2), ("z", "x", "y", "core"))
    return jax.shard_map(
        step,
        mesh=finer,
        in_specs=(
            P(SP, None),
            P(SP, None),
            P(SP, None),
            P(SP, None),
            P(SP, None, TP),
            P(SP, None, TP),
            P(SP, TP, None),
            P(TP, None),
            P(SP, TP),
            P(SP, TP),
            P(SP, TP),
            P(SP, TP),
            P(SP, TP),
            P(TP, SP),
            P(SP, TP, None, None),
        ),
        out_specs=(
            P(SP, None, TP),
            P(SP, None, TP),
            P(SP, TP, None),
            P(SP, TP),
            P(SP, TP),
            P(SP, TP),
            P(SP, TP),
            P(SP, TP),
            P(SP, TP),
        ),
        check_vma=False,
    )
```

```python
import jax
import jax.numpy as jnp
from jax import lax
from jax.experimental import pallas as pl
from jax.experimental.pallas import tpu as pltpu
from jax.sharding import Mesh
from jax.sharding import PartitionSpec as P

D = 2048
TOK = 128
EXP = 32
CAP = 16
ROWS = EXP * CAP
WIDE = 256
FF = 64
HEADS = 4
HD = 64
STATE = 128
SP = ("z", "x")
TP = ("y", "core")
GRANT = 16 * 1024 * 1024
BF = jnp.bfloat16
F32 = jnp.float32


def iota(shape, dim):
    return lax.broadcasted_iota(jnp.int32, shape, dim)


def mm(a, b, precision=None):
    return lax.dot_general(a, b, (((1,), (0,)), ((), ())), precision=precision, preferred_element_type=F32)


def mm_nt(a, b):
    return lax.dot_general(a, b, (((1,), (1,)), ((), ())), preferred_element_type=F32)


def mm_parts(left, right, product):
    total = None
    for i, a in enumerate(left):
        for j, b in enumerate(right):
            if i + j < 2:
                part = product(a, b)
                total = part if total is None else total + part
    return total


def two_parts(value):
    high = value.astype(BF)
    return high, (value - high.astype(F32)).astype(BF)


def chunk_ids(slot):
    y, core = slot >> 1, slot & 1
    turn = 2 * core - 1
    near, far, beyond, home = (y + turn) & 3, (y - turn) & 3, (y + 2) & 3, y & 3
    mine, theirs = core, 1 - core
    return (2 * home + mine, 2 * home + theirs, 2 * near + mine, 2 * near + theirs, 2 * beyond + mine,
            2 * far + theirs, 2 * far + mine, 2 * beyond + theirs)


def columns(row):
    return jnp.broadcast_to(row, (8, row.shape[1])).T[:, 0:1]


def vmem():
    return pl.BlockSpec(memory_space=pltpu.VMEM)


def smem():
    return pl.BlockSpec(memory_space=pltpu.SMEM)


def call(kernel, outs, specs, args, flops=0, scratch=()):
    return pl.pallas_call(
        kernel,
        out_shape=outs,
        in_specs=specs,
        out_specs=jax.tree.map(lambda _: vmem(), outs),
        scratch_shapes=scratch,
        compiler_params=pltpu.CompilerParams(vmem_limit_bytes=GRANT),
        cost_estimate=pl.CostEstimate(flops=flops, bytes_accessed=0, transcendentals=0),
    )(*args)


def prepare_kernel(where, routes, gates, mix, cot, buf, target):
    picks = routes[...]
    expert = iota((EXP, TOK), 0)
    hits = [expert == picks[k : k + 1] for k in range(2)]
    both = jnp.where(hits[0] | hits[1], 1.0, 0.0).astype(BF)
    before = jnp.where(iota((TOK, TOK), 0) < iota((TOK, TOK), 1), 1.0, 0.0).astype(BF)
    count = mm(both, before)
    row = iota((ROWS, TOK), 0)
    cots = cot[...].astype(F32)
    places, scaled, rows = [], [], []
    for k in range(2):
        slot = jnp.sum(jnp.where(hits[k], count, 0.0), axis=0, keepdims=True)
        place = picks[k : k + 1] * CAP + slot.astype(jnp.int32)
        rows.append(place)
        places.append(jnp.where(row == place, 1.0, 0.0).astype(BF))
        scaled.append((columns(gates[k : k + 1, :]) * cots).astype(BF))
    target[...] = jnp.concatenate(rows + [jnp.zeros((6, TOK), jnp.int32)], axis=0)
    toks = mm(places[0] + places[1], mix[...]).astype(BF)
    buf[:, 0:CAP, :] = toks.reshape(EXP, CAP, WIDE)
    spread = mm(jnp.concatenate(places, axis=1), jnp.concatenate(scaled, axis=0)).astype(BF)
    buf[:, CAP : 2 * CAP, :] = spread.reshape(EXP, CAP, WIDE)


def prepare(quarter, routes, gates, mixed, cotangent):
    whole = lambda i, q: (0, 0)
    part = lambda i, q: (0, lax.rem(q[0], 8))
    return pl.pallas_call(
        prepare_kernel,
        out_shape=(
            jax.ShapeDtypeStruct((EXP, 2 * CAP, WIDE), BF),
            jax.ShapeDtypeStruct((8, TOK), jnp.int32),
        ),
        grid_spec=pltpu.PrefetchScalarGridSpec(
            num_scalar_prefetch=1,
            grid=(1,),
            in_specs=[
                pl.BlockSpec((2, TOK), whole),
                pl.BlockSpec((2, TOK), whole),
                pl.BlockSpec((TOK, WIDE), part),
                pl.BlockSpec((TOK, WIDE), part),
            ],
            out_specs=(
                pl.BlockSpec((EXP, 2 * CAP, WIDE), lambda i, q: (0, 0, 0)),
                pl.BlockSpec((8, TOK), whole),
            ),
        ),
        name="prepare",
    )(quarter, routes, gates, mixed, cotangent)


def row_blocks(chunk):
    toks = chunk[:, 0:CAP, :].reshape(ROWS, WIDE)
    cots = chunk[:, CAP : 2 * CAP, :].reshape(ROWS, WIDE)
    return toks, cots


def gate_rows(own, other, at):
    return jnp.concatenate([own[0, :, at], other[0, :, at], own[1, :, at], other[1, :, at]], axis=0)


def chunk_products(chunk, position, own, other):
    at = pl.ds(pl.multiple_of(position * WIDE, WIDE), WIDE)
    toks, cots = row_blocks(chunk)
    down = jnp.concatenate([own[2, :, at], other[2, :, at]], axis=0)
    return mm_nt(toks, gate_rows(own, other, at)), mm_nt(cots, down)


def early_kernel(where, *refs):
    chunks = refs[:7]
    own, other, pre, grad_hidden = refs[7:]
    ids = chunk_ids(where[0])
    first, second = chunk_products(chunks[0], ids[0], own, other)
    for k in range(1, 7):
        more = chunk_products(chunks[k], ids[k], own, other)
        first, second = first + more[0], second + more[1]
    pre[...] = first
    grad_hidden[...] = second


def expert_kernel(where, chunk, early_pre, early_hidden, own, other, *outs):
    near, mid, far, last, home, g_gate, g_up, g_hid = outs
    more = chunk_products(chunk, chunk_ids(where[0])[7], own, other)
    pre = early_pre[...] + more[0]
    grad_hidden = early_hidden[...] + more[1]
    pre_gate = pre[:, : 2 * FF]
    pre_up = pre[:, 2 * FF :]
    logistic = 1.0 / (1.0 + jnp.exp(-pre_gate))
    active = pre_gate * logistic
    slope = logistic * (1.0 + pre_gate * (1.0 - logistic))
    gate = (grad_hidden * pre_up * slope).astype(BF)
    up = (grad_hidden * active).astype(BF)
    g_gate[...] = gate
    g_up[...] = up
    g_hid[...] = (active * pre_up).astype(BF)
    grads = jnp.concatenate([gate, up], axis=1)
    y, core = where[0] >> 1, where[0] & 1
    step = 1 - 2 * core
    for k, out in ((4, last), (3, far), (2, mid), (1, near), (0, home)):
        chip = (y + step * k + 8) & 7
        start = chip * WIDE if k in (1, 2, 3) else chip * WIDE + core * TOK
        size = out.shape[1]
        at = pl.ds(pl.multiple_of(start, TOK), size)
        out[...] = mm(grads, gate_rows(own, other, at)).astype(BF)


def weights_kernel(where, *refs):
    chunks = refs[:8]
    g_gate, g_up, g_hid, d_gate, d_up, d_down = refs[8:]
    gates = jnp.concatenate([g_gate[...].T[:FF], g_up[...].T[:FF]], axis=0)
    hidden = g_hid[...].T[:FF]
    ids = chunk_ids(where[0])
    for k in range(8):
        at = pl.ds(pl.multiple_of(ids[k] * WIDE, WIDE), WIDE)
        toks, cots = row_blocks(chunks[k])
        both = mm(gates, toks).astype(BF)
        d_gate[:, at] = both[:FF]
        d_up[:, at] = both[FF:]
        d_down[:, at] = mm(hidden, cots).astype(BF)


def fold_kernel(where, near, mid, far, last, home, keep, give):
    total = near[...].astype(F32) + mid[...].astype(F32) + far[...].astype(F32)
    first = total[:, :TOK]
    second = total[:, TOK:]
    top = where[0] & 1 == 0
    keep[...] = jnp.where(top, first, second) + last[...].astype(F32) + home[...].astype(F32)
    give[...] = jnp.where(top, second, first).astype(BF)


def join_kernel(keep, taken, out):
    out[...] = (keep[...] + taken[...].astype(F32)).astype(BF).reshape(EXP, CAP, TOK)


def combine_kernel(where, target, rows, cotangent, out, cot, arrived):
    at = pl.ds(pl.multiple_of(where[0] * TOK, TOK), TOK)
    copy = pltpu.make_async_copy(cotangent.at[:, at], cot, arrived)
    copy.start()
    lane = iota((TOK, ROWS), 1)
    places = target[...].T
    pick = jnp.where((lane == places[:, 0:1]) | (lane == places[:, 1:2]), 1.0, 0.0).astype(BF)
    total = mm(pick, rows[...].reshape(ROWS, TOK))
    copy.wait()
    out[...] = (cot[...].astype(F32) + total).astype(BF)


def combine(slot, target, rows, cotangent):
    return pl.pallas_call(
        combine_kernel,
        out_shape=jax.ShapeDtypeStruct((TOK, TOK), BF),
        in_specs=[smem(), vmem(), vmem(), pl.BlockSpec(memory_space=pltpu.HBM)],
        out_specs=vmem(),
        scratch_shapes=[pltpu.VMEM((TOK, TOK), BF), pltpu.SemaphoreType.DMA],
        compiler_params=pltpu.CompilerParams(vmem_limit_bytes=GRANT),
        name="combine",
    )(slot, target, rows, cotangent)


def project_kernel(spot, gathered, weight, gate_pre, mixer, logs, read, d_gate, grad_y, run, buf, *outs):
    quarters = outs[4]
    whole = jnp.concatenate([gathered[k * TOK : (k + 1) * TOK, :] for k in range(16)], axis=1)
    back = mm_nt(whole, weight[...])
    pre = gate_pre[...].astype(F32)
    saved = mixer[...].astype(F32)
    logistic = 1.0 / (1.0 + jnp.exp(-pre))
    active = pre * logistic
    d_gate[...] = (back * saved * (logistic * (1.0 + pre * (1.0 - logistic)))).astype(BF)
    gated = (saved * active).astype(BF)
    for k in range(8):
        turned = whole[:, k * WIDE : (k + 1) * WIDE].T
        part = mm(turned, gated).astype(BF)
        for r in range(4):
            half = part[:, (r & 1) * TOK : (r & 1) * TOK + TOK].reshape(4, FF, TOK)
            quarters[r, 4 * k : 4 * k + 4] = half[:, (r >> 1) * EXP : (r >> 1) * EXP + EXP]
    for k in range(4):
        outs[k][...] = quarters[(spot[0] + k) & 3]
    grad = back * active
    grad_y[...] = grad
    upto = jnp.where(iota((TOK, TOK), 0) <= iota((TOK, TOK), 1), 1.0, 0.0)
    rates = jnp.concatenate([logs[...], jnp.zeros((4, TOK), F32)], axis=0)
    running = mm(rates, upto, lax.Precision.HIGHEST)
    run[...] = running
    start = jnp.exp(running)
    turned = grad.T
    scale = jnp.concatenate([jnp.broadcast_to(start[j : j + 1], (HD, TOK)) for j in range(HEADS)], axis=0)
    high, low = two_parts(turned * scale)
    state = mm(high, read[...]) + mm(low, read[...])
    total = running[0:HEADS, TOK - 1 : TOK]
    first = total.astype(BF).astype(F32)
    second = (total - first).astype(BF).astype(F32)
    third = total - first - second
    line = iota((8, STATE), 0)
    notes = []
    for j in range(HEADS):
        note = jnp.where(line == 0, first[j : j + 1], jnp.where(line == 1, second[j : j + 1], third[j : j + 1]))
        note = jnp.where(line < 3, note, 0.0)
        notes.append(jnp.broadcast_to(note[None], (EXP // HEADS, 8, STATE)))
    sent = jnp.concatenate([state.reshape(EXP, 8, STATE), jnp.concatenate(notes, axis=0)], axis=1)
    buf[...] = sent.astype(BF)


def scan_kernel(received, p0, p1, p2, p3, out):
    total = p0[...].astype(F32) + p1[...].astype(F32) + p2[...].astype(F32) + p3[...].astype(F32)
    out[:, 0:EXP, :] = total.astype(BF)
    state = jnp.zeros((8, STATE), F32)
    for k in reversed(range(EXP)):
        out[k, EXP:, :] = state.astype(BF)
        if k > 0:
            piece = received[k].astype(F32)
            log = piece[8:9] + piece[9:10] + piece[10:11]
            state = jnp.exp(log) * state + piece[0:8]


def inner_kernel(grad_y, values, write, read, run, entry, dx, dw, dr):
    running = run[...]
    cols = running.T
    grads = grad_y[...]
    vals = values[...]
    cross = mm_nt(write[...], read[...])
    later = iota((TOK, TOK), 1) >= iota((TOK, TOK), 0)
    total = jnp.zeros((TOK, TOK), F32)
    parts = []
    starts = []
    for j in range(HEADS):
        spread = running[j : j + 1] - cols[:, j : j + 1]
        decay = jnp.where(later, jnp.exp(jnp.where(later, spread, 0.0)), 0.0)
        grad = grads[:, j * HD : (j + 1) * HD]
        halves = two_parts(grad)
        parts.append(mm_parts(two_parts(cross * decay), halves, mm))
        total = total + mm_parts((vals[:, j * HD : (j + 1) * HD],), halves, mm_nt) * decay
        starts.append(grad * jnp.exp(cols[:, j : j + 1]))
    dx[...] = jnp.concatenate(parts, axis=1)
    dw[...] = mm_parts(two_parts(total), (read[...],), mm)
    entry_rows = two_parts(entry[...].reshape(HEADS * HD, STATE))
    first = mm_parts(two_parts(total.T), (write[...],), mm)
    dr[...] = first + mm_parts(two_parts(jnp.concatenate(starts, axis=1)), entry_rows, mm)


def outer_kernel(dx, dw, values, write, run, second, d_values, d_write, d_out):
    running = run[...]
    ends = jnp.exp(running[:, TOK - 1 : TOK] - running).T
    scale = jnp.concatenate([jnp.broadcast_to(ends[:, j : j + 1], (TOK, HD)) for j in range(HEADS)], axis=1)
    later = second[:, EXP:, :].astype(F32).reshape(HEADS * HD, STATE).astype(BF)
    d_values[...] = (dx[...] + scale * mm_nt(write[...], later)).astype(BF)
    top, rest = two_parts(values[...].astype(F32) * scale)
    d_write[...] = dw[...] + mm(top, later) + mm(rest, later)
    for r in range(4):
        total = second[r, 0:EXP, :].astype(F32)
        for k in range(1, 8):
            total = total + second[4 * k + r, 0:EXP, :].astype(F32)
        d_out[(r >> 1) * EXP : (r >> 1) * EXP + EXP, (r & 1) * TOK : (r & 1) * TOK + TOK] = total


def step(mixed, cotangent, routes, gates, w_gate, w_up, w_down, out_weight, gate_pre, mixer_out, values,
         write_keys, read_keys, log_decay, entry_states):
    shape = jax.ShapeDtypeStruct
    swap = [(0, 1), (1, 0)]
    rings = []
    for k in range(1, 5):
        up = [(2 * y, 2 * ((y + k) % 8)) for y in range(8)]
        rings.append(up + [(2 * y + 1, 2 * ((y - k) % 8) + 1) for y in range(8)])
    ring = rings[0]
    slot = lax.axis_index(TP).astype(jnp.int32).reshape(1)
    own = jnp.stack([w_gate[0].T, w_up[0].T, w_down[0]])
    other = lax.ppermute(own, "core", swap)
    buf, target = prepare(slot, routes.T, gates.T, mixed, cotangent)
    c0 = lax.all_to_all(buf, SP, 0, 0, tiled=True)
    c2 = lax.ppermute(c0, TP, ring)
    c1 = lax.ppermute(c0, "core", swap)
    c3 = lax.ppermute(c1, TP, ring)
    c4 = lax.ppermute(c2, TP, ring)
    moved, other = lax.optimization_barrier((c2, other))
    c5 = lax.ppermute(moved, "core", swap)
    c6 = lax.ppermute(c3, "core", swap)
    c7 = lax.ppermute(c4, "core", swap)
    chunks = (c0, c1, c2, c3, c4, c5, c6, c7)
    grad = shape((ROWS, 2 * FF), BF)
    full, thin = shape((ROWS, WIDE), BF), shape((ROWS, TOK), BF)
    early = call(
        early_kernel, (shape((ROWS, 4 * FF), F32), shape((ROWS, 2 * FF), F32)),
        [smem()] + [vmem()] * 9, (slot, *chunks[:7], own, other), flops=10**8)
    *parts, home, g_gate, g_up, g_hid = call(
        expert_kernel, (full, full, full, thin, thin, grad, grad, grad),
        [smem()] + [vmem()] * 5, (slot, c7, *early, own, other))
    pieces = []
    for k in range(4):
        pieces.append(lax.ppermute(parts[k], TP, rings[k]))
    wide = shape((FF, D), BF)
    d_wg, d_wu, d_wd = call(
        weights_kernel, (wide, wide, wide),
        [smem()] + [vmem()] * 11, (slot, *chunks, g_gate, g_up, g_hid), flops=10**9)
    pieces, d_wg, d_wu, d_wd = lax.optimization_barrier((pieces, d_wg, d_wu, d_wd))
    keep, give = call(
        fold_kernel, (shape((ROWS, TOK), F32), thin),
        [smem()] + [vmem()] * 5, (slot, *pieces, home))
    taken = lax.ppermute(give, "core", swap)
    summed = call(join_kernel, shape((EXP, CAP, TOK), BF), [vmem()] * 2, (keep, taken))
    back = lax.all_to_all(summed, SP, 0, 0, tiled=True)
    d_input = combine(slot, target, back, cotangent)
    whole = lax.all_gather(d_input, TP, axis=0, tiled=True)
    flat = shape((TOK, HEADS * HD), BF)
    quarter = shape((EXP, EXP, TOK), BF)
    spot = lax.axis_index("x").astype(jnp.int32).reshape(1)
    d_gate, grad_y, run, sent, *shares = call(
        project_kernel,
        (flat, shape((TOK, HEADS * HD), F32), shape((8, TOK), F32), shape((EXP, 16, STATE), BF),
         quarter, quarter, quarter, quarter),
        [smem()] + [vmem()] * 6, (spot, whole, out_weight, gate_pre, mixer_out, log_decay, read_keys),
        scratch=[pltpu.VMEM((4, EXP, EXP, TOK), BF)])
    received = lax.all_to_all(sent, SP, 0, 0, tiled=True)
    for k in range(1, 4):
        shares[k] = lax.ppermute(shares[k], "x", [(i, (i + k) % 4) for i in range(4)])
    square = shape((TOK, STATE), F32)
    dx, dw, d_read = call(
        inner_kernel, (shape((TOK, HEADS * HD), F32), square, square),
        [vmem()] * 6, (grad_y, values, write_keys, read_keys, run, entry_states[0]), flops=10**9)
    received, dx, dw, d_read = lax.optimization_barrier((received, dx, dw, d_read))
    states = call(scan_kernel, shape((EXP, 40, STATE), BF), [vmem()] * 5, (received, *shares))
    second = lax.all_to_all(states, SP, 0, 0, tiled=True)
    d_values, d_write, d_out_weight = call(
        outer_kernel, (flat, square, shape((D // EXP, HEADS * HD), F32)), [vmem()] * 6,
        (dx, dw, values, write_keys, run, second))
    return (d_wg.T[None], d_wu.T[None], d_wd[None], d_out_weight, d_input, d_values, d_write, d_read, d_gate)


def solution(mesh):
    finer = Mesh(mesh.devices.reshape(8, 4, 8, 2), ("z", "x", "y", "core"))
    return jax.shard_map(
        step,
        mesh=finer,
        in_specs=(
            P(SP, None),
            P(SP, None),
            P(SP, None),
            P(SP, None),
            P(SP, None, TP),
            P(SP, None, TP),
            P(SP, TP, None),
            P(TP, None),
            P(SP, TP),
            P(SP, TP),
            P(SP, TP),
            P(SP, TP),
            P(SP, TP),
            P(TP, SP),
            P(SP, TP, None, None),
        ),
        out_specs=(
            P(SP, None, TP),
            P(SP, None, TP),
            P(SP, TP, None),
            P(SP, TP),
            P(SP, TP),
            P(SP, TP),
            P(SP, TP),
            P(SP, TP),
            P(SP, TP),
        ),
        check_vma=False,
    )
```
